512 devices in a mesh: grp: 2 (over y), sp: 16 (over z), tp: 16 (over x, core).
Axes of the slice: x: 8, y: 2, z: 16, core: 2. Of those that a mesh axis runs over, the one named last changes fastest.
The devices are a block of a 8x8x16 slice.
Arguments:
- latents: bfloat16 [12288, 4096], P(('grp', 'sp', 'tp')), parts along dimension 0, may hold values from -3 to 3
- conditions: float32 [4, 4096], P('grp', 'sp'), parts along dimension 0, may hold values from -6 to 6
- context: bfloat16 [1024, 4096], P(('grp', 'sp')), parts along dimension 0, may hold values from -6 to 6
- w_shift: bfloat16 [4096, 4096], P('sp', 'tp'), may hold values from -0.09375 to 0.09375
- w_scale: bfloat16 [4096, 4096], P('sp', 'tp'), may hold values from -0.09375 to 0.09375
- w_gate: bfloat16 [4096, 4096], P('sp', 'tp'), may hold values from -0.09375 to 0.09375
- w_qdown: bfloat16 [4096, 1024], P(None, 'tp'), may hold values from -2 to 2
- w_kvdown: bfloat16 [4096, 512], P(None, 'tp'), may hold values from -2 to 2
- w_rope: bfloat16 [4096, 32], replicated, may hold values from -0.09375 to 0.09375
- q_gain: float32 [1024], replicated, may hold values from 1 to 24
- latent_norm_gain: float32 [512], replicated, may hold values from 0.1 to 1.9
- query_up_weight: bfloat16 [1024, 3072], P(None, 'tp'), may hold values from -0.1875 to 0.1875
- key_up_weight: bfloat16 [512, 2048], P(None, 'tp'), may hold values from -0.25 to 0.25
- value_up_weight: bfloat16 [512, 2048], P(None, 'tp'), may hold values from -0.25 to 0.25
- context_bias: float32 [32], P('tp'), may hold values from 0.5 to 2
- w_out: bfloat16 [2048, 4096], P(None, 'tp'), may hold values from -0.5 to 0.5
Outputs:
- mixed: bfloat16 [12288, 4096], P(('grp', 'sp', 'tp')), parts along dimension 0
The draws below stay inside these ranges and needn't reach their ends.
There are 2 independent parts, one for each index of `grp`. The reference program is written for one: setup_inputs(seed, part) draws one part's arguments, and reference() takes and returns one part's arrays. A program takes and returns all parts, laid end to end along the dimension named above; an argument that names none is the same for every part. Nothing has to cross between parts.
All inputs are finite; a program needn't handle non-finite values.
Results may differ from the reference program's by a relative error of at most 0.01345.
The reference program's roundings to bfloat16 on the way count: a program that leaves them out, or rounds other values in their place, can miss the bound.
Values may be sent and summed in bfloat16 or wider, within the bound.
A program may use at most 64 MiB of HBM per device.

```python
import math
import jax
import jax.numpy as jnp
from jax import lax

MODEL_WIDTH = 4096
HEAD_TOTAL = 32
PLAIN_QK_DIM = 64
ROTARY_DIM = 32
VALUE_DIM = 64
QUERY_RANK = 1024
LATENT_KV_RANK = 512
GRID_W = 64
CTX = 512
TOKENS = 6144


def ascending_columns(key, row_count, col_count):
    entries = jax.random.normal(jax.random.fold_in(key, 11), (row_count, col_count), jnp.float32)
    jitter = jax.random.uniform(jax.random.fold_in(key, 12), (col_count,), jnp.float32, math.log(0.6), math.log(1.6))
    steepness = 10.0
    column_scale = jnp.exp(jitter + math.log(steepness) * jnp.arange(col_count, dtype=jnp.float32) / col_count)
    column_scale = column_scale / jnp.sqrt(jnp.mean(column_scale * column_scale))
    return jnp.clip(jnp.clip(entries, -4.0, 4.0) * column_scale * row_count ** (-0.5), -2.0, 2.0)


def draw_w_qdown(key, part):
    return ascending_columns(jax.random.fold_in(key, 3), MODEL_WIDTH, QUERY_RANK).astype(jnp.bfloat16)


def draw_w_kvdown(key, part):
    return ascending_columns(jax.random.fold_in(key, 5), MODEL_WIDTH, LATENT_KV_RANK).astype(jnp.bfloat16)


def draw_q_gain(key, part):
    return jax.random.uniform(jax.random.fold_in(key, 7), (QUERY_RANK,), jnp.float32, 1.5, 3.5)


def levels(stream_key, shape, shards, smallest, high):
    def one(position, shards_of):
        draws = jax.random.uniform(jax.random.fold_in(jax.random.fold_in(stream_key, 6), position), (shards_of,), jnp.float32, smallest / len(shards), high / len(shards))
        return jnp.repeat(jnp.exp(draws), shape[position] // shards_of).reshape((-1,) + (1,) * (len(shape) - position - 1))

    factor_of = one(*shards[0])
    for cut in shards[1:]:
        factor_of = factor_of * one(*cut)
    return factor_of


def noise(rng, extent, scale, most, cuts=(), held_as=jnp.bfloat16):
    loudness = levels(rng, extent, cuts, -0.22, 0.18) if cuts else 1.0
    result = jax.random.normal(rng, extent, jnp.float32) * scale * loudness
    return jnp.minimum(jnp.maximum(result, -most), most).astype(held_as)


def setup_inputs(seed: int = 0, part: int = 0) -> dict:
    streams_of = jax.random.split(jax.random.key(seed), 17)
    part_splits = jax.random.split(jax.random.fold_in(streams_of[16], part), 17)
    latents = noise(part_splits[0], (TOKENS, MODEL_WIDTH), 0.5, 3.0, ((0, 256),))
    conditions = noise(part_splits[1], (2, MODEL_WIDTH), 1.0, 6.0, ((1, 16),), jnp.float32)
    context = noise(part_splits[2], (CTX, MODEL_WIDTH), 1.0, 6.0, ((0, 16),))
    w_shift = noise(streams_of[3], (MODEL_WIDTH, MODEL_WIDTH), MODEL_WIDTH ** -0.5, 0.09375, ((0, 16), (1, 16)))
    w_scale = noise(streams_of[4], (MODEL_WIDTH, MODEL_WIDTH), MODEL_WIDTH ** -0.5, 0.09375, ((0, 16), (1, 16)))
    w_gate = noise(streams_of[5], (MODEL_WIDTH, MODEL_WIDTH), MODEL_WIDTH ** -0.5, 0.09375, ((0, 16), (1, 16)))
    w_qdown = draw_w_qdown(jax.random.fold_in(streams_of[16], 71), part)
    w_kvdown = draw_w_kvdown(jax.random.fold_in(streams_of[16], 71), part)
    w_rope = noise(streams_of[8], (MODEL_WIDTH, ROTARY_DIM), MODEL_WIDTH ** -0.5, 0.09375)
    q_gain = draw_q_gain(jax.random.fold_in(streams_of[16], 71), part)
    latent_norm_gain = jnp.clip(1.0 + 0.18 * jax.random.normal(streams_of[10], (LATENT_KV_RANK,), jnp.float32), 0.1, 1.9)
    query_up_weight = noise(streams_of[11], (QUERY_RANK, HEAD_TOTAL * (PLAIN_QK_DIM + ROTARY_DIM)), QUERY_RANK ** -0.5, 0.1875, ((1, 16),))
    key_up_weight = noise(streams_of[12], (LATENT_KV_RANK, HEAD_TOTAL * PLAIN_QK_DIM), LATENT_KV_RANK ** -0.5, 0.25, ((1, 16),))
    value_up_weight = noise(streams_of[13], (LATENT_KV_RANK, HEAD_TOTAL * VALUE_DIM), LATENT_KV_RANK ** -0.5, 0.25, ((1, 16),))
    context_bias = jnp.clip(0.5 + 1.5 * jax.random.uniform(streams_of[14], (HEAD_TOTAL,), jnp.float32) ** levels(streams_of[14], (HEAD_TOTAL,), ((0, 16),), -0.2, 0.2), 0.5, 2.0)
    w_out = noise(streams_of[15], (HEAD_TOTAL * VALUE_DIM, MODEL_WIDTH), (HEAD_TOTAL * VALUE_DIM // 16) ** -0.5, 0.5, ((1, 16),))
    return {"latents": latents, "conditions": conditions, "context": context, "w_shift": w_shift, "w_scale": w_scale, "w_gate": w_gate, "w_qdown": w_qdown, "w_kvdown": w_kvdown, "w_rope": w_rope, "q_gain": q_gain, "latent_norm_gain": latent_norm_gain, "query_up_weight": query_up_weight, "key_up_weight": key_up_weight, "value_up_weight": value_up_weight, "context_bias": context_bias, "w_out": w_out}


EPSILON = 1e-06

def layer_modulate(row_block, shift_by, scale_by):
    values = row_block.astype(jnp.float32)
    center = values - lax.optimization_barrier(jnp.mean(values, axis=-1, keepdims=True))
    spread = lax.optimization_barrier(jnp.mean(center * center, axis=-1, keepdims=True))
    normed = center * lax.rsqrt(spread + EPSILON)
    return (normed * (1.0 + scale_by) + shift_by).astype(jnp.bfloat16)

def rms_scale(raw_rows, gain_vec):
    values = raw_rows.astype(jnp.float32)
    factor = lax.rsqrt(lax.optimization_barrier(jnp.mean(values * values, axis=-1, keepdims=True)) + EPSILON)
    return (values * factor * gain_vec).astype(jnp.bfloat16)

def axial_turn(values, positions):
    freq_count = values.shape[-1] // 4
    inverse = 10000.0 ** (-jnp.arange(freq_count, dtype=jnp.float32) / freq_count)
    grid_row = (positions // GRID_W).astype(jnp.float32)
    grid_col = (positions % GRID_W).astype(jnp.float32)
    target = (positions.shape[0],) + (1,) * (values.ndim - 2) + (freq_count,)
    pieces = []
    for half_index, coordinate in enumerate((grid_row, grid_col)):
        angles = (coordinate[:, None] * inverse[None, :]).reshape(target)
        cosine = jnp.cos(angles)
        sine_of = jnp.sin(angles)
        segment = values[..., 2 * half_index * freq_count:2 * (half_index + 1) * freq_count]
        low_half = segment[..., :freq_count]
        high_half = segment[..., freq_count:]
        pieces.append(low_half * cosine - high_half * sine_of)
        pieces.append(low_half * sine_of + high_half * cosine)
    return jnp.concatenate(pieces, axis=-1)

def reference(latents, conditions, context, w_shift, w_scale, w_gate, w_qdown, w_kvdown, w_rope, q_gain, latent_norm_gain, query_up_weight, key_up_weight, value_up_weight, context_bias, w_out):
    cond_act = jax.nn.silu(conditions.astype(jnp.float32)).astype(jnp.bfloat16)
    shift_lat = jnp.dot(cond_act[0], w_shift, preferred_element_type=jnp.float32)
    scale_lat = jnp.dot(cond_act[0], w_scale, preferred_element_type=jnp.float32)
    gate_lat = jnp.dot(cond_act[0], w_gate, preferred_element_type=jnp.float32)
    shift_ctx = jnp.dot(cond_act[1], w_shift, preferred_element_type=jnp.float32)
    scale_ctx = jnp.dot(cond_act[1], w_scale, preferred_element_type=jnp.float32)
    h_lat = layer_modulate(latents, shift_lat, scale_lat)
    h_ctx = layer_modulate(context, shift_ctx, scale_ctx)
    cq_all = rms_scale(jnp.dot(h_lat, w_qdown, preferred_element_type=jnp.float32).astype(jnp.bfloat16), q_gain)
    ckv_lat = rms_scale(jnp.dot(h_lat, w_kvdown, preferred_element_type=jnp.float32).astype(jnp.bfloat16), latent_norm_gain)
    ckv_ctx = rms_scale(jnp.dot(h_ctx, w_kvdown, preferred_element_type=jnp.float32).astype(jnp.bfloat16), latent_norm_gain)
    positions = jnp.arange(TOKENS, dtype=jnp.int32)
    kr_lat = axial_turn(jnp.dot(h_lat, w_rope, preferred_element_type=jnp.float32), positions).astype(jnp.bfloat16)
    kr_ctx = jnp.dot(h_ctx, w_rope, preferred_element_type=jnp.float32).astype(jnp.bfloat16)
    q_all = jnp.dot(cq_all, query_up_weight, preferred_element_type=jnp.float32).reshape(TOKENS, HEAD_TOTAL, PLAIN_QK_DIM + ROTARY_DIM)
    queries = jnp.concatenate([q_all[..., :PLAIN_QK_DIM], axial_turn(q_all[..., PLAIN_QK_DIM:], positions)], axis=-1).astype(jnp.bfloat16)
    key_rows = jnp.concatenate([jnp.dot(ckv_lat, key_up_weight, preferred_element_type=jnp.float32).astype(jnp.bfloat16), jnp.dot(ckv_ctx, key_up_weight, preferred_element_type=jnp.float32).astype(jnp.bfloat16)], axis=0)
    value_rows = jnp.concatenate([jnp.dot(ckv_lat, value_up_weight, preferred_element_type=jnp.float32).astype(jnp.bfloat16), jnp.dot(ckv_ctx, value_up_weight, preferred_element_type=jnp.float32).astype(jnp.bfloat16)], axis=0)
    key_rows = key_rows.reshape(TOKENS + CTX, HEAD_TOTAL, PLAIN_QK_DIM)
    value_rows = value_rows.reshape(TOKENS + CTX, HEAD_TOTAL, VALUE_DIM)
    rope_keys = jnp.concatenate([kr_lat, kr_ctx], axis=0)
    is_ctx = (jnp.arange(TOKENS + CTX, dtype=jnp.int32) >= TOKENS).astype(jnp.float32)
    score_scale = (PLAIN_QK_DIM + ROTARY_DIM) ** (-0.5)

    def one_head(operands):
        head_q, head_k, head_v, head_bias = operands
        scores = jnp.dot(head_q[:, :PLAIN_QK_DIM], head_k.T, preferred_element_type=jnp.float32)
        scores = scores + jnp.dot(head_q[:, PLAIN_QK_DIM:], rope_keys.T, preferred_element_type=jnp.float32)
        scores = scores * score_scale + head_bias * is_ctx[None, :]
        largest = lax.optimization_barrier(jnp.max(scores, axis=-1, keepdims=True))
        exponent = jnp.exp(scores - largest)
        row_sum = lax.optimization_barrier(jnp.sum(exponent, axis=-1, keepdims=True))
        weights = exponent.astype(jnp.bfloat16)
        return (jnp.dot(weights, head_v, preferred_element_type=jnp.float32) / row_sum).astype(jnp.bfloat16)
    attended = lax.map(one_head, (queries.transpose(1, 0, 2), key_rows.transpose(1, 0, 2), value_rows.transpose(1, 0, 2), context_bias))
    attended = attended.transpose(1, 0, 2).reshape(TOKENS, HEAD_TOTAL * VALUE_DIM)
    projected = jnp.dot(attended, w_out, preferred_element_type=jnp.float32).astype(jnp.bfloat16)
    return (latents.astype(jnp.float32) + gate_lat * projected.astype(jnp.float32)).astype(jnp.bfloat16)
```

```python
import functools
import math

import jax
import jax.numpy as jnp
from jax import lax
from jax.experimental import pallas as pl
from jax.experimental.pallas import tpu as pltpu
from jax.sharding import PartitionSpec as P

PLAIN = 64
ROTARY = 32
VALUE = 64
GRID_W = 64
EPSILON = 1e-6
NEGATIVE = -1e30
LOG2E = 1.4426950408889634
SCORE = (PLAIN + ROTARY) ** (-0.5)
MESH = pl.DeviceIdType.MESH
BF = jnp.bfloat16
F32 = jnp.float32
KROWS = 2 * PLAIN + ROTARY
VROWS = 2 * VALUE


class Gather:
    def __init__(self, count, place, towards, chunks, sems, partner=None, core=0):
        self.count, self.place, self.towards = count, place, towards
        self.chunks, self.partner, self.core = chunks, partner, core
        self.recv, self.send = sems[0], sems[1]
        self.pair_recv, self.pair_send = (sems[2], sems[3]) if partner is not None else (None, None)
        self.reach = count // 2
        self.cut = (len(chunks) + 1) // 2

    def active(self, d, s, ch):
        if s < self.reach:
            return True
        if s > self.reach:
            return False
        return (ch < self.cut) if d == 0 else (ch >= self.cut)

    def source(self, d, s):
        move = (self.count - s) if d == 0 else s
        return lax.rem(self.place + move, self.count)

    def ring_copy(self, d, s, ch):
        piece = self.chunks[ch](self.source(d, s), self.core)
        return pltpu.make_async_remote_copy(
            src_ref=piece, dst_ref=piece, send_sem=self.send.at[d, s, ch], recv_sem=self.recv.at[d, s + 1, ch],
            device_id=self.towards(1 if d == 0 else self.count - 1), device_id_type=MESH)

    def ring_arrival(self, d, s, ch):
        piece = self.chunks[ch](self.source(d, s), self.core)
        return pltpu.make_async_remote_copy(
            src_ref=piece, dst_ref=piece, send_sem=self.send.at[d, s, ch], recv_sem=self.recv.at[d, s, ch],
            device_id=self.towards(self.count - 1 if d == 0 else 1), device_id_type=MESH)

    def pair_copy(self, d, s, ch, core):
        piece = self.chunks[ch](self.source(d, s), core)
        return pltpu.make_async_remote_copy(
            src_ref=piece, dst_ref=piece, send_sem=self.pair_send.at[d, s, ch], recv_sem=self.pair_recv.at[d, s, ch],
            device_id=self.partner, device_id_type=MESH)

    def start(self, only=None):
        for ch in range(len(self.chunks)) if only is None else only:
            for d in range(2):
                if self.active(d, 1, ch):
                    self.ring_copy(d, 0, ch).start()
            if self.partner is not None:
                self.pair_copy(0, 0, ch, self.core).start()

    def step(self, s):
        for ch in range(len(self.chunks)):
            for d in range(2):
                if self.active(d, s, ch):
                    self.ring_arrival(d, s, ch).wait_recv()
                    if self.active(d, s + 1, ch):
                        self.ring_copy(d, s, ch).start()
                    if self.partner is not None:
                        self.pair_copy(d, s, ch, self.core).start()

    def pair_step(self, s, only=None):
        for ch in range(len(self.chunks)) if only is None else only:
            for d in range(2):
                if (s == 0 and d == 0) or (s > 0 and self.active(d, s, ch)):
                    self.pair_copy(d, s, ch, 1 - self.core).wait_recv()

    def finish(self):
        for s in range(self.reach + 1):
            for ch in range(len(self.chunks)):
                for d in range(2):
                    if self.active(d, s + 1, ch):
                        self.ring_copy(d, s, ch).wait_send()
                    if self.partner is not None and ((s == 0 and d == 0) or (s > 0 and self.active(d, s, ch))):
                        self.pair_copy(d, s, ch, self.core).wait_send()


def axial_turn(a, row_cos, row_sin, col_cos, col_sin):
    a0, a1, a2, a3 = a[0:8], a[8:16], a[16:24], a[24:32]
    return jnp.concatenate(
        [a0 * row_cos - a1 * row_sin, a0 * row_sin + a1 * row_cos,
         a2 * col_cos - a3 * col_sin, a2 * col_sin + a3 * col_cos], axis=0)


def modulated(block, shift, scale):
    values = block.astype(F32)
    center = values - jnp.mean(values, axis=-1, keepdims=True)
    spread = jnp.mean(center * center, axis=-1, keepdims=True)
    return (center * lax.rsqrt(spread + EPSILON) * (1.0 + scale) + shift).astype(BF)


def rms_columns(raw, gain):
    values = raw.astype(F32)
    factor = lax.rsqrt(jnp.mean(values * values, axis=0, keepdims=True) + EPSILON)
    return (values * factor * gain).astype(BF)


def kernel(nz, nt, *refs):
    (lat_hbm, cond_ref, ctx_hbm, wsh_ref, wsc_ref, wg_ref, wq_hbm, wkv_hbm, wr_hbm, qg_ref, kg_ref,
     uq_hbm, uk_hbm, uv_hbm, bias_ref, wo_hbm, out_ref,
     lat, ctx, own_lat, wq, wkv, wr, uq, uk, uv, wo,
     wcat, uqT, ukvT, zmod, xmod, mod, h, hc, qraw, kvraw, kvcraw, kv, kvc, qb,
     m_ref, l_ref, acc, att, pbuf, mbuf,
     load_sem, zm_s, zm_r, xm_s, xm_r, a_s, a_r, lat_x, ctx_z, raw_x, rawc_x, kv_z, att_x) = refs
    z, t = lax.axis_index("sp"), lax.axis_index("tp")
    core = lax.rem(t, 2)
    chip = t // 2
    nx = nt // 2
    rows = own_lat.shape[0]
    tok = rows * nt
    crows = ctx.shape[1]
    width = own_lat.shape[1]
    part = width // nt
    rank_q, rank_kv = wq.shape[1], wkv.shape[1]
    along_z = lambda k: {"sp": lax.rem(z + k, nz)}
    along_x = lambda k: {"tp": lax.rem(t + 2 * k, nt)}
    partner = {"tp": t + 1 - 2 * core}
    half = width // 2

    loads = [
        pltpu.make_async_copy(lat_hbm, lat.at[t], load_sem.at[0]),
        pltpu.make_async_copy(ctx_hbm, ctx.at[z], load_sem.at[1]),
        pltpu.make_async_copy(lat_hbm, own_lat, load_sem.at[2]),
        pltpu.make_async_copy(wq_hbm, wq, load_sem.at[3]),
        pltpu.make_async_copy(wkv_hbm, wkv, load_sem.at[4]),
        pltpu.make_async_copy(wr_hbm, wr, load_sem.at[5]),
        pltpu.make_async_copy(uq_hbm, uq, load_sem.at[6]),
        pltpu.make_async_copy(uk_hbm, uk, load_sem.at[7]),
        pltpu.make_async_copy(uv_hbm, uv, load_sem.at[8]),
        pltpu.make_async_copy(wo_hbm, wo, load_sem.at[9]),
    ]
    barrier = pltpu.get_barrier_semaphore()
    for k in range(1, nz):
        pl.semaphore_signal(barrier, inc=1, device_id=along_z(k), device_id_type=MESH)
    for k in range(1, nt):
        pl.semaphore_signal(barrier, inc=1, device_id={"tp": lax.rem(t + k, nt)}, device_id_type=MESH)
    for load in loads:
        load.start()

    cond = cond_ref[...]
    act = cond / (1.0 + jnp.exp(-cond))
    act = jnp.concatenate([act, jnp.zeros((14, act.shape[1]), F32)], axis=0).astype(BF)
    shift_part = jnp.dot(act, wsh_ref[...], preferred_element_type=F32)
    scale_part = jnp.dot(act, wsc_ref[...], preferred_element_type=F32)
    gate_part = jnp.dot(act, wg_ref[...], preferred_element_type=F32)
    zmod[z] = jnp.concatenate([shift_part[0:2], scale_part[0:2], gate_part[0:2], gate_part[2:4]], axis=0)
    pl.semaphore_wait(barrier, nz + nt - 2)

    def zm(k, incoming):
        if incoming:
            src = lax.rem(z + nz - k, nz)
            return pltpu.make_async_remote_copy(zmod.at[src], zmod.at[src], zm_s.at[k], zm_r.at[k], device_id=along_z(nz - k), device_id_type=MESH)
        return pltpu.make_async_remote_copy(zmod.at[z], zmod.at[z], zm_s.at[k], zm_r.at[k], device_id=along_z(k), device_id_type=MESH)

    def xm(k, incoming):
        if incoming:
            src = lax.rem(t + nt - k, nt)
            return pltpu.make_async_remote_copy(xmod.at[src], xmod.at[src], xm_s.at[k], xm_r.at[k], device_id={"tp": src}, device_id_type=MESH)
        return pltpu.make_async_remote_copy(xmod.at[t], xmod.at[t], xm_s.at[k], xm_r.at[k], device_id={"tp": lax.rem(t + k, nt)}, device_id_type=MESH)

    order = sorted(range(1, nz), key=lambda k: -min(k, nz - k))
    for k in order:
        zm(k, False).start()
    loads[0].wait()
    lat_ring = Gather(nx, chip, along_x,
                      [lambda p, c: lat.at[2 * p + c, :, pl.ds(0, half)], lambda p, c: lat.at[2 * p + c, :, pl.ds(half, half)]],
                      lat_x, partner, core)
    lat_ring.start()
    loads[1].wait()
    quarter = half // 2
    at_half = lambda c, q: pl.ds(pl.multiple_of(c * half + q * quarter, 128), quarter)
    ctx_ring = Gather(nz, z, along_z,
                      [lambda p, c: ctx.at[p, :, at_half(c, 0)], lambda p, c: ctx.at[p, :, at_half(c, 1)]],
                      ctx_z, partner, core)
    for ch in range(2):
        for d in range(2):
            ctx_ring.ring_copy(d, 0, ch).start()

    for load in loads[2:]:
        load.wait()
    steps = 8
    depth = width // steps
    for i in range(steps):
        cut = pl.ds(i * depth, depth)
        wcat[cut, :] = jnp.concatenate([wq[cut, :], wkv[cut, :], wr[cut, :]], axis=1)
    uqT[...] = uq[...].astype(F32).T.astype(BF)
    ukvT[0:2 * PLAIN, :] = uk[...].astype(F32).T.astype(BF)
    ukvT[2 * PLAIN:2 * PLAIN + VROWS, :] = uv[...].astype(F32).T.astype(BF)
    q_gain = jnp.broadcast_to(qg_ref[...], (8, qg_ref.shape[1])).T[:, 0:1]
    kv_gain = jnp.broadcast_to(kg_ref[...], (8, kg_ref.shape[1])).T[:, 0:1]
    pos = lax.broadcasted_iota(jnp.int32, (8, tok), 1) + z * tok
    freq = jnp.exp(lax.broadcasted_iota(jnp.int32, (8, tok), 0).astype(F32) * (-math.log(10000.0) / 8))
    row_angle = (pos >> 6).astype(F32) * freq
    col_angle = (pos & (GRID_W - 1)).astype(F32) * freq
    turn = (jnp.cos(row_angle), jnp.sin(row_angle), jnp.cos(col_angle), jnp.sin(col_angle))

    for k in reversed(order):
        zm(k, True).wait_recv()
    total = zmod[0]
    for k in range(1, nz):
        total = total + zmod[k]
    xmod[t] = total
    for k in range(1, nt):
        xm(k, False).start()

    def ctx_step(s):
        for ch in range(2):
            for d in range(2):
                if ctx_ring.active(d, s, ch):
                    ctx_ring.ring_arrival(d, s, ch).wait_recv()
                    if ctx_ring.active(d, s + 1, ch):
                        ctx_ring.ring_copy(d, s, ch).start()
                    ctx_ring.pair_copy(d, s, ch, core).start()

    steps_z = list(range(1, ctx_ring.reach + 1))
    for s in range(1, lat_ring.reach + 1):
        lat_ring.step(s)
        for _ in range(1):
            if steps_z:
                ctx_step(steps_z.pop(0))
    for s in range(0, lat_ring.reach + 1):
        lat_ring.pair_step(s)
    for k in range(1, nt):
        xm(k, True).wait_recv()
    for j in range(nt):
        mod[:, j * part:(j + 1) * part] = xmod[j]

    @pl.loop(0, nt // 2)
    def _(i):
        block = jnp.concatenate([lat[2 * i].astype(F32), lat[2 * i + 1].astype(F32)], axis=0)
        at = pl.ds(pl.multiple_of(i * 2 * rows, 2 * rows), 2 * rows)
        h[at, :] = modulated(block, mod[0:1, :], mod[2:3, :])

    raw = jnp.dot(h[...], wcat[...], preferred_element_type=F32).T
    q_at = lambda p, c, i: pl.ds(pl.multiple_of((2 * p + c) * rank_q + i * (rank_q // 2), rank_q // 2), rank_q // 2)
    kv_at = lambda p, c: pl.ds(pl.multiple_of((2 * p + c) * rank_kv, rank_kv), rank_kv)
    qraw[pl.ds(pl.multiple_of(t * rank_q, rank_q), rank_q), :] = raw[0:rank_q].astype(BF)
    kvraw[kv_at(chip, core), :] = raw[rank_q:rank_q + rank_kv].astype(BF)
    raw_ring = Gather(nx, chip, along_x,
                      [lambda p, c: kvraw.at[kv_at(p, c), :], lambda p, c: qraw.at[q_at(p, c, 0), :], lambda p, c: qraw.at[q_at(p, c, 1), :]],
                      raw_x, partner, core)
    raw_ring.start()
    kv[z, 2 * PLAIN:KROWS, :] = axial_turn(raw[rank_q + rank_kv:], *turn).astype(BF)

    for s in range(1, raw_ring.reach + 1):
        raw_ring.step(s)
        if steps_z:
            ctx_step(steps_z.pop(0))
    for s in range(0, raw_ring.reach + 1):
        raw_ring.pair_step(s)

    ckv = rms_columns(kvraw[...], kv_gain)
    own = jnp.dot(ukvT[...], ckv, preferred_element_type=F32).astype(BF)
    kv[z, 0:2 * PLAIN, :] = own[0:2 * PLAIN]
    kv[z, KROWS:KROWS + VROWS, :] = own[2 * PLAIN:]
    kv_half = (KROWS + VROWS) // 2
    kv_ring = Gather(nz, z, along_z, [lambda p, c: kv.at[p, pl.ds(0, kv_half)], lambda p, c: kv.at[p, pl.ds(kv_half, kv_half)]], kv_z)
    while steps_z:
        ctx_step(steps_z.pop(0))
    kv_ring.start()

    cq = rms_columns(qraw[...], q_gain)
    q = jnp.dot(uqT[...], cq, preferred_element_type=F32)
    per = PLAIN + ROTARY
    for head in range(2):
        mine = q[head * per:(head + 1) * per]
        plain = mine[0:PLAIN].astype(BF)
        blank = jnp.zeros_like(plain)
        qb[head, head * PLAIN:(head + 1) * PLAIN, :] = plain
        qb[head, (1 - head) * PLAIN:(2 - head) * PLAIN, :] = blank
        qb[head, 2 * PLAIN:KROWS, :] = axial_turn(mine[PLAIN:], *turn).astype(BF)
    m_ref[...] = jnp.full_like(m_ref, NEGATIVE)
    l_ref[...] = jnp.zeros_like(l_ref)
    acc[...] = jnp.zeros_like(acc)

    def attend(keysT, valuesT, biased):
        keys = keysT.astype(F32).T.astype(BF)
        for head in range(2):
            s = jnp.dot(keys, qb[head], preferred_element_type=F32) * (SCORE * LOG2E)
            if biased:
                s = s + bias_ref[0, head] * LOG2E
            old = m_ref[head]
            new = jnp.maximum(old, jnp.max(s, axis=0, keepdims=True))
            alpha = jnp.exp2(old - new)
            e = jnp.exp2(s - new)
            m_ref[head] = new
            l_ref[head] = l_ref[head] * alpha + jnp.sum(e, axis=0, keepdims=True)
            acc[head] = acc[head] * alpha + jnp.dot(valuesT[head * VALUE:(head + 1) * VALUE], e.astype(BF), preferred_element_type=F32)

    for s in range(1, ctx_ring.reach + 1):
        ctx_ring.pair_step(s)

    @pl.loop(0, nz)
    def _(i):
        at = pl.ds(pl.multiple_of(i * crows, crows), crows)
        hc[at, :] = modulated(ctx[i], mod[1:2, :], mod[3:4, :])

    rawc = jnp.dot(hc[...], wcat[...], preferred_element_type=F32).T
    kvcraw[kv_at(chip, core), :] = rawc[rank_q:rank_q + rank_kv].astype(BF)
    chalf = kvcraw.shape[1] // 2
    rawc_ring = Gather(nx, chip, along_x,
                       [lambda p, c: kvcraw.at[kv_at(p, c), pl.ds(0, chalf)], lambda p, c: kvcraw.at[kv_at(p, c), pl.ds(chalf, chalf)]],
                       rawc_x, partner, core)
    rawc_ring.start()
    kvc[2 * PLAIN:KROWS, :] = rawc[rank_q + rank_kv:].astype(BF)

    attend(kv[z, 0:KROWS, :], kv[z, KROWS:KROWS + VROWS, :], False)
    reach = kv_ring.reach

    def ring_source(d, s):
        return lax.rem(z + jnp.where(d == 0, nz - s, s), nz)

    def arrive(d, s, ch):
        piece = kv.at[ring_source(d, s), pl.ds(ch * kv_half, kv_half)]
        return pltpu.make_async_remote_copy(piece, piece, kv_z[1].at[d, s, ch], kv_z[0].at[d, s, ch],
                                            device_id=along_z(jnp.where(d == 0, nz - 1, 1)), device_id_type=MESH)

    def forward(d, s, ch):
        piece = kv.at[ring_source(d, s), pl.ds(ch * kv_half, kv_half)]
        return pltpu.make_async_remote_copy(piece, piece, kv_z[1].at[d, s, ch], kv_z[0].at[d, s + 1, ch],
                                            device_id=along_z(jnp.where(d == 0, 1, nz - 1)), device_id_type=MESH)

    def take(k, waits_only_last):
        s = (k + 1) // 2
        d = 1 - lax.rem(k, 2)
        if waits_only_last:
            kv_ring.ring_arrival(0, reach, 0).wait_recv()
            kv_ring.ring_arrival(1, reach, 1).wait_recv()
        else:
            for ch in range(2):
                arrive(d, s, ch).wait_recv()

                @pl.when((s + 1 < reach) | ((s + 1 == reach) & (d == ch)))
                def _():
                    forward(d, s, ch).start()
        b = ring_source(d, s)
        attend(kv[b, 0:KROWS, :], kv[b, KROWS:KROWS + VROWS, :], False)

    split = min(2 * reach - 1, 2 * rawc_ring.reach + 1)

    def early(k, carry):
        take(k, False)
        return carry

    for s in range(1, rawc_ring.reach + 1):
        rawc_ring.step(s)
    for s in range(0, rawc_ring.reach + 1):
        rawc_ring.pair_step(s)
    lax.fori_loop(1, 2 * reach - 1, early, 0)
    ckvc = rms_columns(kvcraw[...], kv_gain)
    ownc = jnp.dot(ukvT[...], ckvc, preferred_element_type=F32).astype(BF)
    kvc[0:2 * PLAIN, :] = ownc[0:2 * PLAIN]
    kvc[KROWS:KROWS + VROWS, :] = ownc[2 * PLAIN:]
    attend(kvc[0:KROWS, :], kvc[KROWS:KROWS + VROWS, :], True)
    take(2 * reach - 1, True)

    outT = jnp.concatenate([acc[0] / l_ref[0], acc[1] / l_ref[1]], axis=0)
    mine_at = lambda p, c: pl.ds(pl.multiple_of((2 * p + c) * VROWS, VROWS), VROWS)
    att[:, mine_at(chip, core)] = outT.T.astype(BF)
    thalf = tok // 2
    att_ring = Gather(nx, chip, along_x,
                      [lambda p, c: att.at[pl.ds(0, thalf), mine_at(p, c)], lambda p, c: att.at[pl.ds(thalf, thalf), mine_at(p, c)]],
                      att_x, partner, core)
    att_ring.start()
    for s in range(1, att_ring.reach + 1):
        att_ring.step(s)

    def am(k, incoming):
        far = lax.rem(t + nt - k, nt) if incoming else lax.rem(t + k, nt)
        if incoming:
            return pltpu.make_async_remote_copy(pbuf.at[far], mbuf.at[far], a_s.at[k], a_r.at[k], device_id={"tp": far}, device_id_type=MESH)
        return pltpu.make_async_remote_copy(pbuf.at[far], mbuf.at[t], a_s.at[k], a_r.at[k], device_id={"tp": far}, device_id_type=MESH)

    for s in range(0, att_ring.reach + 1):
        att_ring.pair_step(s)
    proj = jnp.dot(att[...], wo[...], preferred_element_type=F32)
    for j in range(nt):
        pbuf[j] = proj[j * rows:(j + 1) * rows].astype(BF)
    for k in sorted(range(1, nt), key=lambda k: -min(k, nt - k)):
        am(k, False).start()
    mbuf[t] = pbuf[t]
    for k in range(1, nt):
        am(k, True).wait_recv()
    for j in range(nt):
        cut = slice(j * part, (j + 1) * part)
        out_ref[:, cut] = (own_lat[:, cut].astype(F32) + mod[4:5, cut] * mbuf[j].astype(F32)).astype(BF)

    for k in range(1, nz):
        zm(k, False).wait_send()
    for k in range(1, nt):
        xm(k, False).wait_send()
        am(k, False).wait_send()
    lat_ring.finish()
    for s in range(ctx_ring.reach + 1):
        for ch in range(2):
            for d in range(2):
                if ctx_ring.active(d, s + 1, ch):
                    ctx_ring.ring_copy(d, s, ch).wait_send()
                if s > 0 and ctx_ring.active(d, s, ch):
                    ctx_ring.pair_copy(d, s, ch, core).wait_send()
    raw_ring.finish()
    rawc_ring.finish()
    kv_ring.finish()
    att_ring.finish()


def sems(count, chunks, paired):
    kinds = 4 if paired else 2
    return tuple(pltpu.SemaphoreType.DMA((2, count // 2 + 2, chunks)) for _ in range(kinds))


def on_device(latents, conditions, context, w_shift, w_scale, w_gate, w_qdown, w_kvdown, w_rope, q_gain,
              latent_norm_gain, query_up_weight, key_up_weight, value_up_weight, context_bias, w_out):
    nz, nt = lax.axis_size("sp"), lax.axis_size("tp")
    nx = nt // 2
    rows, width = latents.shape
    tok = rows * nt
    crows = context.shape[0]
    rank_q, rank_kv = w_qdown.shape[1], w_kvdown.shape[1]
    part = width // nt
    vm = pltpu.VMEM
    dma = pltpu.SemaphoreType.DMA
    scratch = [
        vm((nt, rows, width), BF), vm((nz, crows, width), BF), vm((rows, width), BF),
        vm(w_qdown.shape, BF), vm(w_kvdown.shape, BF), vm(w_rope.shape, BF), vm(query_up_weight.shape, BF),
        vm(key_up_weight.shape, BF), vm(value_up_weight.shape, BF), vm(w_out.shape, BF),
        vm((width, rank_q + rank_kv + ROTARY), BF), vm(query_up_weight.shape[::-1], BF), vm((2 * PLAIN + VROWS, nt * rank_kv), BF),
        vm((nz, 8, part), F32), vm((nt, 8, part), F32), vm((8, width), F32),
        vm((tok, width), BF), vm((nz * crows, width), BF),
        vm((nt * rank_q, tok), BF), vm((nt * rank_kv, tok), BF), vm((nt * rank_kv, nz * crows), BF),
        vm((nz, KROWS + VROWS, tok), BF), vm((KROWS + VROWS, nz * crows), BF), vm((2, KROWS, tok), BF),
        vm((2, 1, tok), F32), vm((2, 1, tok), F32), vm((2, VALUE, tok), F32),
        vm((tok, nt * VROWS), BF), vm((nt, rows, part), BF), vm((nt, rows, part), BF),
        dma((10,)), dma((nz,)), dma((nz,)), dma((nt,)), dma((nt,)), dma((nt,)), dma((nt,)),
        sems(nx, 2, True), sems(nz, 2, True), sems(nx, 3, True), sems(nx, 2, True), sems(nz, 2, False), sems(nx, 2, True),
    ]
    here = pl.BlockSpec(memory_space=vm)
    away = pl.BlockSpec(memory_space=pl.ANY)
    small = pl.BlockSpec(memory_space=pltpu.SMEM)
    return pl.pallas_call(
        functools.partial(kernel, nz, nt),
        out_shape=jax.ShapeDtypeStruct((rows, width), BF),
        in_specs=[away, here, away, here, here, here, away, away, away, here, here, away, away, away, small, away],
        out_specs=here,
        scratch_shapes=scratch,
        compiler_params=pltpu.CompilerParams(collective_id=0, has_side_effects=True, vmem_limit_bytes=60 * 1024 * 1024),
        name="block",
    )(latents, conditions, context, w_shift, w_scale, w_gate, w_qdown, w_kvdown, w_rope, q_gain.reshape(1, -1),
      latent_norm_gain.reshape(1, -1), query_up_weight, key_up_weight, value_up_weight, context_bias.reshape(1, -1), w_out)


def solution(mesh):
    in_specs = (
        P(("grp", "sp", "tp"), None),
        P("grp", "sp"),
        P(("grp", "sp"), None),
        P("sp", "tp"),
        P("sp", "tp"),
        P("sp", "tp"),
        P(None, "tp"),
        P(None, "tp"),
        P(),
        P(),
        P(),
        P(None, "tp"),
        P(None, "tp"),
        P(None, "tp"),
        P("tp"),
        P(None, "tp"),
    )
    return jax.shard_map(on_device, mesh=mesh, in_specs=in_specs, out_specs=P(("grp", "sp", "tp"), None), check_vma=False)
```

```python
import functools
import math

import jax
import jax.numpy as jnp
from jax import lax
from jax.experimental import pallas as pl
from jax.experimental.pallas import tpu as pltpu
from jax.sharding import PartitionSpec as P

PLAIN = 64
ROTARY = 32
VALUE = 64
GRID_W = 64
EPSILON = 1e-6
NEGATIVE = -1e30
LOG2E = 1.4426950408889634
SCORE = (PLAIN + ROTARY) ** (-0.5)
MESH = pl.DeviceIdType.MESH
BF = jnp.bfloat16
F32 = jnp.float32
KROWS = 2 * PLAIN + ROTARY
VROWS = 2 * VALUE


class Gather:
    def __init__(self, count, place, towards, chunks, sems, partner=None, core=0):
        self.count, self.place, self.towards = count, place, towards
        self.chunks, self.partner, self.core = chunks, partner, core
        self.recv, self.send = sems[0], sems[1]
        self.pair_recv, self.pair_send = (sems[2], sems[3]) if partner is not None else (None, None)
        self.reach = count // 2
        self.cut = (len(chunks) + 1) // 2

    def active(self, d, s, ch):
        if s < self.reach:
            return True
        if s > self.reach:
            return False
        return (ch < self.cut) if d == 0 else (ch >= self.cut)

    def source(self, d, s):
        move = (self.count - s) if d == 0 else s
        return lax.rem(self.place + move, self.count)

    def ring_copy(self, d, s, ch):
        piece = self.chunks[ch](self.source(d, s), self.core)
        return pltpu.make_async_remote_copy(
            src_ref=piece, dst_ref=piece, send_sem=self.send.at[d, s, ch], recv_sem=self.recv.at[d, s + 1, ch],
            device_id=self.towards(1 if d == 0 else self.count - 1), device_id_type=MESH)

    def ring_arrival(self, d, s, ch):
        piece = self.chunks[ch](self.source(d, s), self.core)
        return pltpu.make_async_remote_copy(
            src_ref=piece, dst_ref=piece, send_sem=self.send.at[d, s, ch], recv_sem=self.recv.at[d, s, ch],
            device_id=self.towards(self.count - 1 if d == 0 else 1), device_id_type=MESH)

    def pair_copy(self, d, s, ch, core):
        piece = self.chunks[ch](self.source(d, s), core)
        return pltpu.make_async_remote_copy(
            src_ref=piece, dst_ref=piece, send_sem=self.pair_send.at[d, s, ch], recv_sem=self.pair_recv.at[d, s, ch],
            device_id=self.partner, device_id_type=MESH)

    def start(self, only=None):
        for ch in range(len(self.chunks)) if only is None else only:
            for d in range(2):
                if self.active(d, 1, ch):
                    self.ring_copy(d, 0, ch).start()
            if self.partner is not None:
                self.pair_copy(0, 0, ch, self.core).start()

    def step(self, s):
        for ch in range(len(self.chunks)):
            for d in range(2):
                if self.active(d, s, ch):
                    self.ring_arrival(d, s, ch).wait_recv()
                    if self.active(d, s + 1, ch):
                        self.ring_copy(d, s, ch).start()
                    if self.partner is not None:
                        self.pair_copy(d, s, ch, self.core).start()

    def pair_step(self, s, only=None):
        for ch in range(len(self.chunks)) if only is None else only:
            for d in range(2):
                if (s == 0 and d == 0) or (s > 0 and self.active(d, s, ch)):
                    self.pair_copy(d, s, ch, 1 - self.core).wait_recv()

    def finish(self):
        for s in range(self.reach + 1):
            for ch in range(len(self.chunks)):
                for d in range(2):
                    if self.active(d, s + 1, ch):
                        self.ring_copy(d, s, ch).wait_send()
                    if self.partner is not None and ((s == 0 and d == 0) or (s > 0 and self.active(d, s, ch))):
                        self.pair_copy(d, s, ch, self.core).wait_send()


def axial_turn(a, row_cos, row_sin, col_cos, col_sin):
    a0, a1, a2, a3 = a[0:8], a[8:16], a[16:24], a[24:32]
    return jnp.concatenate(
        [a0 * row_cos - a1 * row_sin, a0 * row_sin + a1 * row_cos,
         a2 * col_cos - a3 * col_sin, a2 * col_sin + a3 * col_cos], axis=0)


def modulated(block, shift, scale):
    values = block.astype(F32)
    center = values - jnp.mean(values, axis=-1, keepdims=True)
    spread = jnp.mean(center * center, axis=-1, keepdims=True)
    return (center * lax.rsqrt(spread + EPSILON) * (1.0 + scale) + shift).astype(BF)


def rms_columns(raw, gain):
    values = raw.astype(F32)
    factor = lax.rsqrt(jnp.mean(values * values, axis=0, keepdims=True) + EPSILON)
    return (values * factor * gain).astype(BF)


def kernel(nz, nt, *refs):
    (lat_hbm, cond_ref, ctx_hbm, wsh_ref, wsc_ref, wg_ref, wq_hbm, wkv_hbm, wr_hbm, qg_ref, kg_ref,
     uq_hbm, uk_hbm, uv_hbm, bias_ref, wo_hbm, proj_ref, gate_ref,
     lat, ctx, mean_ref, rstd_ref, uk, uv, wo,
     wcat, uqT, ukvT, zmod, xmod, mod, h, hc, qraw, kvraw, kvcraw, kv, kvc, qb,
     m_ref, l_ref, acc, att, pbuf, mbuf, q_gain_ref, kv_gain_ref,
     load_sem, zm_s, zm_r, xm_s, xm_r, a_s, a_r, lat_x, ctx_z, raw_x, rawc_x, kv_z, att_x) = refs
    z, t = lax.axis_index("sp"), lax.axis_index("tp")
    core = lax.rem(t, 2)
    chip = t // 2
    nx = nt // 2
    rows = lat.shape[1]
    tok = rows * nt
    crows = ctx.shape[1]
    width = lat.shape[2]
    part = width // nt
    rank_q, rank_kv = wq_hbm.shape[0], wkv_hbm.shape[0]
    along_z = lambda k: {"sp": lax.rem(z + k, nz)}
    along_x = lambda k: {"tp": lax.rem(t + 2 * k, nt)}
    partner = {"tp": t + 1 - 2 * core}
    half = width // 2

    loads = [
        pltpu.make_async_copy(lat_hbm, lat.at[t], load_sem.at[0]),
        pltpu.make_async_copy(ctx_hbm, ctx.at[z], load_sem.at[1]),
        pltpu.make_async_copy(wq_hbm, wcat.at[pl.ds(0, rank_q)], load_sem.at[2]),
        pltpu.make_async_copy(wkv_hbm, wcat.at[pl.ds(rank_q, rank_kv)], load_sem.at[3]),
        pltpu.make_async_copy(wr_hbm, wcat.at[pl.ds(rank_q + rank_kv, ROTARY)], load_sem.at[4]),
        pltpu.make_async_copy(uq_hbm, uqT, load_sem.at[5]),
        pltpu.make_async_copy(uk_hbm, uk, load_sem.at[6]),
        pltpu.make_async_copy(uv_hbm, uv, load_sem.at[7]),
        pltpu.make_async_copy(wo_hbm, wo, load_sem.at[8]),
    ]
    barrier = pltpu.get_barrier_semaphore()
    for k in range(1, nz):
        pl.semaphore_signal(barrier, inc=1, device_id=along_z(k), device_id_type=MESH)
    for k in range(1, nt):
        pl.semaphore_signal(barrier, inc=1, device_id={"tp": lax.rem(t + k, nt)}, device_id_type=MESH)
    for load in loads:
        load.start()

    cond = cond_ref[...]
    act = cond / (1.0 + jnp.exp(-cond))
    act = jnp.concatenate([act, jnp.zeros((14, act.shape[1]), F32)], axis=0).astype(BF)
    shift_part = jnp.dot(act, wsh_ref[...], preferred_element_type=F32)
    scale_part = jnp.dot(act, wsc_ref[...], preferred_element_type=F32)
    gate_part = jnp.dot(act, wg_ref[...], preferred_element_type=F32)
    zmod[z] = jnp.concatenate([shift_part[0:2], scale_part[0:2], gate_part[0:2], gate_part[2:4]], axis=0)
    pl.semaphore_wait(barrier, nz + nt - 2)

    def zm(k, incoming):
        if incoming:
            src = lax.rem(z + nz - k, nz)
            return pltpu.make_async_remote_copy(zmod.at[src], zmod.at[src], zm_s.at[k], zm_r.at[k], device_id=along_z(nz - k), device_id_type=MESH)
        return pltpu.make_async_remote_copy(zmod.at[z], zmod.at[z], zm_s.at[k], zm_r.at[k], device_id=along_z(k), device_id_type=MESH)

    def xm(k, incoming):
        if incoming:
            src = lax.rem(t + nt - k, nt)
            return pltpu.make_async_remote_copy(xmod.at[src], xmod.at[src], xm_s.at[k], xm_r.at[k], device_id={"tp": src}, device_id_type=MESH)
        return pltpu.make_async_remote_copy(xmod.at[t], xmod.at[t], xm_s.at[k], xm_r.at[k], device_id={"tp": lax.rem(t + k, nt)}, device_id_type=MESH)

    order = sorted(range(1, nz), key=lambda k: -min(k, nz - k))
    for k in order:
        zm(k, False).start()
    loads[0].wait()
    lat_ring = Gather(nx, chip, along_x,
                      [lambda p, c: lat.at[2 * p + c, :, pl.ds(0, half)], lambda p, c: lat.at[2 * p + c, :, pl.ds(half, half)]],
                      lat_x, partner, core)
    lat_ring.start()
    loads[1].wait()
    quarter = half // 2
    at_half = lambda c, q: pl.ds(pl.multiple_of(c * half + q * quarter, 128), quarter)
    ctx_ring = Gather(nz, z, along_z,
                      [lambda p, c: ctx.at[p, :, at_half(c, 0)], lambda p, c: ctx.at[p, :, at_half(c, 1)]],
                      ctx_z, partner, core)
    for ch in range(2):
        for d in range(2):
            ctx_ring.ring_copy(d, 0, ch).start()

    for load in loads[2:]:
        load.wait()
    ukvT[0:2 * PLAIN, :] = uk[...].astype(F32).T.astype(BF)
    ukvT[2 * PLAIN:2 * PLAIN + VROWS, :] = uv[...].astype(F32).T.astype(BF)
    q_gain_ref[...] = jnp.broadcast_to(qg_ref[...], (8, qg_ref.shape[1])).T[:, 0:1]
    kv_gain_ref[...] = jnp.broadcast_to(kg_ref[...], (8, kg_ref.shape[1])).T[:, 0:1]
    pos = lax.broadcasted_iota(jnp.int32, (8, tok), 1) + z * tok
    freq = jnp.exp(lax.broadcasted_iota(jnp.int32, (8, tok), 0).astype(F32) * (-math.log(10000.0) / 8))
    row_angle = (pos >> 6).astype(F32) * freq
    col_angle = (pos & (GRID_W - 1)).astype(F32) * freq
    turn = (jnp.cos(row_angle), jnp.sin(row_angle), jnp.cos(col_angle), jnp.sin(col_angle))

    def ctx_step(s):
        for ch in range(2):
            for d in range(2):
                if ctx_ring.active(d, s, ch):
                    ctx_ring.ring_arrival(d, s, ch).wait_recv()
                    if ctx_ring.active(d, s + 1, ch):
                        ctx_ring.ring_copy(d, s, ch).start()
                    ctx_ring.pair_copy(d, s, ch, core).start()

    steps_z = list(range(1, ctx_ring.reach + 1))

    def ctx_next(least=0):
        if len(steps_z) > least:
            ctx_step(steps_z.pop(0))

    def chip_rows(p):
        return jnp.concatenate([lat[2 * p].astype(F32), lat[2 * p + 1].astype(F32)], axis=0)

    def note_statistics(p):
        values = chip_rows(p)
        center = values - jnp.mean(values, axis=-1, keepdims=True)
        mean_ref[p] = jnp.mean(values, axis=-1, keepdims=True)
        rstd_ref[p] = lax.rsqrt(jnp.mean(center * center, axis=-1, keepdims=True) + EPSILON)

    lat_ring.step(1)
    ctx_next()
    for k in reversed(order):
        zm(k, True).wait_recv()
    total = zmod[0]
    for k in range(1, nz):
        total = total + zmod[k]
    xmod[t] = total
    for k in range(1, nt):
        xm(k, False).start()
    far = lat_ring.reach
    for s in range(2, far + 1):
        lat_ring.pair_step(s - 2)

        @pl.loop(0, 1 if s == 2 else 2)
        def _(i):
            note_statistics(lax.rem(chip + jnp.where(i == 0, nx - (s - 2), s - 2), nx))

        lat_ring.step(s)
        ctx_next()
    lat_ring.pair_step(far - 1)

    @pl.loop(0, 2 if far > 1 else 1)
    def _(i):
        note_statistics(lax.rem(chip + jnp.where(i == 0, nx - (far - 1), far - 1), nx))

    lat_ring.pair_step(far)
    note_statistics(lax.rem(chip + far, nx))
    for k in range(1, nt):
        xm(k, True).wait_recv()
    for j in range(nt):
        mod[:, j * part:(j + 1) * part] = xmod[j]

    for piece in range(2):
        @pl.loop(piece * nx // 2, (piece + 1) * nx // 2)
        def _(p):
            at = pl.ds(pl.multiple_of(p * 2 * rows, 2 * rows), 2 * rows)
            normed = (chip_rows(p) - mean_ref[p]) * rstd_ref[p]
            h[at, :] = (normed * (1.0 + mod[2:3, :]) + mod[0:1, :]).astype(BF)
        ctx_next()

    raw = lax.dot_general(h[...], wcat[...], (((1,), (1,)), ((), ())), preferred_element_type=F32).T
    q_at = lambda p, c, i: pl.ds(pl.multiple_of((2 * p + c) * rank_q + i * (rank_q // 2), rank_q // 2), rank_q // 2)
    kv_at = lambda p, c: pl.ds(pl.multiple_of((2 * p + c) * rank_kv, rank_kv), rank_kv)
    qraw[pl.ds(pl.multiple_of(t * rank_q, rank_q), rank_q), :] = raw[0:rank_q].astype(BF)
    kvraw[kv_at(chip, core), :] = raw[rank_q:rank_q + rank_kv].astype(BF)
    raw_ring = Gather(nx, chip, along_x,
                      [lambda p, c: kvraw.at[kv_at(p, c), :], lambda p, c: qraw.at[q_at(p, c, 0), :], lambda p, c: qraw.at[q_at(p, c, 1), :]],
                      raw_x, partner, core)
    raw_ring.start()
    kv[z, 2 * PLAIN:KROWS, :] = axial_turn(raw[rank_q + rank_kv:], *turn).astype(BF)

    for s in range(1, raw_ring.reach + 1):
        raw_ring.step(s)
        if s == 2:
            ctx_next(1)
    for s in range(0, raw_ring.reach + 1):
        raw_ring.pair_step(s)

    ckv = rms_columns(kvraw[...], kv_gain_ref[...])
    own = jnp.dot(ukvT[...], ckv, preferred_element_type=F32).astype(BF)
    kv[z, 0:2 * PLAIN, :] = own[0:2 * PLAIN]
    kv[z, KROWS:KROWS + VROWS, :] = own[2 * PLAIN:]
    kv_half = (KROWS + VROWS) // 2
    kv_ring = Gather(nz, z, along_z, [lambda p, c: kv.at[p, pl.ds(0, kv_half)], lambda p, c: kv.at[p, pl.ds(kv_half, kv_half)]], kv_z)
    kv_ring.start()
    while len(steps_z) > 1:
        ctx_next()

    cq = rms_columns(qraw[...], q_gain_ref[...])
    q = jnp.dot(uqT[...], cq, preferred_element_type=F32)
    per = PLAIN + ROTARY
    for head in range(2):
        mine = q[head * per:(head + 1) * per]
        plain = mine[0:PLAIN].astype(BF)
        blank = jnp.zeros_like(plain)
        qb[head, head * PLAIN:(head + 1) * PLAIN, :] = plain
        qb[head, (1 - head) * PLAIN:(2 - head) * PLAIN, :] = blank
        qb[head, 2 * PLAIN:KROWS, :] = axial_turn(mine[PLAIN:], *turn).astype(BF)
    m_ref[...] = jnp.full_like(m_ref, NEGATIVE)
    l_ref[...] = jnp.zeros_like(l_ref)
    acc[...] = jnp.zeros_like(acc)

    def attend(keysT, valuesT, biased):
        keys = keysT.astype(F32).T.astype(BF)
        for head in range(2):
            s = jnp.dot(keys, qb[head], preferred_element_type=F32) * (SCORE * LOG2E)
            if biased:
                s = s + bias_ref[0, head] * LOG2E
            old = m_ref[head]
            new = jnp.maximum(old, jnp.max(s, axis=0, keepdims=True))
            alpha = jnp.exp2(old - new)
            e = jnp.exp2(s - new)
            m_ref[head] = new
            l_ref[head] = l_ref[head] * alpha + jnp.sum(e, axis=0, keepdims=True)
            acc[head] = acc[head] * alpha + jnp.dot(valuesT[head * VALUE:(head + 1) * VALUE], e.astype(BF), preferred_element_type=F32)

    attend(kv[z, 0:KROWS, :], kv[z, KROWS:KROWS + VROWS, :], False)
    while steps_z:
        ctx_next()
    for s in range(1, ctx_ring.reach + 1):
        ctx_ring.pair_step(s)
    chalf = kvcraw.shape[1] // 2
    rawc_ring = Gather(nx, chip, along_x,
                       [lambda p, c: kvcraw.at[kv_at(p, c), pl.ds(0, chalf)], lambda p, c: kvcraw.at[kv_at(p, c), pl.ds(chalf, chalf)]],
                       rawc_x, partner, core)
    reach = kv_ring.reach

    def ring_source(d, s):
        return lax.rem(z + jnp.where(d == 0, nz - s, s), nz)

    def hop(d, s, ch, into):
        piece = kv.at[ring_source(d, s), pl.ds(ch * kv_half, kv_half)]
        return pltpu.make_async_remote_copy(piece, piece, kv_z[1].at[d, s, ch], kv_z[0].at[d, into, ch],
                                            device_id=along_z(1 if d == 0 else nz - 1), device_id_type=MESH)

    def pass_on(s, ch):
        for d in range(2):
            hop(d, s, ch, s).wait_recv()
        for d in range(2):
            if d == ch:
                hop(d, s, ch, s + 1).start()
            else:
                @pl.when(s + 1 < reach)
                def _():
                    hop(d, s, ch, s + 1).start()

    def attend_block(d, s):
        b = ring_source(d, s)
        attend(kv[b, 0:KROWS, :], kv[b, KROWS:KROWS + VROWS, :], False)

    def context_quarter(quarter):
        @pl.loop(quarter * nz // 4, (quarter + 1) * nz // 4)
        def _(i):
            at = pl.ds(pl.multiple_of(i * crows, crows), crows)
            hc[at, :] = modulated(ctx[i], mod[1:2, :], mod[3:4, :])

    def context_down():
        rawc = lax.dot_general(hc[...], wcat[...], (((1,), (1,)), ((), ())), preferred_element_type=F32).T
        kvcraw[kv_at(chip, core), :] = rawc[rank_q:rank_q + rank_kv].astype(BF)
        kvc[2 * PLAIN:KROWS, :] = rawc[rank_q + rank_kv:].astype(BF)
        rawc_ring.start()

    def context_up():
        for s in range(0, rawc_ring.reach + 1):
            rawc_ring.pair_step(s)
        ckvc = rms_columns(kvcraw[...], kv_gain_ref[...])
        ownc = jnp.dot(ukvT[...], ckvc, preferred_element_type=F32).astype(BF)
        kvc[0:2 * PLAIN, :] = ownc[0:2 * PLAIN]
        kvc[KROWS:KROWS + VROWS, :] = ownc[2 * PLAIN:]

    jobs = [functools.partial(context_quarter, i) for i in range(4)] + [context_down]
    jobs += [functools.partial(rawc_ring.step, s) for s in range(1, rawc_ring.reach + 1)] + [context_up]
    slots = 2 * (reach - 1)
    place = {}
    for i, job in enumerate(jobs):
        spare = i if i < 5 else 5 + 2 * (i - 5) + 1
        place.setdefault(min(spare, slots - 1), []).append(job)

    def do_jobs(slot, now):
        for at, work in place.items():
            if at % 2 == slot:
                @pl.when(now == at // 2 + 1)
                def _():
                    for job in work:
                        job()

    def kv_step(s, carry):
        pass_on(s, 0)

        @pl.when(s > 1)
        def _():
            attend_block(0, s - 1)
        do_jobs(0, s)
        pass_on(s, 1)

        @pl.when(s > 1)
        def _():
            attend_block(1, s - 1)
        do_jobs(1, s)
        return carry

    lax.fori_loop(1, reach, kv_step, 0)

    @pl.loop(0, 2)
    def _(d):
        attend_block(d, reach - 1)
    attend(kvc[0:KROWS, :], kvc[KROWS:KROWS + VROWS, :], True)
    kv_ring.ring_arrival(0, reach, 0).wait_recv()
    kv_ring.ring_arrival(1, reach, 1).wait_recv()
    attend_block(0, reach)

    outT = jnp.concatenate([acc[0] / l_ref[0], acc[1] / l_ref[1]], axis=0)
    mine_at = lambda p, c: pl.ds(pl.multiple_of((2 * p + c) * VROWS, VROWS), VROWS)
    att[:, mine_at(chip, core)] = outT.T.astype(BF)
    fourth = tok // 4
    att_ring = Gather(nx, chip, along_x,
                      [lambda p, c, i=i: att.at[pl.ds(i * fourth, fourth), mine_at(p, c)] for i in range(4)],
                      att_x, partner, core)
    att_ring.start()
    for s in range(1, att_ring.reach + 1):
        att_ring.step(s)

    def am(k, incoming):
        far = lax.rem(t + nt - k, nt) if incoming else lax.rem(t + k, nt)
        if incoming:
            return pltpu.make_async_remote_copy(pbuf.at[far], mbuf.at[far], a_s.at[k], a_r.at[k], device_id={"tp": far}, device_id_type=MESH)
        return pltpu.make_async_remote_copy(pbuf.at[far], mbuf.at[t], a_s.at[k], a_r.at[k], device_id={"tp": far}, device_id_type=MESH)

    for s in range(0, att_ring.reach + 1):
        att_ring.pair_step(s)
    proj = jnp.dot(att[...], wo[...], preferred_element_type=F32)
    for j in range(nt):
        pbuf[j] = proj[j * rows:(j + 1) * rows].astype(BF)
    for k in sorted(range(1, nt), key=lambda k: -min(k, nt - k)):
        am(k, False).start()
    mbuf[t] = pbuf[t]
    gate_ref[...] = mod[4:5, :]
    for k in range(1, nt):
        am(k, True).wait_recv()
    for j in range(nt):
        cut = slice(j * part, (j + 1) * part)
        proj_ref[:, cut] = mbuf[j]

    for k in range(1, nz):
        zm(k, False).wait_send()
    for k in range(1, nt):
        xm(k, False).wait_send()
        am(k, False).wait_send()
    lat_ring.finish()
    for s in range(ctx_ring.reach + 1):
        for ch in range(2):
            for d in range(2):
                if ctx_ring.active(d, s + 1, ch):
                    ctx_ring.ring_copy(d, s, ch).wait_send()
                if s > 0 and ctx_ring.active(d, s, ch):
                    ctx_ring.pair_copy(d, s, ch, core).wait_send()
    raw_ring.finish()
    rawc_ring.finish()
    kv_ring.finish()
    att_ring.finish()


def sems(count, chunks, paired):
    kinds = 4 if paired else 2
    return tuple(pltpu.SemaphoreType.DMA((2, count // 2 + 2, chunks)) for _ in range(kinds))


def on_device(latents, conditions, context, w_shift, w_scale, w_gate, w_qdown, w_kvdown, w_rope, q_gain,
              latent_norm_gain, query_up_weight, key_up_weight, value_up_weight, context_bias, w_out):
    nz, nt = lax.axis_size("sp"), lax.axis_size("tp")
    nx = nt // 2
    rows, width = latents.shape
    tok = rows * nt
    crows = context.shape[0]
    rank_q, rank_kv = w_qdown.shape[1], w_kvdown.shape[1]
    part = width // nt
    vm = pltpu.VMEM
    dma = pltpu.SemaphoreType.DMA
    scratch = [
        vm((nt, rows, width), BF), vm((nz, crows, width), BF), vm((nx, 2 * rows, 1), F32), vm((nx, 2 * rows, 1), F32),
        vm(key_up_weight.shape, BF), vm(value_up_weight.shape, BF), vm(w_out.shape, BF),
        vm((rank_q + rank_kv + ROTARY, width), BF), vm(query_up_weight.shape[::-1], BF), vm((2 * PLAIN + VROWS, nt * rank_kv), BF),
        vm((nz, 8, part), F32), vm((nt, 8, part), F32), vm((8, width), F32),
        vm((tok, width), BF), vm((nz * crows, width), BF),
        vm((nt * rank_q, tok), BF), vm((nt * rank_kv, tok), BF), vm((nt * rank_kv, nz * crows), BF),
        vm((nz, KROWS + VROWS, tok), BF), vm((KROWS + VROWS, nz * crows), BF), vm((2, KROWS, tok), BF),
        vm((2, 1, tok), F32), vm((2, 1, tok), F32), vm((2, VALUE, tok), F32),
        vm((tok, nt * VROWS), BF), vm((nt, rows, part), BF), vm((nt, rows, part), BF),
        vm((nt * rank_q, 1), F32), vm((nt * rank_kv, 1), F32),
        dma((9,)), dma((nz,)), dma((nz,)), dma((nt,)), dma((nt,)), dma((nt,)), dma((nt,)),
        sems(nx, 2, True), sems(nz, 2, True), sems(nx, 3, True), sems(nx, 2, True), sems(nz, 2, False), sems(nx, 4, True),
    ]
    here = pl.BlockSpec(memory_space=vm)
    away = pl.BlockSpec(memory_space=pl.ANY)
    small = pl.BlockSpec(memory_space=pltpu.SMEM)
    proj, gate = pl.pallas_call(
        functools.partial(kernel, nz, nt),
        out_shape=(jax.ShapeDtypeStruct((rows, width), BF), jax.ShapeDtypeStruct((1, width), F32)),
        in_specs=[away, here, away, here, here, here, away, away, away, here, here, away, away, away, small, away],
        out_specs=(here, here),
        scratch_shapes=scratch,
        compiler_params=pltpu.CompilerParams(collective_id=0, has_side_effects=True, vmem_limit_bytes=60 * 1024 * 1024),
        name="block",
    )(latents, conditions, context, w_shift, w_scale, w_gate, w_qdown.T, w_kvdown.T, w_rope.T, q_gain.reshape(1, -1),
      latent_norm_gain.reshape(1, -1), query_up_weight.T, key_up_weight, value_up_weight, context_bias.reshape(1, -1), w_out)
    return (latents.astype(F32) + gate * proj.astype(F32)).astype(BF)


def solution(mesh):
    in_specs = (
        P(("grp", "sp", "tp"), None),
        P("grp", "sp"),
        P(("grp", "sp"), None),
        P("sp", "tp"),
        P("sp", "tp"),
        P("sp", "tp"),
        P(None, "tp"),
        P(None, "tp"),
        P(),
        P(),
        P(),
        P(None, "tp"),
        P(None, "tp"),
        P(None, "tp"),
        P("tp"),
        P(None, "tp"),
    )
    return jax.shard_map(on_device, mesh=mesh, in_specs=in_specs, out_specs=P(("grp", "sp", "tp"), None), check_vma=False)
```

```python
import functools
import math

import jax
import jax.numpy as jnp
from jax import lax
from jax.experimental import pallas as pl
from jax.experimental.pallas import tpu as pltpu
from jax.sharding import PartitionSpec as P

PLAIN = 64
ROTARY = 32
VALUE = 64
GRID_W = 64
EPSILON = 1e-6
NEGATIVE = -1e30
LOG2E = 1.4426950408889634
SCORE = (PLAIN + ROTARY) ** (-0.5)
MESH = pl.DeviceIdType.MESH
BF = jnp.bfloat16
F32 = jnp.float32
KROWS = 2 * PLAIN + ROTARY
VROWS = 2 * VALUE


class Gather:
    def __init__(self, count, place, towards, chunks, sems, partner=None, core=0):
        self.count, self.place, self.towards = count, place, towards
        self.chunks, self.partner, self.core = chunks, partner, core
        self.recv, self.send = sems[0], sems[1]
        self.pair_recv, self.pair_send = (sems[2], sems[3]) if partner is not None else (None, None)
        self.reach = count // 2
        self.cut = (len(chunks) + 1) // 2

    def active(self, d, s, ch):
        if s < self.reach:
            return True
        if s > self.reach:
            return False
        return (ch < self.cut) if d == 0 else (ch >= self.cut)

    def source(self, d, s):
        move = (self.count - s) if d == 0 else s
        return lax.rem(self.place + move, self.count)

    def ring_copy(self, d, s, ch):
        piece = self.chunks[ch](self.source(d, s), self.core)
        return pltpu.make_async_remote_copy(
            src_ref=piece, dst_ref=piece, send_sem=self.send.at[d, s, ch], recv_sem=self.recv.at[d, s + 1, ch],
            device_id=self.towards(1 if d == 0 else self.count - 1), device_id_type=MESH)

    def ring_arrival(self, d, s, ch):
        piece = self.chunks[ch](self.source(d, s), self.core)
        return pltpu.make_async_remote_copy(
            src_ref=piece, dst_ref=piece, send_sem=self.send.at[d, s, ch], recv_sem=self.recv.at[d, s, ch],
            device_id=self.towards(self.count - 1 if d == 0 else 1), device_id_type=MESH)

    def pair_copy(self, d, s, ch, core):
        piece = self.chunks[ch](self.source(d, s), core)
        return pltpu.make_async_remote_copy(
            src_ref=piece, dst_ref=piece, send_sem=self.pair_send.at[d, s, ch], recv_sem=self.pair_recv.at[d, s, ch],
            device_id=self.partner, device_id_type=MESH)

    def start(self, only=None):
        for ch in range(len(self.chunks)) if only is None else only:
            for d in range(2):
                if self.active(d, 1, ch):
                    self.ring_copy(d, 0, ch).start()
            if self.partner is not None:
                self.pair_copy(0, 0, ch, self.core).start()

    def step(self, s):
        for ch in range(len(self.chunks)):
            for d in range(2):
                if self.active(d, s, ch):
                    self.ring_arrival(d, s, ch).wait_recv()
                    if self.active(d, s + 1, ch):
                        self.ring_copy(d, s, ch).start()
                    if self.partner is not None:
                        self.pair_copy(d, s, ch, self.core).start()

    def pair_step(self, s, only=None):
        for ch in range(len(self.chunks)) if only is None else only:
            for d in range(2):
                if (s == 0 and d == 0) or (s > 0 and self.active(d, s, ch)):
                    self.pair_copy(d, s, ch, 1 - self.core).wait_recv()

    def finish(self):
        for s in range(self.reach + 1):
            for ch in range(len(self.chunks)):
                for d in range(2):
                    if self.active(d, s + 1, ch):
                        self.ring_copy(d, s, ch).wait_send()
                    if self.partner is not None and ((s == 0 and d == 0) or (s > 0 and self.active(d, s, ch))):
                        self.pair_copy(d, s, ch, self.core).wait_send()


def axial_turn(a, row_cos, row_sin, col_cos, col_sin):
    a0, a1, a2, a3 = a[0:8], a[8:16], a[16:24], a[24:32]
    return jnp.concatenate(
        [a0 * row_cos - a1 * row_sin, a0 * row_sin + a1 * row_cos,
         a2 * col_cos - a3 * col_sin, a2 * col_sin + a3 * col_cos], axis=0)


def modulated(block, shift, scale):
    values = block.astype(F32)
    center = values - jnp.mean(values, axis=-1, keepdims=True)
    spread = jnp.mean(center * center, axis=-1, keepdims=True)
    return (center * lax.rsqrt(spread + EPSILON) * (1.0 + scale) + shift).astype(BF)


def rms_columns(raw, gain):
    values = raw.astype(F32)
    factor = lax.rsqrt(jnp.mean(values * values, axis=0, keepdims=True) + EPSILON)
    return (values * factor * gain).astype(BF)


def kernel(nz, nt, *refs):
    (lat_hbm, cond_ref, ctx_hbm, wsh_ref, wsc_ref, wg_ref, wq_hbm, wkv_hbm, wr_hbm, qg_ref, kg_ref,
     uq_hbm, uk_hbm, uv_hbm, bias_ref, wo_hbm, proj_ref, gate_ref,
     lat, ctx, mean_ref, rstd_ref, uk, uv, wo,
     wcat, uqT, ukvT, zmod, xmod, mod, h, qraw, kvraw, kv, kvp, kvc, qb,
     m_ref, l_ref, acc, att, pbuf, mbuf, q_gain_ref, kv_gain_ref, turn_ref,
     load_sem, zm_s, zm_r, xm_s, xm_r, a_s, a_r, lat_x, raw_x, q_x, kv_z, att_x) = refs
    z, t = lax.axis_index("sp"), lax.axis_index("tp")
    core = lax.rem(t, 2)
    chip = t // 2
    nx = nt // 2
    rows = lat.shape[1]
    tok = rows * nt
    crows = ctx.shape[0]
    width = lat.shape[2]
    part = width // nt
    rank_q, rank_kv = wq_hbm.shape[0], wkv_hbm.shape[0]
    along_z = lambda k: {"sp": lax.rem(z + k, nz)}
    along_x = lambda k: {"tp": lax.rem(t + 2 * k, nt)}
    partner = {"tp": t + 1 - 2 * core}
    half = width // 2

    loads = [
        pltpu.make_async_copy(lat_hbm, lat.at[t], load_sem.at[0]),
        pltpu.make_async_copy(ctx_hbm, ctx, load_sem.at[1]),
        pltpu.make_async_copy(wq_hbm, wcat.at[pl.ds(0, rank_q)], load_sem.at[2]),
        pltpu.make_async_copy(wkv_hbm, wcat.at[pl.ds(rank_q, rank_kv)], load_sem.at[3]),
        pltpu.make_async_copy(wr_hbm, wcat.at[pl.ds(rank_q + rank_kv, ROTARY)], load_sem.at[4]),
        pltpu.make_async_copy(uq_hbm, uqT, load_sem.at[5]),
        pltpu.make_async_copy(uk_hbm, uk, load_sem.at[6]),
        pltpu.make_async_copy(uv_hbm, uv, load_sem.at[7]),
        pltpu.make_async_copy(wo_hbm, wo, load_sem.at[8]),
    ]
    barrier = pltpu.get_barrier_semaphore()
    for k in range(1, nz):
        pl.semaphore_signal(barrier, inc=1, device_id=along_z(k), device_id_type=MESH)
    for k in range(1, nt):
        pl.semaphore_signal(barrier, inc=1, device_id={"tp": lax.rem(t + k, nt)}, device_id_type=MESH)
    for load in loads:
        load.start()

    cond = cond_ref[...]
    act = cond / (1.0 + jnp.exp(-cond))
    act = jnp.concatenate([act, jnp.zeros((14, act.shape[1]), F32)], axis=0).astype(BF)
    shift_part = jnp.dot(act, wsh_ref[...], preferred_element_type=F32)
    scale_part = jnp.dot(act, wsc_ref[...], preferred_element_type=F32)
    gate_part = jnp.dot(act, wg_ref[...], preferred_element_type=F32)
    zmod[z] = jnp.concatenate([shift_part[0:2], scale_part[0:2], gate_part[0:2], gate_part[2:4]], axis=0)
    pl.semaphore_wait(barrier, nz + nt - 2)

    def zm(k, incoming):
        if incoming:
            src = lax.rem(z + nz - k, nz)
            return pltpu.make_async_remote_copy(zmod.at[src], zmod.at[src], zm_s.at[k], zm_r.at[k], device_id=along_z(nz - k), device_id_type=MESH)
        return pltpu.make_async_remote_copy(zmod.at[z], zmod.at[z], zm_s.at[k], zm_r.at[k], device_id=along_z(k), device_id_type=MESH)

    def xm(k, incoming):
        if incoming:
            src = lax.rem(t + nt - k, nt)
            return pltpu.make_async_remote_copy(xmod.at[src], xmod.at[src], xm_s.at[k], xm_r.at[k], device_id={"tp": src}, device_id_type=MESH)
        return pltpu.make_async_remote_copy(xmod.at[t], xmod.at[t], xm_s.at[k], xm_r.at[k], device_id={"tp": lax.rem(t + k, nt)}, device_id_type=MESH)

    order = sorted(range(1, nz), key=lambda k: -min(k, nz - k))
    for k in order:
        zm(k, False).start()
    loads[0].wait()
    lat_ring = Gather(nx, chip, along_x,
                      [lambda p, c: lat.at[2 * p + c, :, pl.ds(0, half)], lambda p, c: lat.at[2 * p + c, :, pl.ds(half, half)]],
                      lat_x, partner, core)
    lat_ring.start()
    for load in loads[1:]:
        load.wait()
    ukvT[0:2 * PLAIN, :] = uk[...].astype(F32).T.astype(BF)
    ukvT[2 * PLAIN:2 * PLAIN + VROWS, :] = uv[...].astype(F32).T.astype(BF)
    q_gain_ref[...] = jnp.broadcast_to(qg_ref[...], (8, qg_ref.shape[1])).T[:, 0:1]
    kv_gain_ref[...] = jnp.broadcast_to(kg_ref[...], (8, kg_ref.shape[1])).T[:, 0:1]
    pos = lax.broadcasted_iota(jnp.int32, (8, tok), 1) + z * tok
    freq = jnp.exp(lax.broadcasted_iota(jnp.int32, (8, tok), 0).astype(F32) * (-math.log(10000.0) / 8))
    row_angle = (pos >> 6).astype(F32) * freq
    col_angle = (pos & (GRID_W - 1)).astype(F32) * freq
    turn = (jnp.cos(row_angle), jnp.sin(row_angle), jnp.cos(col_angle), jnp.sin(col_angle))

    def chip_rows(p):
        return jnp.concatenate([lat[2 * p].astype(F32), lat[2 * p + 1].astype(F32)], axis=0)

    def note_statistics(p):
        values = chip_rows(p)
        center = values - jnp.mean(values, axis=-1, keepdims=True)
        mean_ref[p] = jnp.mean(values, axis=-1, keepdims=True)
        rstd_ref[p] = lax.rsqrt(jnp.mean(center * center, axis=-1, keepdims=True) + EPSILON)

    lat_ring.step(1)
    for k in reversed(order):
        zm(k, True).wait_recv()
    total = zmod[0]
    for k in range(1, nz):
        total = total + zmod[k]
    xmod[t] = total
    for k in range(1, nt):
        xm(k, False).start()
    far = lat_ring.reach
    for s in range(2, far + 1):
        lat_ring.pair_step(s - 2)

        @pl.loop(0, 1 if s == 2 else 2)
        def _(i):
            note_statistics(lax.rem(chip + jnp.where(i == 0, nx - (s - 2), s - 2), nx))

        lat_ring.step(s)
    lat_ring.pair_step(far - 1)

    @pl.loop(0, 2 if far > 1 else 1)
    def _(i):
        note_statistics(lax.rem(chip + jnp.where(i == 0, nx - (far - 1), far - 1), nx))

    lat_ring.pair_step(far)
    note_statistics(lax.rem(chip + far, nx))
    for k in range(1, nt):
        xm(k, True).wait_recv()
    for j in range(nt):
        mod[:, j * part:(j + 1) * part] = xmod[j]

    @pl.loop(0, nx)
    def _(p):
        at = pl.ds(pl.multiple_of(p * 2 * rows, 2 * rows), 2 * rows)
        normed = (chip_rows(p) - mean_ref[p]) * rstd_ref[p]
        h[at, :] = (normed * (1.0 + mod[2:3, :]) + mod[0:1, :]).astype(BF)

    h[tok:, :] = modulated(ctx[...], mod[1:2, :], mod[3:4, :])
    product = lax.dot_general(h[...], wcat[...], (((1,), (1,)), ((), ())), preferred_element_type=F32)
    raw = product[0:tok].T
    rawc = jnp.concatenate([product[tok:], jnp.zeros((128 - crows, product.shape[1]), F32)], axis=0).T
    q_at = lambda p, c, i: pl.ds(pl.multiple_of((2 * p + c) * rank_q + i * (rank_q // 2), rank_q // 2), rank_q // 2)
    kv_at = lambda p, c: pl.ds(pl.multiple_of((2 * p + c) * rank_kv, rank_kv), rank_kv)
    kvraw[kv_at(chip, core), 0:tok] = raw[rank_q:rank_q + rank_kv].astype(BF)
    kvraw[kv_at(chip, core), tok:] = rawc[rank_q:rank_q + rank_kv].astype(BF)
    lane_half = kvraw.shape[1] // 2
    raw_ring = Gather(nx, chip, along_x,
                      [lambda p, c: kvraw.at[kv_at(p, c), pl.ds(0, lane_half)], lambda p, c: kvraw.at[kv_at(p, c), pl.ds(lane_half, lane_half)]],
                      raw_x, partner, core)
    raw_ring.start()
    qraw[pl.ds(pl.multiple_of(t * rank_q, rank_q), rank_q), :] = raw[0:rank_q].astype(BF)
    q_ring = Gather(nx, chip, along_x,
                    [lambda p, c: qraw.at[q_at(p, c, 0), :], lambda p, c: qraw.at[q_at(p, c, 1), :]],
                    q_x, partner, core)
    q_ring.start()
    kv[z, 2 * PLAIN:KROWS, :] = axial_turn(raw[rank_q + rank_kv:], *turn).astype(BF)
    for i in range(4):
        turn_ref[i] = turn[i]

    for s in range(1, raw_ring.reach + 1):
        raw_ring.step(s)
    for s in range(0, raw_ring.reach + 1):
        raw_ring.pair_step(s)

    ckv = rms_columns(kvraw[...], kv_gain_ref[...])
    own = jnp.dot(ukvT[...], ckv, preferred_element_type=F32).astype(BF)
    kv[z, 0:2 * PLAIN, :] = own[0:2 * PLAIN, 0:tok]
    kv[z, KROWS:KROWS + VROWS, :] = own[2 * PLAIN:, 0:tok]
    loose = jnp.concatenate([own[0:2 * PLAIN, tok:].astype(F32), rawc[rank_q + rank_kv:].astype(BF).astype(F32), own[2 * PLAIN:, tok:].astype(F32)], axis=0)
    group = (KROWS + VROWS) // 4
    packed = loose[0:group]
    for g in range(1, 4):
        packed = packed + pltpu.roll(loose[g * group:(g + 1) * group], g * crows, 1)
    kvp[z] = jnp.concatenate([packed, jnp.zeros((kvp.shape[1] - group, 128), F32)], axis=0).astype(BF)
    kv_half = (KROWS + VROWS) // 2
    kv_chunks = [lambda p, c: kv.at[p, pl.ds(0, kv_half)], lambda p, c: kv.at[p, pl.ds(kv_half, kv_half)], lambda p, c: kvp.at[p]]
    kv_ring = Gather(nz, z, along_z, kv_chunks, kv_z)
    kv_ring.cut = 1
    kv_ring.start()

    def query_up():
        for s in range(0, q_ring.reach + 1):
            q_ring.pair_step(s)
        cq = rms_columns(qraw[...], q_gain_ref[...])
        q = jnp.dot(uqT[...], cq, preferred_element_type=F32)
        per = PLAIN + ROTARY
        for head in range(2):
            mine = q[head * per:(head + 1) * per]
            plain = mine[0:PLAIN].astype(BF)
            blank = jnp.zeros_like(plain)
            qb[head, head * PLAIN:(head + 1) * PLAIN, :] = plain
            qb[head, (1 - head) * PLAIN:(2 - head) * PLAIN, :] = blank
            qb[head, 2 * PLAIN:KROWS, :] = axial_turn(mine[PLAIN:], *[turn_ref[i] for i in range(4)]).astype(BF)

    m_ref[...] = jnp.full_like(m_ref, NEGATIVE)
    l_ref[...] = jnp.zeros_like(l_ref)
    acc[...] = jnp.zeros_like(acc)

    def attend(keysT, valuesT, biased):
        keys = keysT.astype(F32).T.astype(BF)
        for head in range(2):
            s = jnp.dot(keys, qb[head], preferred_element_type=F32) * (SCORE * LOG2E)
            if biased:
                s = s + bias_ref[0, head] * LOG2E
            old = m_ref[head]
            new = jnp.maximum(old, jnp.max(s, axis=0, keepdims=True))
            alpha = jnp.exp2(old - new)
            e = jnp.exp2(s - new)
            m_ref[head] = new
            l_ref[head] = l_ref[head] * alpha + jnp.sum(e, axis=0, keepdims=True)
            acc[head] = acc[head] * alpha + jnp.dot(valuesT[head * VALUE:(head + 1) * VALUE], e.astype(BF), preferred_element_type=F32)

    reach = kv_ring.reach

    def ring_source(d, s):
        return lax.rem(z + jnp.where(d == 0, nz - s, s), nz)

    def nth_source(n):
        return ring_source(1 - lax.rem(n, 2), (n + 1) // 2)

    def hop(d, s, ch, into):
        piece = kv_chunks[ch](ring_source(d, s), 0)
        return pltpu.make_async_remote_copy(piece, piece, kv_z[1].at[d, s, ch], kv_z[0].at[d, into, ch],
                                            device_id=along_z(1 if d == 0 else nz - 1), device_id_type=MESH)

    def pass_on(s, ch):
        for d in range(2):
            hop(d, s, ch, s).wait_recv()
            if d == min(ch, 1):
                hop(d, s, ch, s + 1).start()
            else:
                @pl.when(s + 1 < reach)
                def _():
                    hop(d, s, ch, s + 1).start()

    def attend_block(n):
        b = nth_source(n)
        attend(kv[b, 0:KROWS, :], kv[b, KROWS:KROWS + VROWS, :], False)

    def unpack(tile):
        lanes = lax.broadcasted_iota(jnp.int32, (group, 128), 1) // crows
        parts = [None] * 4
        for j in range(4):
            held = kvp[nth_source(4 * tile + j)][0:group].astype(F32)
            for g in range(4):
                moved = jnp.where(lanes == g, held, 0.0)
                if g != j:
                    moved = pltpu.roll(moved, ((j - g) % 4) * crows, 1)
                parts[g] = moved if parts[g] is None else parts[g] + moved
        kvc[:, tile * 128:(tile + 1) * 128] = jnp.concatenate(parts, axis=0).astype(BF)

    slots = 2 * (reach - 1)
    first = min(q_ring.reach, slots)

    def done_after(i):
        return jnp.clip(2 * (i - first + 1), 0, i + 1)

    def kv_slot(i, carry):
        s = i // 2 + 1

        @pl.when(lax.rem(i, 2) == 0)
        def _():
            pass_on(s, 0)

        @pl.when(lax.rem(i, 2) == 1)
        def _():
            pass_on(s, 1)
            pass_on(s, 2)

        for step in range(1, q_ring.reach + 1):
            @pl.when(i == min(step, first) - 1)
            def _():
                q_ring.step(step)
                if step == q_ring.reach:
                    query_up()

        @pl.loop(jnp.where(i >= first, done_after(i - 1), 0), jnp.where(i >= first, done_after(i), 0))
        def _(n):
            attend_block(n)
        return carry

    lax.fori_loop(0, slots, kv_slot, 0)

    @pl.loop(done_after(slots - 1), 2 * reach - 1)
    def _(n):
        attend_block(n)
    tiles = nz // 4
    for tile in range(tiles - 1):
        unpack(tile)
    if tiles > 1:
        attend(kvc[0:KROWS, 0:128 * (tiles - 1)], kvc[KROWS:KROWS + VROWS, 0:128 * (tiles - 1)], True)
    kv_ring.ring_arrival(0, reach, 0).wait_recv()
    kv_ring.ring_arrival(1, reach, 1).wait_recv()
    kv_ring.ring_arrival(1, reach, 2).wait_recv()
    attend_block(2 * reach - 1)
    unpack(tiles - 1)
    attend(kvc[0:KROWS, 128 * (tiles - 1):], kvc[KROWS:KROWS + VROWS, 128 * (tiles - 1):], True)

    outT = jnp.concatenate([acc[0] / l_ref[0], acc[1] / l_ref[1]], axis=0)
    mine_at = lambda p, c: pl.ds(pl.multiple_of((2 * p + c) * VROWS, VROWS), VROWS)
    att[:, mine_at(chip, core)] = outT.T.astype(BF)
    fourth = tok // 4
    att_ring = Gather(nx, chip, along_x,
                      [lambda p, c, i=i: att.at[pl.ds(i * fourth, fourth), mine_at(p, c)] for i in range(4)],
                      att_x, partner, core)
    att_ring.start()
    for s in range(1, att_ring.reach + 1):
        att_ring.step(s)

    def am(k, incoming):
        far = lax.rem(t + nt - k, nt) if incoming else lax.rem(t + k, nt)
        if incoming:
            return pltpu.make_async_remote_copy(pbuf.at[far], mbuf.at[far], a_s.at[k], a_r.at[k], device_id={"tp": far}, device_id_type=MESH)
        return pltpu.make_async_remote_copy(pbuf.at[far], mbuf.at[t], a_s.at[k], a_r.at[k], device_id={"tp": far}, device_id_type=MESH)

    for s in range(0, att_ring.reach + 1):
        att_ring.pair_step(s)
    proj = jnp.dot(att[...], wo[...], preferred_element_type=F32)
    for j in range(nt):
        pbuf[j] = proj[j * rows:(j + 1) * rows].astype(BF)
    for k in sorted(range(1, nt), key=lambda k: -min(k, nt - k)):
        am(k, False).start()
    mbuf[t] = pbuf[t]
    gate_ref[...] = mod[4:5, :]
    for k in range(1, nt):
        am(k, True).wait_recv()
    for j in range(nt):
        cut = slice(j * part, (j + 1) * part)
        proj_ref[:, cut] = mbuf[j]

    for k in range(1, nz):
        zm(k, False).wait_send()
    for k in range(1, nt):
        xm(k, False).wait_send()
        am(k, False).wait_send()
    lat_ring.finish()
    raw_ring.finish()
    q_ring.finish()
    kv_ring.finish()
    att_ring.finish()


def sems(count, chunks, paired):
    kinds = 4 if paired else 2
    return tuple(pltpu.SemaphoreType.DMA((2, count // 2 + 2, chunks)) for _ in range(kinds))


def on_device(latents, conditions, context, w_shift, w_scale, w_gate, w_qdown, w_kvdown, w_rope, q_gain,
              latent_norm_gain, query_up_weight, key_up_weight, value_up_weight, context_bias, w_out):
    nz, nt = lax.axis_size("sp"), lax.axis_size("tp")
    nx = nt // 2
    rows, width = latents.shape
    tok = rows * nt
    crows = context.shape[0]
    rank_q, rank_kv = w_qdown.shape[1], w_kvdown.shape[1]
    part = width // nt
    vm = pltpu.VMEM
    dma = pltpu.SemaphoreType.DMA
    scratch = [
        vm((nt, rows, width), BF), vm((crows, width), BF), vm((nx, 2 * rows, 1), F32), vm((nx, 2 * rows, 1), F32),
        vm(key_up_weight.shape, BF), vm(value_up_weight.shape, BF), vm(w_out.shape, BF),
        vm((rank_q + rank_kv + ROTARY, width), BF), vm(query_up_weight.shape[::-1], BF), vm((2 * PLAIN + VROWS, nt * rank_kv), BF),
        vm((nz, 8, part), F32), vm((nt, 8, part), F32), vm((8, width), F32),
        vm((tok + crows, width), BF),
        vm((nt * rank_q, tok), BF), vm((nt * rank_kv, tok + 128), BF),
        vm((nz, KROWS + VROWS, tok), BF), vm((nz, 80, 128), BF), vm((KROWS + VROWS, nz * crows), BF), vm((2, KROWS, tok), BF),
        vm((2, 1, tok), F32), vm((2, 1, tok), F32), vm((2, VALUE, tok), F32),
        vm((tok, nt * VROWS), BF), vm((nt, rows, part), BF), vm((nt, rows, part), BF),
        vm((nt * rank_q, 1), F32), vm((nt * rank_kv, 1), F32), vm((4, 8, tok), F32),
        dma((9,)), dma((nz,)), dma((nz,)), dma((nt,)), dma((nt,)), dma((nt,)), dma((nt,)),
        sems(nx, 2, True), sems(nx, 2, True), sems(nx, 2, True), sems(nz, 3, False), sems(nx, 4, True),
    ]
    here = pl.BlockSpec(memory_space=vm)
    away = pl.BlockSpec(memory_space=pl.ANY)
    small = pl.BlockSpec(memory_space=pltpu.SMEM)
    proj, gate = pl.pallas_call(
        functools.partial(kernel, nz, nt),
        out_shape=(jax.ShapeDtypeStruct((rows, width), BF), jax.ShapeDtypeStruct((1, width), F32)),
        in_specs=[away, here, away, here, here, here, away, away, away, here, here, away, away, away, small, away],
        out_specs=(here, here),
        scratch_shapes=scratch,
        compiler_params=pltpu.CompilerParams(collective_id=0, has_side_effects=True, vmem_limit_bytes=60 * 1024 * 1024),
        name="block",
    )(latents, conditions, context, w_shift, w_scale, w_gate, w_qdown.T, w_kvdown.T, w_rope.T, q_gain.reshape(1, -1),
      latent_norm_gain.reshape(1, -1), query_up_weight.T, key_up_weight, value_up_weight, context_bias.reshape(1, -1), w_out)
    return (latents.astype(F32) + gate * proj.astype(F32)).astype(BF)


def solution(mesh):
    in_specs = (
        P(("grp", "sp", "tp"), None),
        P("grp", "sp"),
        P(("grp", "sp"), None),
        P("sp", "tp"),
        P("sp", "tp"),
        P("sp", "tp"),
        P(None, "tp"),
        P(None, "tp"),
        P(),
        P(),
        P(),
        P(None, "tp"),
        P(None, "tp"),
        P(None, "tp"),
        P("tp"),
        P(None, "tp"),
    )
    return jax.shard_map(on_device, mesh=mesh, in_specs=in_specs, out_specs=P(("grp", "sp", "tp"), None), check_vma=False)
```

```python
import functools
import math

import jax
import jax.numpy as jnp
from jax import lax
from jax.experimental import pallas as pl
from jax.experimental.pallas import tpu as pltpu
from jax.sharding import PartitionSpec as P

PLAIN = 64
ROTARY = 32
VALUE = 64
GRID_W = 64
EPSILON = 1e-6
NEGATIVE = -1e30
LOG2E = 1.4426950408889634
SCORE = (PLAIN + ROTARY) ** (-0.5)
MESH = pl.DeviceIdType.MESH
BF = jnp.bfloat16
F32 = jnp.float32
KROWS = 2 * PLAIN + ROTARY
VROWS = 2 * VALUE


class Gather:
    def __init__(self, count, place, towards, chunks, sems, partner=None, core=0):
        self.count, self.place, self.towards = count, place, towards
        self.chunks, self.partner, self.core = chunks, partner, core
        self.recv, self.send = sems[0], sems[1]
        self.pair_recv, self.pair_send = (sems[2], sems[3]) if partner is not None else (None, None)
        self.reach = count // 2
        self.cut = (len(chunks) + 1) // 2

    def active(self, d, s, ch):
        if s < self.reach:
            return True
        if s > self.reach:
            return False
        return (ch < self.cut) if d == 0 else (ch >= self.cut)

    def source(self, d, s):
        move = (self.count - s) if d == 0 else s
        return lax.rem(self.place + move, self.count)

    def ring_copy(self, d, s, ch):
        piece = self.chunks[ch](self.source(d, s), self.core)
        return pltpu.make_async_remote_copy(
            src_ref=piece, dst_ref=piece, send_sem=self.send.at[d, s, ch], recv_sem=self.recv.at[d, s + 1, ch],
            device_id=self.towards(1 if d == 0 else self.count - 1), device_id_type=MESH)

    def ring_arrival(self, d, s, ch):
        piece = self.chunks[ch](self.source(d, s), self.core)
        return pltpu.make_async_remote_copy(
            src_ref=piece, dst_ref=piece, send_sem=self.send.at[d, s, ch], recv_sem=self.recv.at[d, s, ch],
            device_id=self.towards(self.count - 1 if d == 0 else 1), device_id_type=MESH)

    def pair_copy(self, d, s, ch, core):
        piece = self.chunks[ch](self.source(d, s), core)
        return pltpu.make_async_remote_copy(
            src_ref=piece, dst_ref=piece, send_sem=self.pair_send.at[d, s, ch], recv_sem=self.pair_recv.at[d, s, ch],
            device_id=self.partner, device_id_type=MESH)

    def start(self, only=None):
        for ch in range(len(self.chunks)) if only is None else only:
            for d in range(2):
                if self.active(d, 1, ch):
                    self.ring_copy(d, 0, ch).start()
            if self.partner is not None:
                self.pair_copy(0, 0, ch, self.core).start()

    def step(self, s):
        for ch in range(len(self.chunks)):
            for d in range(2):
                if self.active(d, s, ch):
                    self.ring_arrival(d, s, ch).wait_recv()
                    if self.active(d, s + 1, ch):
                        self.ring_copy(d, s, ch).start()
                    if self.partner is not None:
                        self.pair_copy(d, s, ch, self.core).start()

    def pair_step(self, s, only=None):
        for ch in range(len(self.chunks)) if only is None else only:
            for d in range(2):
                if (s == 0 and d == 0) or (s > 0 and self.active(d, s, ch)):
                    self.pair_copy(d, s, ch, 1 - self.core).wait_recv()

    def finish(self):
        for s in range(self.reach + 1):
            for ch in range(len(self.chunks)):
                for d in range(2):
                    if self.active(d, s + 1, ch):
                        self.ring_copy(d, s, ch).wait_send()
                    if self.partner is not None and ((s == 0 and d == 0) or (s > 0 and self.active(d, s, ch))):
                        self.pair_copy(d, s, ch, self.core).wait_send()


def axial_turn(a, row_cos, row_sin, col_cos, col_sin):
    a0, a1, a2, a3 = a[0:8], a[8:16], a[16:24], a[24:32]
    return jnp.concatenate(
        [a0 * row_cos - a1 * row_sin, a0 * row_sin + a1 * row_cos,
         a2 * col_cos - a3 * col_sin, a2 * col_sin + a3 * col_cos], axis=0)


def modulated(block, shift, scale):
    values = block.astype(F32)
    center = values - jnp.mean(values, axis=-1, keepdims=True)
    spread = jnp.mean(center * center, axis=-1, keepdims=True)
    return (center * lax.rsqrt(spread + EPSILON) * (1.0 + scale) + shift).astype(BF)


def rms_columns(raw, gain):
    values = raw.astype(F32)
    factor = lax.rsqrt(jnp.mean(values * values, axis=0, keepdims=True) + EPSILON)
    return (values * factor * gain).astype(BF)


def kernel(nz, nt, *refs):
    (lat_hbm, cond_ref, ctx_hbm, wsh_ref, wsc_ref, wg_ref, wq_hbm, wkv_hbm, wr_hbm, qg_ref, kg_ref,
     uq_hbm, uk_hbm, uv_hbm, bias_ref, wo_hbm, proj_ref, gate_ref,
     lat, ctx, mean_ref, rstd_ref, uk, uv, wo,
     wcat, uqT, ukvT, zmod, xmod, mod, h, qraw, kvraw, kv, kvp, kvc, qb,
     m_ref, l_ref, acc, att, pbuf, mbuf, q_gain_ref, kv_gain_ref, turn_ref,
     load_sem, zm_s, zm_r, xm_s, xm_r, a_s, a_r, lat_x, raw_s, raw_r, rawp_s, rawp_r, q_x, kv_z, kr_s, kr_r, att_x) = refs
    z, t = lax.axis_index("sp"), lax.axis_index("tp")
    core = lax.rem(t, 2)
    chip = t // 2
    nx = nt // 2
    rows = lat.shape[1]
    tok = rows * nt
    crows = ctx.shape[0]
    width = lat.shape[2]
    part = width // nt
    rank_q, rank_kv = wq_hbm.shape[0], wkv_hbm.shape[0]
    along_z = lambda k: {"sp": lax.rem(z + k, nz)}
    along_x = lambda k: {"tp": lax.rem(t + 2 * k, nt)}
    partner = {"tp": t + 1 - 2 * core}
    fourth_of_width = width // 4

    loads = [
        pltpu.make_async_copy(lat_hbm, lat.at[t], load_sem.at[0]),
        pltpu.make_async_copy(ctx_hbm, ctx, load_sem.at[1]),
        pltpu.make_async_copy(wq_hbm, wcat.at[pl.ds(0, rank_q)], load_sem.at[2]),
        pltpu.make_async_copy(wkv_hbm, wcat.at[pl.ds(rank_q, rank_kv)], load_sem.at[3]),
        pltpu.make_async_copy(wr_hbm, wcat.at[pl.ds(rank_q + rank_kv, ROTARY)], load_sem.at[4]),
        pltpu.make_async_copy(uq_hbm, uqT, load_sem.at[5]),
        pltpu.make_async_copy(uk_hbm, uk, load_sem.at[6]),
        pltpu.make_async_copy(uv_hbm, uv, load_sem.at[7]),
        pltpu.make_async_copy(wo_hbm, wo, load_sem.at[8]),
    ]
    barrier = pltpu.get_barrier_semaphore()
    for k in range(1, nz):
        pl.semaphore_signal(barrier, inc=1, device_id=along_z(k), device_id_type=MESH)
    for k in range(1, nt):
        pl.semaphore_signal(barrier, inc=1, device_id={"tp": lax.rem(t + k, nt)}, device_id_type=MESH)
    for load in loads:
        load.start()

    cond = cond_ref[...]
    act = cond / (1.0 + jnp.exp(-cond))
    act = jnp.concatenate([act, jnp.zeros((14, act.shape[1]), F32)], axis=0).astype(BF)
    shift_part = jnp.dot(act, wsh_ref[...], preferred_element_type=F32)
    scale_part = jnp.dot(act, wsc_ref[...], preferred_element_type=F32)
    gate_part = jnp.dot(act, wg_ref[...], preferred_element_type=F32)
    zmod[z] = jnp.concatenate([shift_part[0:2], scale_part[0:2], gate_part[0:2], gate_part[2:4]], axis=0)
    pl.semaphore_wait(barrier, nz + nt - 2)

    def zm(k, incoming):
        if incoming:
            src = lax.rem(z + nz - k, nz)
            return pltpu.make_async_remote_copy(zmod.at[src], zmod.at[src], zm_s.at[k], zm_r.at[k], device_id=along_z(nz - k), device_id_type=MESH)
        return pltpu.make_async_remote_copy(zmod.at[z], zmod.at[z], zm_s.at[k], zm_r.at[k], device_id=along_z(k), device_id_type=MESH)

    def xm(k, incoming):
        if incoming:
            src = lax.rem(t + nt - k, nt)
            return pltpu.make_async_remote_copy(xmod.at[src], xmod.at[src], xm_s.at[k], xm_r.at[k], device_id={"tp": src}, device_id_type=MESH)
        return pltpu.make_async_remote_copy(xmod.at[t], xmod.at[t], xm_s.at[k], xm_r.at[k], device_id={"tp": lax.rem(t + k, nt)}, device_id_type=MESH)

    order = sorted(range(1, nz), key=lambda k: -min(k, nz - k))
    for k in order:
        zm(k, False).start()
    loads[0].wait()
    lat_ring = Gather(nx, chip, along_x,
                      [lambda p, c, i=i: lat.at[2 * p + c, :, pl.ds(i * fourth_of_width, fourth_of_width)] for i in range(4)],
                      lat_x, partner, core)
    lat_ring.start()
    for load in loads[1:]:
        load.wait()
    ukvT[0:2 * PLAIN, :] = uk[...].astype(F32).T.astype(BF)
    ukvT[2 * PLAIN:2 * PLAIN + VROWS, :] = uv[...].astype(F32).T.astype(BF)
    q_gain_ref[...] = jnp.broadcast_to(qg_ref[...], (8, qg_ref.shape[1])).T[:, 0:1]
    kv_gain_ref[...] = jnp.broadcast_to(kg_ref[...], (8, kg_ref.shape[1])).T[:, 0:1]
    pos = lax.broadcasted_iota(jnp.int32, (8, tok), 1) + z * tok
    freq = jnp.exp(lax.broadcasted_iota(jnp.int32, (8, tok), 0).astype(F32) * (-math.log(10000.0) / 8))
    row_angle = (pos >> 6).astype(F32) * freq
    col_angle = (pos & (GRID_W - 1)).astype(F32) * freq
    turn = (jnp.cos(row_angle), jnp.sin(row_angle), jnp.cos(col_angle), jnp.sin(col_angle))

    def chip_rows(p):
        return jnp.concatenate([lat[2 * p].astype(F32), lat[2 * p + 1].astype(F32)], axis=0)

    def note_statistics(p):
        values = chip_rows(p)
        center = values - jnp.mean(values, axis=-1, keepdims=True)
        mean_ref[p] = jnp.mean(values, axis=-1, keepdims=True)
        rstd_ref[p] = lax.rsqrt(jnp.mean(center * center, axis=-1, keepdims=True) + EPSILON)

    lat_ring.step(1)
    for k in reversed(order):
        zm(k, True).wait_recv()
    total = zmod[0]
    for k in range(1, nz):
        total = total + zmod[k]
    xmod[t] = total
    for k in range(1, nt):
        xm(k, False).start()
    far = lat_ring.reach
    for s in range(2, far + 1):
        lat_ring.pair_step(s - 2)

        @pl.loop(0, 1 if s == 2 else 2)
        def _(i):
            note_statistics(lax.rem(chip + jnp.where(i == 0, nx - (s - 2), s - 2), nx))

        lat_ring.step(s)
    lat_ring.pair_step(far - 1)

    @pl.loop(0, 2 if far > 1 else 1)
    def _(i):
        note_statistics(lax.rem(chip + jnp.where(i == 0, nx - (far - 1), far - 1), nx))

    lat_ring.pair_step(far)
    note_statistics(lax.rem(chip + far, nx))
    for k in range(1, nt):
        xm(k, True).wait_recv()
    for j in range(nt):
        mod[:, j * part:(j + 1) * part] = xmod[j]

    @pl.loop(0, nx)
    def _(p):
        at = pl.ds(pl.multiple_of(p * 2 * rows, 2 * rows), 2 * rows)
        normed = (chip_rows(p) - mean_ref[p]) * rstd_ref[p]
        h[at, :] = (normed * (1.0 + mod[2:3, :]) + mod[0:1, :]).astype(BF)

    h[tok:, :] = modulated(ctx[...], mod[1:2, :], mod[3:4, :])
    product = lax.dot_general(h[...], wcat[...], (((1,), (1,)), ((), ())), preferred_element_type=F32)
    raw = product[0:tok].T
    rawc = jnp.concatenate([product[tok:], jnp.zeros((128 - crows, product.shape[1]), F32)], axis=0).T
    q_at = lambda p, c, i: pl.ds(pl.multiple_of((2 * p + c) * rank_q + i * (rank_q // 2), rank_q // 2), rank_q // 2)
    kv_at = lambda p, c: pl.ds(pl.multiple_of((2 * p + c) * rank_kv, rank_kv), rank_kv)
    kvraw[kv_at(chip, core), 0:tok] = raw[rank_q:rank_q + rank_kv].astype(BF)
    kvraw[kv_at(chip, core), tok:] = rawc[rank_q:rank_q + rank_kv].astype(BF)
    lane_half = kvraw.shape[1] // 2
    opposite = nx // 2

    def raw_piece(k, side, c):
        piece = kvraw.at[kv_at(lax.rem(chip + nx - k, nx), c)]
        return piece if side is None else kvraw.at[kv_at(lax.rem(chip + nx - k, nx), c), pl.ds(side * lane_half, lane_half)]

    def raw_copy(k, incoming):
        piece = raw_piece(k if incoming else 0, None, core)
        return pltpu.make_async_remote_copy(piece, piece, raw_s.at[k], raw_r.at[k], device_id=along_x(k), device_id_type=MESH)

    def raw_last(side, incoming):
        near = 1 if side == 0 else nx - 1
        piece = raw_piece(opposite if incoming else near, side, core)
        at = opposite if side == 0 else nx
        return pltpu.make_async_remote_copy(piece, piece, raw_s.at[at], raw_r.at[at],
                                            device_id=along_x(opposite - 1 if side == 0 else nx - opposite + 1), device_id_type=MESH)

    def raw_pair(k, incoming):
        piece = raw_piece(k, None, 1 - core if incoming else core)
        return pltpu.make_async_remote_copy(piece, piece, rawp_s.at[k], rawp_r.at[k], device_id=partner, device_id_type=MESH)

    by_distance = [k for m in range(1, opposite) for k in (m, nx - m)]
    for k in by_distance:
        raw_copy(k, False).start()
    raw_pair(0, False).start()
    qraw[pl.ds(pl.multiple_of(t * rank_q, rank_q), rank_q), :] = raw[0:rank_q].astype(BF)
    q_ring = Gather(nx, chip, along_x,
                    [lambda p, c: qraw.at[q_at(p, c, 0), :], lambda p, c: qraw.at[q_at(p, c, 1), :]],
                    q_x, partner, core)
    q_ring.start()
    own_last = lambda a: jnp.where(core == 0, jnp.concatenate([a[ROTARY // 2:], a[:ROTARY // 2]], axis=0), a)
    kv[z, 2 * PLAIN:KROWS, :] = own_last(axial_turn(raw[rank_q + rank_kv:], *turn)).astype(BF)
    for i in range(4):
        turn_ref[i] = turn[i]
    for k in by_distance:
        raw_copy(k, True).wait_recv()
        if k in (1, nx - 1):
            raw_last(0 if k == 1 else 1, False).start()
        raw_pair(k, False).start()
    for side in range(2):
        raw_last(side, True).wait_recv()
    raw_pair(opposite, False).start()
    for k in range(nx):
        raw_pair(k, True).wait_recv()

    ckv = rms_columns(kvraw[...], kv_gain_ref[...])
    own = jnp.dot(ukvT[...], ckv, preferred_element_type=F32).astype(BF)
    kv[z, 0:2 * PLAIN, :] = own[0:2 * PLAIN, 0:tok]
    kv[z, KROWS:KROWS + VROWS, :] = own[2 * PLAIN:, 0:tok]
    loose = jnp.concatenate([own[0:2 * PLAIN, tok:].astype(F32), own_last(rawc[rank_q + rank_kv:]).astype(BF).astype(F32), own[2 * PLAIN:, tok:].astype(F32)], axis=0)
    group = (KROWS + VROWS) // 4
    packed = loose[0:group]
    for g in range(1, 4):
        packed = packed + pltpu.roll(loose[g * group:(g + 1) * group], g * crows, 1)
    kvp[z] = jnp.concatenate([packed, jnp.zeros((kvp.shape[1] - group, 128), F32)], axis=0).astype(BF)
    kr_half = ROTARY // 2
    kv_chunks = [lambda p, c: kv.at[p, pl.ds(0, 2 * PLAIN)], lambda p, c: kvp.at[p],
                 lambda p, c: kv.at[p, pl.ds(2 * PLAIN + kr_half, kr_half + VROWS)]]
    kv_ring = Gather(nz, z, along_z, kv_chunks, kv_z)
    kv_ring.start()

    def query_up():
        for s in range(0, q_ring.reach + 1):
            q_ring.pair_step(s)
        cq = rms_columns(qraw[...], q_gain_ref[...])
        q = jnp.dot(uqT[...], cq, preferred_element_type=F32)
        per = PLAIN + ROTARY
        for head in range(2):
            mine = q[head * per:(head + 1) * per]
            plain = mine[0:PLAIN].astype(BF)
            blank = jnp.zeros_like(plain)
            qb[head, head * PLAIN:(head + 1) * PLAIN, :] = plain
            qb[head, (1 - head) * PLAIN:(2 - head) * PLAIN, :] = blank
            qb[head, 2 * PLAIN:KROWS, :] = own_last(axial_turn(mine[PLAIN:], *[turn_ref[i] for i in range(4)])).astype(BF)

    m_ref[...] = jnp.full_like(m_ref, NEGATIVE)
    l_ref[...] = jnp.zeros_like(l_ref)
    acc[...] = jnp.zeros_like(acc)

    def attend(keysT, valuesT, biased):
        keys = keysT.astype(F32).T.astype(BF)
        for head in range(2):
            s = jnp.dot(keys, qb[head], preferred_element_type=F32) * (SCORE * LOG2E)
            if biased:
                s = s + bias_ref[0, head] * LOG2E
            old = m_ref[head]
            new = jnp.maximum(old, jnp.max(s, axis=0, keepdims=True))
            alpha = jnp.exp2(old - new)
            e = jnp.exp2(s - new)
            m_ref[head] = new
            l_ref[head] = l_ref[head] * alpha + jnp.sum(e, axis=0, keepdims=True)
            acc[head] = acc[head] * alpha + jnp.dot(valuesT[head * VALUE:(head + 1) * VALUE], e.astype(BF), preferred_element_type=F32)

    reach = kv_ring.reach

    def ring_source(d, s):
        return lax.rem(z + jnp.where(d == 0, nz - s, s), nz)

    def nth_source(n):
        return ring_source(1 - lax.rem(n, 2), (n + 1) // 2)

    def hop(d, s, ch, into):
        piece = kv_chunks[ch](ring_source(d, s), 0)
        return pltpu.make_async_remote_copy(piece, piece, kv_z[1].at[d, s, ch], kv_z[0].at[d, into, ch],
                                            device_id=along_z(1 if d == 0 else nz - 1), device_id_type=MESH)

    def kr_swap(d, s, incoming):
        b = ring_source(d, s)
        mine, theirs = kv.at[b, pl.ds(2 * PLAIN + kr_half, kr_half)], kv.at[b, pl.ds(2 * PLAIN, kr_half)]
        return pltpu.make_async_remote_copy(theirs if incoming else mine, theirs, kr_s.at[d, s], kr_r.at[d, s],
                                            device_id=partner, device_id_type=MESH)

    def pass_on(s, ch):
        for d in range(2):
            hop(d, s, ch, s).wait_recv()
            if d == ch // 2:
                hop(d, s, ch, s + 1).start()
            else:
                @pl.when(s + 1 < reach)
                def _():
                    hop(d, s, ch, s + 1).start()
            if ch == 2:
                kr_swap(d, s, False).start()

    def attend_block(n):
        b = nth_source(n)
        attend(kv[b, 0:KROWS, :], kv[b, KROWS:KROWS + VROWS, :], False)

    def unpack(tile):
        lanes = lax.broadcasted_iota(jnp.int32, (group, 128), 1) // crows
        parts = [None] * 4
        for j in range(4):
            held = kvp[nth_source(4 * tile + j)][0:group].astype(F32)
            for g in range(4):
                moved = jnp.where(lanes == g, held, 0.0)
                if g != j:
                    moved = pltpu.roll(moved, ((j - g) % 4) * crows, 1)
                parts[g] = moved if parts[g] is None else parts[g] + moved
        kvc[:, tile * 128:(tile + 1) * 128] = jnp.concatenate(parts, axis=0).astype(BF)

    slots = 2 * (reach - 1)
    first = min(q_ring.reach, slots)

    def done_after(i):
        return jnp.clip(2 * (i - first + 1), 0, i)

    def kv_slot(i, carry):
        s = i // 2 + 1

        @pl.when(lax.rem(i, 2) == 0)
        def _():
            pass_on(s, 0)
            pass_on(s, 1)

            @pl.when(s > 1)
            def _():
                for d in range(2):
                    kr_swap(d, s - 1, True).wait_recv()

        @pl.when(lax.rem(i, 2) == 1)
        def _():
            pass_on(s, 2)

        for step in range(1, q_ring.reach + 1):
            @pl.when(i == min(step, first) - 1)
            def _():
                q_ring.step(step)
                if step == q_ring.reach:
                    query_up()

        @pl.loop(jnp.where(i >= first, done_after(i - 1), 0), jnp.where(i >= first, done_after(i), 0))
        def _(n):
            attend_block(n)
        return carry

    lax.fori_loop(0, slots, kv_slot, 0)
    for d in range(2):
        kr_swap(d, reach - 1, True).wait_recv()

    @pl.loop(done_after(slots - 1), 2 * reach - 1)
    def _(n):
        attend_block(n)
    tiles = nz // 4
    for tile in range(tiles - 1):
        unpack(tile)
    if tiles > 1:
        attend(kvc[0:KROWS, 0:128 * (tiles - 1)], kvc[KROWS:KROWS + VROWS, 0:128 * (tiles - 1)], True)
    kv_ring.ring_arrival(0, reach, 0).wait_recv()
    kv_ring.ring_arrival(0, reach, 1).wait_recv()
    kv_ring.ring_arrival(1, reach, 2).wait_recv()
    kr_swap(0, reach, False).start()
    unpack(tiles - 1)
    kr_swap(0, reach, True).wait_recv()
    attend_block(2 * reach - 1)
    attend(kvc[0:KROWS, 128 * (tiles - 1):], kvc[KROWS:KROWS + VROWS, 128 * (tiles - 1):], True)

    outT = jnp.concatenate([acc[0] / l_ref[0], acc[1] / l_ref[1]], axis=0)
    mine_at = lambda p, c: pl.ds(pl.multiple_of((2 * p + c) * VROWS, VROWS), VROWS)
    att[:, mine_at(chip, core)] = outT.T.astype(BF)
    fourth = tok // 4
    att_ring = Gather(nx, chip, along_x,
                      [lambda p, c, i=i: att.at[pl.ds(i * fourth, fourth), mine_at(p, c)] for i in range(4)],
                      att_x, partner, core)
    att_ring.start()
    for s in range(1, att_ring.reach + 1):
        att_ring.step(s)

    def am(k, incoming):
        far = lax.rem(t + nt - k, nt) if incoming else lax.rem(t + k, nt)
        if incoming:
            return pltpu.make_async_remote_copy(pbuf.at[far], mbuf.at[far], a_s.at[k], a_r.at[k], device_id={"tp": far}, device_id_type=MESH)
        return pltpu.make_async_remote_copy(pbuf.at[far], mbuf.at[t], a_s.at[k], a_r.at[k], device_id={"tp": far}, device_id_type=MESH)

    for s in range(0, att_ring.reach + 1):
        att_ring.pair_step(s)
    proj = jnp.dot(att[...], wo[...], preferred_element_type=F32)
    for j in range(nt):
        pbuf[j] = proj[j * rows:(j + 1) * rows].astype(BF)
    for k in sorted(range(1, nt), key=lambda k: -min(k, nt - k)):
        am(k, False).start()
    mbuf[t] = pbuf[t]
    gate_ref[...] = mod[4:5, :]
    for k in range(1, nt):
        am(k, True).wait_recv()
    for j in range(nt):
        cut = slice(j * part, (j + 1) * part)
        proj_ref[:, cut] = mbuf[j]

    for k in range(1, nz):
        zm(k, False).wait_send()
    for k in range(1, nt):
        xm(k, False).wait_send()
        am(k, False).wait_send()
    lat_ring.finish()
    for k in by_distance:
        raw_copy(k, False).wait_send()
    for side in range(2):
        raw_last(side, False).wait_send()
    for k in range(nx):
        raw_pair(k, False).wait_send()
    for s in range(1, reach + 1):
        for d in range(2 if s < reach else 1):
            kr_swap(d, s, False).wait_send()
    q_ring.finish()
    kv_ring.finish()
    att_ring.finish()


def sems(count, chunks, paired):
    kinds = 4 if paired else 2
    return tuple(pltpu.SemaphoreType.DMA((2, count // 2 + 2, chunks)) for _ in range(kinds))


def on_device(latents, conditions, context, w_shift, w_scale, w_gate, w_qdown, w_kvdown, w_rope, q_gain,
              latent_norm_gain, query_up_weight, key_up_weight, value_up_weight, context_bias, w_out):
    nz, nt = lax.axis_size("sp"), lax.axis_size("tp")
    nx = nt // 2
    rows, width = latents.shape
    tok = rows * nt
    crows = context.shape[0]
    rank_q, rank_kv = w_qdown.shape[1], w_kvdown.shape[1]
    part = width // nt
    vm = pltpu.VMEM
    dma = pltpu.SemaphoreType.DMA
    scratch = [
        vm((nt, rows, width), BF), vm((crows, width), BF), vm((nx, 2 * rows, 1), F32), vm((nx, 2 * rows, 1), F32),
        vm(key_up_weight.shape, BF), vm(value_up_weight.shape, BF), vm(w_out.shape, BF),
        vm((rank_q + rank_kv + ROTARY, width), BF), vm(query_up_weight.shape[::-1], BF), vm((2 * PLAIN + VROWS, nt * rank_kv), BF),
        vm((nz, 8, part), F32), vm((nt, 8, part), F32), vm((8, width), F32),
        vm((tok + crows, width), BF),
        vm((nt * rank_q, tok), BF), vm((nt * rank_kv, tok + 128), BF),
        vm((nz, KROWS + VROWS, tok), BF), vm((nz, 80, 128), BF), vm((KROWS + VROWS, nz * crows), BF), vm((2, KROWS, tok), BF),
        vm((2, 1, tok), F32), vm((2, 1, tok), F32), vm((2, VALUE, tok), F32),
        vm((tok, nt * VROWS), BF), vm((nt, rows, part), BF), vm((nt, rows, part), BF),
        vm((nt * rank_q, 1), F32), vm((nt * rank_kv, 1), F32), vm((4, 8, tok), F32),
        dma((9,)), dma((nz,)), dma((nz,)), dma((nt,)), dma((nt,)), dma((nt,)), dma((nt,)),
        sems(nx, 4, True), dma((nx + 1,)), dma((nx + 1,)), dma((nx,)), dma((nx,)), sems(nx, 2, True), sems(nz, 3, False),
        dma((2, nz // 2 + 1)), dma((2, nz // 2 + 1)), sems(nx, 4, True),
    ]
    here = pl.BlockSpec(memory_space=vm)
    away = pl.BlockSpec(memory_space=pl.ANY)
    small = pl.BlockSpec(memory_space=pltpu.SMEM)
    proj, gate = pl.pallas_call(
        functools.partial(kernel, nz, nt),
        out_shape=(jax.ShapeDtypeStruct((rows, width), BF), jax.ShapeDtypeStruct((1, width), F32)),
        in_specs=[away, here, away, here, here, here, away, away, away, here, here, away, away, away, small, away],
        out_specs=(here, here),
        scratch_shapes=scratch,
        compiler_params=pltpu.CompilerParams(collective_id=0, has_side_effects=True, vmem_limit_bytes=60 * 1024 * 1024),
        name="block",
    )(latents, conditions, context, w_shift, w_scale, w_gate, w_qdown.T, w_kvdown.T, w_rope.T, q_gain.reshape(1, -1),
      latent_norm_gain.reshape(1, -1), query_up_weight.T, key_up_weight, value_up_weight, context_bias.reshape(1, -1), w_out)
    return (latents.astype(F32) + gate * proj.astype(F32)).astype(BF)


def solution(mesh):
    in_specs = (
        P(("grp", "sp", "tp"), None),
        P("grp", "sp"),
        P(("grp", "sp"), None),
        P("sp", "tp"),
        P("sp", "tp"),
        P("sp", "tp"),
        P(None, "tp"),
        P(None, "tp"),
        P(),
        P(),
        P(),
        P(None, "tp"),
        P(None, "tp"),
        P(None, "tp"),
        P("tp"),
        P(None, "tp"),
    )
    return jax.shard_map(on_device, mesh=mesh, in_specs=in_specs, out_specs=P(("grp", "sp", "tp"), None), check_vma=False)
```

```python
import functools
import math

import jax
import jax.numpy as jnp
from jax import lax
from jax.experimental import pallas as pl
from jax.experimental.pallas import tpu as pltpu
from jax.sharding import PartitionSpec as P

PLAIN = 64
ROTARY = 32
VALUE = 64
GRID_W = 64
EPSILON = 1e-6
NEGATIVE = -1e30
LOG2E = 1.4426950408889634
SCORE = (PLAIN + ROTARY) ** (-0.5)
MESH = pl.DeviceIdType.MESH
BF = jnp.bfloat16
F32 = jnp.float32
KROWS = 2 * PLAIN + ROTARY
VROWS = 2 * VALUE


class Gather:
    def __init__(self, count, place, towards, chunks, sems, partner=None, core=0):
        self.count, self.place, self.towards = count, place, towards
        self.chunks, self.partner, self.core = chunks, partner, core
        self.recv, self.send = sems[0], sems[1]
        self.pair_recv, self.pair_send = (sems[2], sems[3]) if partner is not None else (None, None)
        self.reach = count // 2
        self.cut = (len(chunks) + 1) // 2

    def active(self, d, s, ch):
        if s < self.reach:
            return True
        if s > self.reach:
            return False
        return (ch < self.cut) if d == 0 else (ch >= self.cut)

    def source(self, d, s):
        move = (self.count - s) if d == 0 else s
        return lax.rem(self.place + move, self.count)

    def ring_copy(self, d, s, ch):
        piece = self.chunks[ch](self.source(d, s), self.core)
        return pltpu.make_async_remote_copy(
            src_ref=piece, dst_ref=piece, send_sem=self.send.at[d, s, ch], recv_sem=self.recv.at[d, s + 1, ch],
            device_id=self.towards(1 if d == 0 else self.count - 1), device_id_type=MESH)

    def ring_arrival(self, d, s, ch):
        piece = self.chunks[ch](self.source(d, s), self.core)
        return pltpu.make_async_remote_copy(
            src_ref=piece, dst_ref=piece, send_sem=self.send.at[d, s, ch], recv_sem=self.recv.at[d, s, ch],
            device_id=self.towards(self.count - 1 if d == 0 else 1), device_id_type=MESH)

    def pair_copy(self, d, s, ch, core):
        piece = self.chunks[ch](self.source(d, s), core)
        return pltpu.make_async_remote_copy(
            src_ref=piece, dst_ref=piece, send_sem=self.pair_send.at[d, s, ch], recv_sem=self.pair_recv.at[d, s, ch],
            device_id=self.partner, device_id_type=MESH)

    def start(self, only=None):
        for ch in range(len(self.chunks)) if only is None else only:
            for d in range(2):
                if self.active(d, 1, ch):
                    self.ring_copy(d, 0, ch).start()
            if self.partner is not None:
                self.pair_copy(0, 0, ch, self.core).start()

    def step(self, s):
        for ch in range(len(self.chunks)):
            for d in range(2):
                if self.active(d, s, ch):
                    self.ring_arrival(d, s, ch).wait_recv()
                    if self.active(d, s + 1, ch):
                        self.ring_copy(d, s, ch).start()
                    if self.partner is not None:
                        self.pair_copy(d, s, ch, self.core).start()

    def pair_step(self, s, only=None):
        for ch in range(len(self.chunks)) if only is None else only:
            for d in range(2):
                if (s == 0 and d == 0) or (s > 0 and self.active(d, s, ch)):
                    self.pair_copy(d, s, ch, 1 - self.core).wait_recv()

    def finish(self):
        for s in range(self.reach + 1):
            for ch in range(len(self.chunks)):
                for d in range(2):
                    if self.active(d, s + 1, ch):
                        self.ring_copy(d, s, ch).wait_send()
                    if self.partner is not None and ((s == 0 and d == 0) or (s > 0 and self.active(d, s, ch))):
                        self.pair_copy(d, s, ch, self.core).wait_send()


def axial_turn(a, row_cos, row_sin, col_cos, col_sin):
    a0, a1, a2, a3 = a[0:8], a[8:16], a[16:24], a[24:32]
    return jnp.concatenate(
        [a0 * row_cos - a1 * row_sin, a0 * row_sin + a1 * row_cos,
         a2 * col_cos - a3 * col_sin, a2 * col_sin + a3 * col_cos], axis=0)


def modulated(block, shift, scale):
    values = block.astype(F32)
    center = values - jnp.mean(values, axis=-1, keepdims=True)
    spread = jnp.mean(center * center, axis=-1, keepdims=True)
    return (center * lax.rsqrt(spread + EPSILON) * (1.0 + scale) + shift).astype(BF)


def rms_columns(raw, gain):
    values = raw.astype(F32)
    factor = lax.rsqrt(jnp.mean(values * values, axis=0, keepdims=True) + EPSILON)
    return (values * factor * gain).astype(BF)


def kernel(nz, nt, *refs):
    (lat_hbm, cond_ref, ctx_hbm, wsh_ref, wsc_ref, wg_ref, wq_hbm, wkv_hbm, wr_hbm, qg_ref, kg_ref,
     uq_hbm, uk_hbm, uv_hbm, bias_ref, wo_hbm, proj_ref, gate_ref,
     lat, ctx, mean_ref, rstd_ref, uk, uv, wo,
     wcat, uqT, ukvT, zmod, xmod, mod, h, qraw, kvraw, kv, kvp, kvc, qb,
     m_ref, l_ref, acc, att, pbuf, mbuf, q_gain_ref, kv_gain_ref, turn_ref,
     load_sem, zm_s, zm_r, xm_s, xm_r, a_s, a_r, lat_x, raw_s, raw_r, rawp_s, rawp_r, q_x, kv_z, kr_s, kr_r, att_x) = refs
    z, t = lax.axis_index("sp"), lax.axis_index("tp")
    core = lax.rem(t, 2)
    chip = t // 2
    nx = nt // 2
    rows = lat.shape[1]
    tok = rows * nt
    crows = ctx.shape[0]
    width = lat.shape[2]
    part = width // nt
    rank_q, rank_kv = wq_hbm.shape[0], wkv_hbm.shape[0]
    along_z = lambda k: {"sp": lax.rem(z + k, nz)}
    along_x = lambda k: {"tp": lax.rem(t + 2 * k, nt)}
    partner = {"tp": t + 1 - 2 * core}
    fourth_of_width = width // 4

    loads = [
        pltpu.make_async_copy(lat_hbm, lat.at[t], load_sem.at[0]),
        pltpu.make_async_copy(ctx_hbm, ctx, load_sem.at[1]),
        pltpu.make_async_copy(wq_hbm, wcat.at[pl.ds(0, rank_q)], load_sem.at[2]),
        pltpu.make_async_copy(wkv_hbm, wcat.at[pl.ds(rank_q, rank_kv)], load_sem.at[3]),
        pltpu.make_async_copy(wr_hbm, wcat.at[pl.ds(rank_q + rank_kv, ROTARY)], load_sem.at[4]),
        pltpu.make_async_copy(uq_hbm, uqT, load_sem.at[5]),
        pltpu.make_async_copy(uk_hbm, uk, load_sem.at[6]),
        pltpu.make_async_copy(uv_hbm, uv, load_sem.at[7]),
        pltpu.make_async_copy(wo_hbm, wo, load_sem.at[8]),
    ]
    barrier = pltpu.get_barrier_semaphore()
    for k in range(1, nz):
        pl.semaphore_signal(barrier, inc=1, device_id=along_z(k), device_id_type=MESH)
    for k in range(1, nt):
        pl.semaphore_signal(barrier, inc=1, device_id={"tp": lax.rem(t + k, nt)}, device_id_type=MESH)
    for load in loads:
        load.start()

    cond = cond_ref[...]
    act = cond / (1.0 + jnp.exp(-cond))
    act = jnp.concatenate([act, jnp.zeros((14, act.shape[1]), F32)], axis=0).astype(BF)
    shift_part = jnp.dot(act, wsh_ref[...], preferred_element_type=F32)
    scale_part = jnp.dot(act, wsc_ref[...], preferred_element_type=F32)
    gate_part = jnp.dot(act, wg_ref[...], preferred_element_type=F32)
    zmod[z] = jnp.concatenate([shift_part[0:2], scale_part[0:2], gate_part[0:2], gate_part[2:4]], axis=0)
    pl.semaphore_wait(barrier, nz + nt - 2)

    def zm(k, incoming):
        if incoming:
            src = lax.rem(z + nz - k, nz)
            return pltpu.make_async_remote_copy(zmod.at[src], zmod.at[src], zm_s.at[k], zm_r.at[k], device_id=along_z(nz - k), device_id_type=MESH)
        return pltpu.make_async_remote_copy(zmod.at[z], zmod.at[z], zm_s.at[k], zm_r.at[k], device_id=along_z(k), device_id_type=MESH)

    def xm(k, incoming):
        if incoming:
            src = lax.rem(t + nt - k, nt)
            return pltpu.make_async_remote_copy(xmod.at[src], xmod.at[src], xm_s.at[k], xm_r.at[k], device_id={"tp": src}, device_id_type=MESH)
        return pltpu.make_async_remote_copy(xmod.at[t], xmod.at[t], xm_s.at[k], xm_r.at[k], device_id={"tp": lax.rem(t + k, nt)}, device_id_type=MESH)

    order = sorted(range(1, nz), key=lambda k: -min(k, nz - k))
    for k in order:
        zm(k, False).start()
    loads[0].wait()
    lat_ring = Gather(nx, chip, along_x,
                      [lambda p, c, i=i: lat.at[2 * p + c, :, pl.ds(i * fourth_of_width, fourth_of_width)] for i in range(4)],
                      lat_x, partner, core)
    lat_ring.start()
    for load in loads[1:]:
        load.wait()
    ukvT[0:2 * PLAIN, :] = uk[...].astype(F32).T.astype(BF)
    ukvT[2 * PLAIN:2 * PLAIN + VROWS, :] = uv[...].astype(F32).T.astype(BF)
    q_gain_ref[...] = jnp.broadcast_to(qg_ref[...], (8, qg_ref.shape[1])).T[:, 0:1]
    kv_gain_ref[...] = jnp.broadcast_to(kg_ref[...], (8, kg_ref.shape[1])).T[:, 0:1]
    pos = lax.broadcasted_iota(jnp.int32, (8, tok), 1) + z * tok
    freq = jnp.exp(lax.broadcasted_iota(jnp.int32, (8, tok), 0).astype(F32) * (-math.log(10000.0) / 8))
    row_angle = (pos >> 6).astype(F32) * freq
    col_angle = (pos & (GRID_W - 1)).astype(F32) * freq
    turn = (jnp.cos(row_angle), jnp.sin(row_angle), jnp.cos(col_angle), jnp.sin(col_angle))

    def chip_rows(p):
        return jnp.concatenate([lat[2 * p].astype(F32), lat[2 * p + 1].astype(F32)], axis=0)

    def note_statistics(p):
        values = chip_rows(p)
        center = values - jnp.mean(values, axis=-1, keepdims=True)
        mean_ref[p] = jnp.mean(values, axis=-1, keepdims=True)
        rstd_ref[p] = lax.rsqrt(jnp.mean(center * center, axis=-1, keepdims=True) + EPSILON)

    lat_ring.step(1)
    far = lat_ring.reach
    for s in range(2, far + 1):
        lat_ring.pair_step(s - 2)

        @pl.loop(0, 1 if s == 2 else 2)
        def _(i):
            note_statistics(lax.rem(chip + jnp.where(i == 0, nx - (s - 2), s - 2), nx))

        lat_ring.step(s)
        if s == min(2, far):
            for k in reversed(order):
                zm(k, True).wait_recv()
            total = zmod[0]
            for k in range(1, nz):
                total = total + zmod[k]
            xmod[t] = total
            for k in range(1, nt):
                xm(k, False).start()
    lat_ring.pair_step(far - 1)

    @pl.loop(0, 2 if far > 1 else 1)
    def _(i):
        note_statistics(lax.rem(chip + jnp.where(i == 0, nx - (far - 1), far - 1), nx))

    lat_ring.pair_step(far)
    note_statistics(lax.rem(chip + far, nx))
    for k in range(1, nt):
        xm(k, True).wait_recv()
    for j in range(nt):
        mod[:, j * part:(j + 1) * part] = xmod[j]

    @pl.loop(0, nx)
    def _(p):
        at = pl.ds(pl.multiple_of(p * 2 * rows, 2 * rows), 2 * rows)
        normed = (chip_rows(p) - mean_ref[p]) * rstd_ref[p]
        h[at, :] = (normed * (1.0 + mod[2:3, :]) + mod[0:1, :]).astype(BF)

    h[tok:, :] = modulated(ctx[...], mod[1:2, :], mod[3:4, :])
    product = lax.dot_general(h[...], wcat[...], (((1,), (1,)), ((), ())), preferred_element_type=F32)
    raw = product[0:tok].T
    rawc = jnp.concatenate([product[tok:], jnp.zeros((128 - crows, product.shape[1]), F32)], axis=0).T
    q_at = lambda p, c, i: pl.ds(pl.multiple_of((2 * p + c) * rank_q + i * (rank_q // 2), rank_q // 2), rank_q // 2)
    kv_at = lambda p, c: pl.ds(pl.multiple_of((2 * p + c) * rank_kv, rank_kv), rank_kv)
    kvraw[kv_at(chip, core), 0:tok] = raw[rank_q:rank_q + rank_kv].astype(BF)
    kvraw[kv_at(chip, core), tok:] = rawc[rank_q:rank_q + rank_kv].astype(BF)
    lane_half = kvraw.shape[1] // 2
    opposite = nx // 2

    def raw_piece(k, side, c):
        piece = kvraw.at[kv_at(lax.rem(chip + nx - k, nx), c)]
        return piece if side is None else kvraw.at[kv_at(lax.rem(chip + nx - k, nx), c), pl.ds(side * lane_half, lane_half)]

    def raw_copy(k, incoming):
        piece = raw_piece(k if incoming else 0, None, core)
        return pltpu.make_async_remote_copy(piece, piece, raw_s.at[k], raw_r.at[k], device_id=along_x(k), device_id_type=MESH)

    def raw_last(side, incoming):
        near = 1 if side == 0 else nx - 1
        piece = raw_piece(opposite if incoming else near, side, core)
        at = opposite if side == 0 else nx
        return pltpu.make_async_remote_copy(piece, piece, raw_s.at[at], raw_r.at[at],
                                            device_id=along_x(opposite - 1 if side == 0 else nx - opposite + 1), device_id_type=MESH)

    def raw_pair(k, incoming):
        piece = raw_piece(k, None, 1 - core if incoming else core)
        return pltpu.make_async_remote_copy(piece, piece, rawp_s.at[k], rawp_r.at[k], device_id=partner, device_id_type=MESH)

    by_distance = [k for m in range(1, opposite) for k in (m, nx - m)]
    for k in by_distance:
        raw_copy(k, False).start()
    raw_pair(0, False).start()
    qraw[pl.ds(pl.multiple_of(t * rank_q, rank_q), rank_q), :] = raw[0:rank_q].astype(BF)
    q_ring = Gather(nx, chip, along_x,
                    [lambda p, c: qraw.at[q_at(p, c, 0), :], lambda p, c: qraw.at[q_at(p, c, 1), :]],
                    q_x, partner, core)
    q_ring.start()
    own_last = lambda a: jnp.where(core == 0, jnp.concatenate([a[ROTARY // 2:], a[:ROTARY // 2]], axis=0), a)
    kv[z, 2 * PLAIN:KROWS, :] = own_last(axial_turn(raw[rank_q + rank_kv:], *turn)).astype(BF)
    for i in range(4):
        turn_ref[i] = turn[i]
    for k in by_distance:
        raw_copy(k, True).wait_recv()
        if k in (1, nx - 1):
            raw_last(0 if k == 1 else 1, False).start()
        raw_pair(k, False).start()
    q_ring.step(1)
    for side in range(2):
        raw_last(side, True).wait_recv()
    raw_pair(opposite, False).start()
    for k in range(nx):
        raw_pair(k, True).wait_recv()

    ckv = rms_columns(kvraw[...], kv_gain_ref[...])
    own = jnp.dot(ukvT[...], ckv, preferred_element_type=F32).astype(BF)
    kv[z, 0:2 * PLAIN, :] = own[0:2 * PLAIN, 0:tok]
    kv[z, KROWS:KROWS + VROWS, :] = own[2 * PLAIN:, 0:tok]
    loose = jnp.concatenate([own[0:2 * PLAIN, tok:].astype(F32), own_last(rawc[rank_q + rank_kv:]).astype(BF).astype(F32), own[2 * PLAIN:, tok:].astype(F32)], axis=0)
    group = (KROWS + VROWS) // 4
    packed = loose[0:group]
    for g in range(1, 4):
        packed = packed + pltpu.roll(loose[g * group:(g + 1) * group], g * crows, 1)
    kvp[z] = jnp.concatenate([packed, jnp.zeros((kvp.shape[1] - group, 128), F32)], axis=0).astype(BF)
    kr_half = ROTARY // 2
    top = 2 * PLAIN + kr_half
    kv_chunks = [lambda p, c: kv.at[p, pl.ds(0, PLAIN)], lambda p, c: kv.at[p, pl.ds(PLAIN, PLAIN)], lambda p, c: kvp.at[p],
                 lambda p, c: kv.at[p, pl.ds(top, kr_half + VALUE)], lambda p, c: kv.at[p, pl.ds(top + kr_half + VALUE, VALUE)]]
    kv_ring = Gather(nz, z, along_z, kv_chunks, kv_z)
    kv_ring.start()

    def query_up():
        for s in range(0, q_ring.reach + 1):
            q_ring.pair_step(s)
        cq = rms_columns(qraw[...], q_gain_ref[...])
        q = jnp.dot(uqT[...], cq, preferred_element_type=F32)
        per = PLAIN + ROTARY
        for head in range(2):
            mine = q[head * per:(head + 1) * per]
            plain = mine[0:PLAIN].astype(BF)
            blank = jnp.zeros_like(plain)
            qb[head, head * PLAIN:(head + 1) * PLAIN, :] = plain
            qb[head, (1 - head) * PLAIN:(2 - head) * PLAIN, :] = blank
            qb[head, 2 * PLAIN:KROWS, :] = own_last(axial_turn(mine[PLAIN:], *[turn_ref[i] for i in range(4)])).astype(BF)

    m_ref[...] = jnp.full_like(m_ref, NEGATIVE)
    l_ref[...] = jnp.zeros_like(l_ref)
    acc[...] = jnp.zeros_like(acc)

    def attend(keysT, valuesT, biased):
        keys = keysT.astype(F32).T.astype(BF)
        for head in range(2):
            s = jnp.dot(keys, qb[head], preferred_element_type=F32) * (SCORE * LOG2E)
            if biased:
                s = s + bias_ref[0, head] * LOG2E
            old = m_ref[head]
            new = jnp.maximum(old, jnp.max(s, axis=0, keepdims=True))
            alpha = jnp.exp2(old - new)
            e = jnp.exp2(s - new)
            m_ref[head] = new
            l_ref[head] = l_ref[head] * alpha + jnp.sum(e, axis=0, keepdims=True)
            acc[head] = acc[head] * alpha + jnp.dot(valuesT[head * VALUE:(head + 1) * VALUE], e.astype(BF), preferred_element_type=F32)

    reach = kv_ring.reach

    def ring_source(d, s):
        return lax.rem(z + jnp.where(d == 0, nz - s, s), nz)

    def nth_source(n):
        return ring_source(1 - lax.rem(n, 2), (n + 1) // 2)

    def hop(d, s, ch, into):
        piece = kv_chunks[ch](ring_source(d, s), 0)
        return pltpu.make_async_remote_copy(piece, piece, kv_z[1].at[d, s, ch], kv_z[0].at[d, into, ch],
                                            device_id=along_z(1 if d == 0 else nz - 1), device_id_type=MESH)

    def kr_swap(d, s, incoming):
        b = ring_source(d, s)
        mine, theirs = kv.at[b, pl.ds(2 * PLAIN + kr_half, kr_half)], kv.at[b, pl.ds(2 * PLAIN, kr_half)]
        return pltpu.make_async_remote_copy(theirs if incoming else mine, theirs, kr_s.at[d, s], kr_r.at[d, s],
                                            device_id=partner, device_id_type=MESH)

    def pass_on(s, ch):
        for d in range(2):
            hop(d, s, ch, s).wait_recv()
            if d == ch // 3:
                hop(d, s, ch, s + 1).start()
            else:
                @pl.when(s + 1 < reach)
                def _():
                    hop(d, s, ch, s + 1).start()
            if ch == 3:
                kr_swap(d, s, False).start()

    def attend_block(n):
        b = nth_source(n)
        attend(kv[b, 0:KROWS, :], kv[b, KROWS:KROWS + VROWS, :], False)

    def unpack(tile):
        lanes = lax.broadcasted_iota(jnp.int32, (group, 128), 1) // crows
        parts = [None] * 4
        for j in range(4):
            held = kvp[nth_source(4 * tile + j)][0:group].astype(F32)
            for g in range(4):
                moved = jnp.where(lanes == g, held, 0.0)
                if g != j:
                    moved = pltpu.roll(moved, ((j - g) % 4) * crows, 1)
                parts[g] = moved if parts[g] is None else parts[g] + moved
        kvc[:, tile * 128:(tile + 1) * 128] = jnp.concatenate(parts, axis=0).astype(BF)

    slots = 4 * (reach - 1)
    first = min(2, q_ring.reach - 1)
    tiles = nz // 4

    def done_after(j):
        return jnp.clip(2 * (j - first + 1), 0, j)

    def context_tiles():
        for tile in range(tiles - 1):
            unpack(tile)
        attend(kvc[0:KROWS, 0:128 * (tiles - 1)], kvc[KROWS:KROWS + VROWS, 0:128 * (tiles - 1)], True)

    def kv_slot(i, carry):
        s = i // 4 + 1

        @pl.when(lax.rem(i, 4) == 0)
        def _():
            pass_on(s, 0)

            @pl.when(s > 1)
            def _():
                for d in range(2):
                    kr_swap(d, s - 1, True).wait_recv()

        @pl.when(lax.rem(i, 4) == 1)
        def _():
            pass_on(s, 1)
            pass_on(s, 2)

        for part_of in (2, 3):
            @pl.when(lax.rem(i, 4) == part_of)
            def _():
                pass_on(s, part_of + 1)

        for step in range(2, q_ring.reach + 1):
            @pl.when(i == 2 * (step - 2))
            def _():
                q_ring.step(step)
                if step == q_ring.reach:
                    query_up()

        if tiles > 1:
            @pl.when(i == slots - 4)
            def _():
                context_tiles()

        @pl.when(lax.rem(i, 2) == 1)
        def _():
            j = i // 2

            @pl.loop(jnp.where(j > first, done_after(j - 1), 0), jnp.where(j >= first, done_after(j), 0))
            def _(n):
                attend_block(n)
        return carry

    lax.fori_loop(0, slots, kv_slot, 0)
    for d in range(2):
        kr_swap(d, reach - 1, True).wait_recv()

    @pl.loop(done_after(slots // 2 - 1), 2 * reach - 1)
    def _(n):
        attend_block(n)
    kv_ring.ring_arrival(0, reach, 0).wait_recv()
    for d, ch in ((0, 1), (0, 2), (1, 3), (1, 4)):
        kv_ring.ring_arrival(d, reach, ch).wait_recv()
    kr_swap(0, reach, False).start()
    unpack(tiles - 1)
    kr_swap(0, reach, True).wait_recv()
    attend_block(2 * reach - 1)
    attend(kvc[0:KROWS, 128 * (tiles - 1):], kvc[KROWS:KROWS + VROWS, 128 * (tiles - 1):], True)

    outT = jnp.concatenate([acc[0] / l_ref[0], acc[1] / l_ref[1]], axis=0)
    mine_at = lambda p, c: pl.ds(pl.multiple_of((2 * p + c) * VROWS, VROWS), VROWS)
    att[:, mine_at(chip, core)] = outT.T.astype(BF)
    fourth = tok // 4
    att_ring = Gather(nx, chip, along_x,
                      [lambda p, c, i=i: att.at[pl.ds(i * fourth, fourth), mine_at(p, c)] for i in range(4)],
                      att_x, partner, core)
    att_ring.start()
    for s in range(1, att_ring.reach + 1):
        att_ring.step(s)

    def am(k, incoming):
        far = lax.rem(t + nt - k, nt) if incoming else lax.rem(t + k, nt)
        if incoming:
            return pltpu.make_async_remote_copy(pbuf.at[far], mbuf.at[far], a_s.at[k], a_r.at[k], device_id={"tp": far}, device_id_type=MESH)
        return pltpu.make_async_remote_copy(pbuf.at[far], mbuf.at[t], a_s.at[k], a_r.at[k], device_id={"tp": far}, device_id_type=MESH)

    for s in range(0, att_ring.reach + 1):
        att_ring.pair_step(s)
    proj = jnp.dot(att[...], wo[...], preferred_element_type=F32)
    for j in range(nt):
        pbuf[j] = proj[j * rows:(j + 1) * rows].astype(BF)
    for k in sorted(range(1, nt), key=lambda k: -min(k, nt - k)):
        am(k, False).start()
    mbuf[t] = pbuf[t]
    gate_ref[...] = mod[4:5, :]
    for k in range(1, nt):
        am(k, True).wait_recv()
    for j in range(nt):
        cut = slice(j * part, (j + 1) * part)
        proj_ref[:, cut] = mbuf[j]

    for k in range(1, nz):
        zm(k, False).wait_send()
    for k in range(1, nt):
        xm(k, False).wait_send()
        am(k, False).wait_send()
    lat_ring.finish()
    for k in by_distance:
        raw_copy(k, False).wait_send()
    for side in range(2):
        raw_last(side, False).wait_send()
    for k in range(nx):
        raw_pair(k, False).wait_send()
    for s in range(1, reach + 1):
        for d in range(2 if s < reach else 1):
            kr_swap(d, s, False).wait_send()
    q_ring.finish()
    kv_ring.finish()
    att_ring.finish()


def sems(count, chunks, paired):
    kinds = 4 if paired else 2
    return tuple(pltpu.SemaphoreType.DMA((2, count // 2 + 2, chunks)) for _ in range(kinds))


def on_device(latents, conditions, context, w_shift, w_scale, w_gate, w_qdown, w_kvdown, w_rope, q_gain,
              latent_norm_gain, query_up_weight, key_up_weight, value_up_weight, context_bias, w_out):
    nz, nt = lax.axis_size("sp"), lax.axis_size("tp")
    nx = nt // 2
    rows, width = latents.shape
    tok = rows * nt
    crows = context.shape[0]
    rank_q, rank_kv = w_qdown.shape[1], w_kvdown.shape[1]
    part = width // nt
    vm = pltpu.VMEM
    dma = pltpu.SemaphoreType.DMA
    scratch = [
        vm((nt, rows, width), BF), vm((crows, width), BF), vm((nx, 2 * rows, 1), F32), vm((nx, 2 * rows, 1), F32),
        vm(key_up_weight.shape, BF), vm(value_up_weight.shape, BF), vm(w_out.shape, BF),
        vm((rank_q + rank_kv + ROTARY, width), BF), vm(query_up_weight.shape[::-1], BF), vm((2 * PLAIN + VROWS, nt * rank_kv), BF),
        vm((nz, 8, part), F32), vm((nt, 8, part), F32), vm((8, width), F32),
        vm((tok + crows, width), BF),
        vm((nt * rank_q, tok), BF), vm((nt * rank_kv, tok + 128), BF),
        vm((nz, KROWS + VROWS, tok), BF), vm((nz, 80, 128), BF), vm((KROWS + VROWS, nz * crows), BF), vm((2, KROWS, tok), BF),
        vm((2, 1, tok), F32), vm((2, 1, tok), F32), vm((2, VALUE, tok), F32),
        vm((tok, nt * VROWS), BF), vm((nt, rows, part), BF), vm((nt, rows, part), BF),
        vm((nt * rank_q, 1), F32), vm((nt * rank_kv, 1), F32), vm((4, 8, tok), F32),
        dma((9,)), dma((nz,)), dma((nz,)), dma((nt,)), dma((nt,)), dma((nt,)), dma((nt,)),
        sems(nx, 4, True), dma((nx + 1,)), dma((nx + 1,)), dma((nx,)), dma((nx,)), sems(nx, 2, True), sems(nz, 5, False),
        dma((2, nz // 2 + 1)), dma((2, nz // 2 + 1)), sems(nx, 4, True),
    ]
    here = pl.BlockSpec(memory_space=vm)
    away = pl.BlockSpec(memory_space=pl.ANY)
    small = pl.BlockSpec(memory_space=pltpu.SMEM)
    proj, gate = pl.pallas_call(
        functools.partial(kernel, nz, nt),
        out_shape=(jax.ShapeDtypeStruct((rows, width), BF), jax.ShapeDtypeStruct((1, width), F32)),
        in_specs=[away, here, away, here, here, here, away, away, away, here, here, away, away, away, small, away],
        out_specs=(here, here),
        scratch_shapes=scratch,
        compiler_params=pltpu.CompilerParams(collective_id=0, has_side_effects=True, vmem_limit_bytes=60 * 1024 * 1024),
        name="block",
    )(latents, conditions, context, w_shift, w_scale, w_gate, w_qdown.T, w_kvdown.T, w_rope.T, q_gain.reshape(1, -1),
      latent_norm_gain.reshape(1, -1), query_up_weight.T, key_up_weight, value_up_weight, context_bias.reshape(1, -1), w_out)
    return (latents.astype(F32) + gate * proj.astype(F32)).astype(BF)


def solution(mesh):
    in_specs = (
        P(("grp", "sp", "tp"), None),
        P("grp", "sp"),
        P(("grp", "sp"), None),
        P("sp", "tp"),
        P("sp", "tp"),
        P("sp", "tp"),
        P(None, "tp"),
        P(None, "tp"),
        P(),
        P(),
        P(),
        P(None, "tp"),
        P(None, "tp"),
        P(None, "tp"),
        P("tp"),
        P(None, "tp"),
    )
    return jax.shard_map(on_device, mesh=mesh, in_specs=in_specs, out_specs=P(("grp", "sp", "tp"), None), check_vma=False)
```

```python
import functools
import math

import jax
import jax.numpy as jnp
from jax import lax
from jax.experimental import pallas as pl
from jax.experimental.pallas import tpu as pltpu
from jax.sharding import PartitionSpec as P

PLAIN = 64
ROTARY = 32
VALUE = 64
GRID_W = 64
EPSILON = 1e-6
NEGATIVE = -1e30
LOG2E = 1.4426950408889634
SCORE = (PLAIN + ROTARY) ** (-0.5)
MESH = pl.DeviceIdType.MESH
BF = jnp.bfloat16
F32 = jnp.float32
KROWS = 2 * PLAIN + ROTARY
VROWS = 2 * VALUE


class Gather:
    def __init__(self, count, place, towards, chunks, sems, partner=None, core=0):
        self.count, self.place, self.towards = count, place, towards
        self.chunks, self.partner, self.core = chunks, partner, core
        self.recv, self.send = sems[0], sems[1]
        self.pair_recv, self.pair_send = (sems[2], sems[3]) if partner is not None else (None, None)
        self.reach = count // 2
        self.cut = (len(chunks) + 1) // 2

    def active(self, d, s, ch):
        if s < self.reach:
            return True
        if s > self.reach:
            return False
        return (ch < self.cut) if d == 0 else (ch >= self.cut)

    def source(self, d, s):
        move = (self.count - s) if d == 0 else s
        return lax.rem(self.place + move, self.count)

    def ring_copy(self, d, s, ch):
        piece = self.chunks[ch](self.source(d, s), self.core)
        return pltpu.make_async_remote_copy(
            src_ref=piece, dst_ref=piece, send_sem=self.send.at[d, s, ch], recv_sem=self.recv.at[d, s + 1, ch],
            device_id=self.towards(1 if d == 0 else self.count - 1), device_id_type=MESH)

    def ring_arrival(self, d, s, ch):
        piece = self.chunks[ch](self.source(d, s), self.core)
        return pltpu.make_async_remote_copy(
            src_ref=piece, dst_ref=piece, send_sem=self.send.at[d, s, ch], recv_sem=self.recv.at[d, s, ch],
            device_id=self.towards(self.count - 1 if d == 0 else 1), device_id_type=MESH)

    def pair_copy(self, d, s, ch, core):
        piece = self.chunks[ch](self.source(d, s), core)
        return pltpu.make_async_remote_copy(
            src_ref=piece, dst_ref=piece, send_sem=self.pair_send.at[d, s, ch], recv_sem=self.pair_recv.at[d, s, ch],
            device_id=self.partner, device_id_type=MESH)

    def start(self, only=None):
        for ch in range(len(self.chunks)) if only is None else only:
            for d in range(2):
                if self.active(d, 1, ch):
                    self.ring_copy(d, 0, ch).start()
            if self.partner is not None:
                self.pair_copy(0, 0, ch, self.core).start()

    def step(self, s):
        for ch in range(len(self.chunks)):
            for d in range(2):
                if self.active(d, s, ch):
                    self.ring_arrival(d, s, ch).wait_recv()
                    if self.active(d, s + 1, ch):
                        self.ring_copy(d, s, ch).start()
                    if self.partner is not None:
                        self.pair_copy(d, s, ch, self.core).start()

    def pair_step(self, s, only=None):
        for ch in range(len(self.chunks)) if only is None else only:
            for d in range(2):
                if (s == 0 and d == 0) or (s > 0 and self.active(d, s, ch)):
                    self.pair_copy(d, s, ch, 1 - self.core).wait_recv()

    def finish(self):
        for s in range(self.reach + 1):
            for ch in range(len(self.chunks)):
                for d in range(2):
                    if self.active(d, s + 1, ch):
                        self.ring_copy(d, s, ch).wait_send()
                    if self.partner is not None and ((s == 0 and d == 0) or (s > 0 and self.active(d, s, ch))):
                        self.pair_copy(d, s, ch, self.core).wait_send()


def axial_turn(a, row_cos, row_sin, col_cos, col_sin):
    a0, a1, a2, a3 = a[0:8], a[8:16], a[16:24], a[24:32]
    return jnp.concatenate(
        [a0 * row_cos - a1 * row_sin, a0 * row_sin + a1 * row_cos,
         a2 * col_cos - a3 * col_sin, a2 * col_sin + a3 * col_cos], axis=0)


def modulated(block, shift, scale):
    values = block.astype(F32)
    center = values - jnp.mean(values, axis=-1, keepdims=True)
    spread = jnp.mean(center * center, axis=-1, keepdims=True)
    return (center * lax.rsqrt(spread + EPSILON) * (1.0 + scale) + shift).astype(BF)


def rms_columns(raw, gain):
    values = raw.astype(F32)
    factor = lax.rsqrt(jnp.mean(values * values, axis=0, keepdims=True) + EPSILON)
    return (values * factor * gain).astype(BF)


def kernel(nz, nt, *refs):
    (lat_hbm, cond_ref, ctx_hbm, wsh_ref, wsc_ref, wg_ref, wq_hbm, wkv_hbm, wr_hbm, qg_ref, kg_ref,
     uq_hbm, uk_hbm, uv_hbm, bias_ref, wo_hbm, proj_ref, gate_ref,
     lat, ctx, mean_ref, rstd_ref, uk, uv, wo,
     wcat, uqT, ukvT, zmod, xmod, mod, h, qraw, kvraw, kv, kvp, kvc, qb,
     m_ref, l_ref, acc, att, pbuf, mbuf, q_gain_ref, kv_gain_ref, turn_ref,
     load_sem, zm_s, zm_r, xm_s, xm_r, a_s, a_r, lat_x, raw_s, raw_r, rawp_s, rawp_r, q_x, kv_z, kr_s, kr_r, att_x) = refs
    z, t = lax.axis_index("sp"), lax.axis_index("tp")
    core = lax.rem(t, 2)
    chip = t // 2
    nx = nt // 2
    rows = lat.shape[1]
    tok = rows * nt
    crows = ctx.shape[0]
    width = lat.shape[2]
    part = width // nt
    rank_q, rank_kv = wq_hbm.shape[0], wkv_hbm.shape[0]
    along_z = lambda k: {"sp": lax.rem(z + k, nz)}
    along_x = lambda k: {"tp": lax.rem(t + 2 * k, nt)}
    partner = {"tp": t + 1 - 2 * core}
    fourth_of_width = width // 4

    loads = [
        pltpu.make_async_copy(lat_hbm, lat.at[t], load_sem.at[0]),
        pltpu.make_async_copy(ctx_hbm, ctx, load_sem.at[1]),
        pltpu.make_async_copy(wq_hbm, wcat.at[pl.ds(0, rank_q)], load_sem.at[2]),
        pltpu.make_async_copy(wkv_hbm, wcat.at[pl.ds(rank_q, rank_kv)], load_sem.at[3]),
        pltpu.make_async_copy(wr_hbm, wcat.at[pl.ds(rank_q + rank_kv, ROTARY)], load_sem.at[4]),
        pltpu.make_async_copy(uq_hbm, uqT, load_sem.at[5]),
        pltpu.make_async_copy(uk_hbm, uk, load_sem.at[6]),
        pltpu.make_async_copy(uv_hbm, uv, load_sem.at[7]),
        pltpu.make_async_copy(wo_hbm, wo, load_sem.at[8]),
    ]
    barrier = pltpu.get_barrier_semaphore()
    for k in range(1, nz):
        pl.semaphore_signal(barrier, inc=1, device_id=along_z(k), device_id_type=MESH)
    for k in range(1, nt):
        pl.semaphore_signal(barrier, inc=1, device_id={"tp": lax.rem(t + k, nt)}, device_id_type=MESH)
    for load in loads:
        load.start()

    cond = cond_ref[...]
    act = cond / (1.0 + jnp.exp(-cond))
    act = jnp.concatenate([act, jnp.zeros((14, act.shape[1]), F32)], axis=0).astype(BF)
    shift_part = jnp.dot(act, wsh_ref[...], preferred_element_type=F32)
    scale_part = jnp.dot(act, wsc_ref[...], preferred_element_type=F32)
    gate_part = jnp.dot(act, wg_ref[...], preferred_element_type=F32)
    zmod[z] = jnp.concatenate([shift_part[0:2], scale_part[0:2], gate_part[0:2], gate_part[2:4]], axis=0)
    pl.semaphore_wait(barrier, nz + nt - 2)

    def zm(k, incoming):
        if incoming:
            src = lax.rem(z + nz - k, nz)
            return pltpu.make_async_remote_copy(zmod.at[src], zmod.at[src], zm_s.at[k], zm_r.at[k], device_id=along_z(nz - k), device_id_type=MESH)
        return pltpu.make_async_remote_copy(zmod.at[z], zmod.at[z], zm_s.at[k], zm_r.at[k], device_id=along_z(k), device_id_type=MESH)

    def xm(k, incoming):
        if incoming:
            src = lax.rem(t + nt - k, nt)
            return pltpu.make_async_remote_copy(xmod.at[src], xmod.at[src], xm_s.at[k], xm_r.at[k], device_id={"tp": src}, device_id_type=MESH)
        return pltpu.make_async_remote_copy(xmod.at[t], xmod.at[t], xm_s.at[k], xm_r.at[k], device_id={"tp": lax.rem(t + k, nt)}, device_id_type=MESH)

    order = sorted(range(1, nz), key=lambda k: -min(k, nz - k))
    for k in order:
        zm(k, False).start()
    loads[0].wait()
    lat_ring = Gather(nx, chip, along_x,
                      [lambda p, c, i=i: lat.at[2 * p + c, :, pl.ds(i * fourth_of_width, fourth_of_width)] for i in range(4)],
                      lat_x, partner, core)
    lat_ring.start()
    for load in loads[1:]:
        load.wait()
    ukvT[0:2 * PLAIN, :] = uk[...].astype(F32).T.astype(BF)
    ukvT[2 * PLAIN:2 * PLAIN + VROWS, :] = uv[...].astype(F32).T.astype(BF)
    q_gain_ref[...] = jnp.broadcast_to(qg_ref[...], (8, qg_ref.shape[1])).T[:, 0:1]
    kv_gain_ref[...] = jnp.broadcast_to(kg_ref[...], (8, kg_ref.shape[1])).T[:, 0:1]
    pos = lax.broadcasted_iota(jnp.int32, (8, tok), 1) + z * tok
    freq = jnp.exp(lax.broadcasted_iota(jnp.int32, (8, tok), 0).astype(F32) * (-math.log(10000.0) / 8))
    row_angle = (pos >> 6).astype(F32) * freq
    col_angle = (pos & (GRID_W - 1)).astype(F32) * freq
    turn = (jnp.cos(row_angle), jnp.sin(row_angle), jnp.cos(col_angle), jnp.sin(col_angle))

    def chip_rows(p):
        return jnp.concatenate([lat[2 * p].astype(F32), lat[2 * p + 1].astype(F32)], axis=0)

    def note_statistics(p):
        values = chip_rows(p)
        center = values - jnp.mean(values, axis=-1, keepdims=True)
        mean_ref[p] = jnp.mean(values, axis=-1, keepdims=True)
        rstd_ref[p] = lax.rsqrt(jnp.mean(center * center, axis=-1, keepdims=True) + EPSILON)

    lat_ring.step(1)
    far = lat_ring.reach
    for s in range(2, far + 1):
        lat_ring.pair_step(s - 2)

        @pl.loop(0, 1 if s == 2 else 2)
        def _(i):
            note_statistics(lax.rem(chip + jnp.where(i == 0, nx - (s - 2), s - 2), nx))

        lat_ring.step(s)
        if s == min(2, far):
            for k in reversed(order):
                zm(k, True).wait_recv()
            total = zmod[0]
            for k in range(1, nz):
                total = total + zmod[k]
            xmod[t] = total
            for k in range(1, nt):
                xm(k, False).start()
    lat_ring.pair_step(far - 1)

    @pl.loop(0, 2 if far > 1 else 1)
    def _(i):
        note_statistics(lax.rem(chip + jnp.where(i == 0, nx - (far - 1), far - 1), nx))

    lat_ring.pair_step(far)
    note_statistics(lax.rem(chip + far, nx))
    for k in range(1, nt):
        xm(k, True).wait_recv()
    for j in range(nt):
        mod[:, j * part:(j + 1) * part] = xmod[j]

    @pl.loop(0, nx)
    def _(p):
        at = pl.ds(pl.multiple_of(p * 2 * rows, 2 * rows), 2 * rows)
        normed = (chip_rows(p) - mean_ref[p]) * rstd_ref[p]
        h[at, :] = (normed * (1.0 + mod[2:3, :]) + mod[0:1, :]).astype(BF)

    h[tok:, :] = modulated(ctx[...], mod[1:2, :], mod[3:4, :])
    product = lax.dot_general(h[...], wcat[...], (((1,), (1,)), ((), ())), preferred_element_type=F32)
    raw = product[0:tok].T
    rawc = jnp.concatenate([product[tok:], jnp.zeros((128 - crows, product.shape[1]), F32)], axis=0).T
    q_at = lambda p, c, i: pl.ds(pl.multiple_of((2 * p + c) * rank_q + i * (rank_q // 2), rank_q // 2), rank_q // 2)
    kv_at = lambda p, c: pl.ds(pl.multiple_of((2 * p + c) * rank_kv, rank_kv), rank_kv)
    kvraw[kv_at(chip, core), 0:tok] = raw[rank_q:rank_q + rank_kv].astype(BF)
    kvraw[kv_at(chip, core), tok:] = rawc[rank_q:rank_q + rank_kv].astype(BF)
    lane_half = kvraw.shape[1] // 2
    opposite = nx // 2

    def raw_piece(k, side, c):
        piece = kvraw.at[kv_at(lax.rem(chip + nx - k, nx), c)]
        return piece if side is None else kvraw.at[kv_at(lax.rem(chip + nx - k, nx), c), pl.ds(side * lane_half, lane_half)]

    def raw_copy(k, incoming):
        piece = raw_piece(k if incoming else 0, None, core)
        return pltpu.make_async_remote_copy(piece, piece, raw_s.at[k], raw_r.at[k], device_id=along_x(k), device_id_type=MESH)

    def raw_last(side, incoming):
        near = 1 if side == 0 else nx - 1
        piece = raw_piece(opposite if incoming else near, side, core)
        at = opposite if side == 0 else nx
        return pltpu.make_async_remote_copy(piece, piece, raw_s.at[at], raw_r.at[at],
                                            device_id=along_x(opposite - 1 if side == 0 else nx - opposite + 1), device_id_type=MESH)

    def raw_pair(k, incoming):
        piece = raw_piece(k, None, 1 - core if incoming else core)
        return pltpu.make_async_remote_copy(piece, piece, rawp_s.at[k], rawp_r.at[k], device_id=partner, device_id_type=MESH)

    by_distance = [k for m in range(1, opposite) for k in (m, nx - m)]
    for k in by_distance:
        raw_copy(k, False).start()
    raw_pair(0, False).start()
    qraw[pl.ds(pl.multiple_of(t * rank_q, rank_q), rank_q), :] = raw[0:rank_q].astype(BF)
    q_ring = Gather(nx, chip, along_x,
                    [lambda p, c: qraw.at[q_at(p, c, 0), :], lambda p, c: qraw.at[q_at(p, c, 1), :]],
                    q_x, partner, core)
    q_ring.start()
    own_last = lambda a: jnp.where(core == 0, jnp.concatenate([a[ROTARY // 2:], a[:ROTARY // 2]], axis=0), a)
    kv[z, 2 * PLAIN:KROWS, :] = own_last(axial_turn(raw[rank_q + rank_kv:], *turn)).astype(BF)
    for i in range(4):
        turn_ref[i] = turn[i]
    for k in by_distance:
        raw_copy(k, True).wait_recv()
        if k in (1, nx - 1):
            raw_last(0 if k == 1 else 1, False).start()
        raw_pair(k, False).start()
    q_ring.step(1)
    for side in range(2):
        raw_last(side, True).wait_recv()
    raw_pair(opposite, False).start()
    for k in range(nx):
        raw_pair(k, True).wait_recv()

    ckv = rms_columns(kvraw[...], kv_gain_ref[...])
    own = jnp.dot(ukvT[...], ckv, preferred_element_type=F32).astype(BF)
    kv[z, 0:2 * PLAIN, :] = own[0:2 * PLAIN, 0:tok]
    kv[z, KROWS:KROWS + VROWS, :] = own[2 * PLAIN:, 0:tok]
    loose = jnp.concatenate([own[0:2 * PLAIN, tok:].astype(F32), own_last(rawc[rank_q + rank_kv:]).astype(BF).astype(F32), own[2 * PLAIN:, tok:].astype(F32)], axis=0)
    group = (KROWS + VROWS) // 4
    packed = loose[0:group]
    for g in range(1, 4):
        packed = packed + pltpu.roll(loose[g * group:(g + 1) * group], g * crows, 1)
    kvp[z] = jnp.concatenate([packed, jnp.zeros((kvp.shape[1] - group, 128), F32)], axis=0).astype(BF)
    kr_half = ROTARY // 2
    top = 2 * PLAIN + kr_half
    kv_chunks = [lambda p, c: kv.at[p, pl.ds(0, PLAIN)], lambda p, c: kv.at[p, pl.ds(PLAIN, PLAIN)], lambda p, c: kvp.at[p],
                 lambda p, c: kv.at[p, pl.ds(top, kr_half + VALUE)], lambda p, c: kv.at[p, pl.ds(top + kr_half + VALUE, VALUE)]]
    kv_ring = Gather(nz, z, along_z, kv_chunks, kv_z)
    kv_ring.start()

    def query_up():
        for s in range(0, q_ring.reach + 1):
            q_ring.pair_step(s)
        cq = rms_columns(qraw[...], q_gain_ref[...])
        q = jnp.dot(uqT[...], cq, preferred_element_type=F32)
        per = PLAIN + ROTARY
        for head in range(2):
            mine = q[head * per:(head + 1) * per]
            plain = mine[0:PLAIN].astype(BF)
            blank = jnp.zeros_like(plain)
            qb[head, head * PLAIN:(head + 1) * PLAIN, :] = plain
            qb[head, (1 - head) * PLAIN:(2 - head) * PLAIN, :] = blank
            qb[head, 2 * PLAIN:KROWS, :] = own_last(axial_turn(mine[PLAIN:], *[turn_ref[i] for i in range(4)])).astype(BF)

    m_ref[...] = jnp.full_like(m_ref, NEGATIVE)
    l_ref[...] = jnp.zeros_like(l_ref)
    acc[...] = jnp.zeros_like(acc)

    def attend(keysT, valuesT, biased):
        keys = keysT.astype(F32).T.astype(BF)
        for head in range(2):
            s = jnp.dot(keys, qb[head], preferred_element_type=F32) * (SCORE * LOG2E)
            if biased:
                s = s + bias_ref[0, head] * LOG2E
            old = m_ref[head]
            new = jnp.maximum(old, jnp.max(s, axis=0, keepdims=True))
            alpha = jnp.exp2(old - new)
            e = jnp.exp2(s - new)
            m_ref[head] = new
            l_ref[head] = l_ref[head] * alpha + jnp.sum(e, axis=0, keepdims=True)
            acc[head] = acc[head] * alpha + jnp.dot(valuesT[head * VALUE:(head + 1) * VALUE], e.astype(BF), preferred_element_type=F32)

    reach = kv_ring.reach

    def ring_source(d, s):
        return lax.rem(z + jnp.where(d == 0, nz - s, s), nz)

    def nth_source(n):
        return ring_source(1 - lax.rem(n, 2), (n + 1) // 2)

    def hop(d, s, ch, into):
        piece = kv_chunks[ch](ring_source(d, s), 0)
        return pltpu.make_async_remote_copy(piece, piece, kv_z[1].at[d, s, ch], kv_z[0].at[d, into, ch],
                                            device_id=along_z(1 if d == 0 else nz - 1), device_id_type=MESH)

    def kr_swap(d, s, incoming):
        b = ring_source(d, s)
        mine, theirs = kv.at[b, pl.ds(2 * PLAIN + kr_half, kr_half)], kv.at[b, pl.ds(2 * PLAIN, kr_half)]
        return pltpu.make_async_remote_copy(theirs if incoming else mine, theirs, kr_s.at[d, s], kr_r.at[d, s],
                                            device_id=partner, device_id_type=MESH)

    def pass_on(s, ch):
        for d in range(2):
            hop(d, s, ch, s).wait_recv()
            if d == ch // 3:
                hop(d, s, ch, s + 1).start()
            else:
                @pl.when(s + 1 < reach)
                def _():
                    hop(d, s, ch, s + 1).start()
            if ch == 3:
                kr_swap(d, s, False).start()

    def attend_block(n):
        b = nth_source(n)
        attend(kv[b, 0:KROWS, :], kv[b, KROWS:KROWS + VROWS, :], False)

    def unpack(tile):
        lanes = lax.broadcasted_iota(jnp.int32, (group, 128), 1) // crows
        parts = [None] * 4
        for j in range(4):
            held = kvp[nth_source(4 * tile + j)][0:group].astype(F32)
            for g in range(4):
                moved = jnp.where(lanes == g, held, 0.0)
                if g != j:
                    moved = pltpu.roll(moved, ((j - g) % 4) * crows, 1)
                parts[g] = moved if parts[g] is None else parts[g] + moved
        kvc[:, tile * 128:(tile + 1) * 128] = jnp.concatenate(parts, axis=0).astype(BF)

    slots = 4 * (reach - 1)
    first = min(2, q_ring.reach - 1)
    tiles = nz // 4

    def done_after(j):
        return jnp.clip(2 * (j - first + 1), 0, j)

    def context_tiles():
        for tile in range(tiles - 1):
            unpack(tile)
        attend(kvc[0:KROWS, 0:128 * (tiles - 1)], kvc[KROWS:KROWS + VROWS, 0:128 * (tiles - 1)], True)

    def kv_slot(i, carry):
        s = i // 4 + 1

        @pl.when(lax.rem(i, 4) == 0)
        def _():
            pass_on(s, 0)

            @pl.when(s > 1)
            def _():
                for d in range(2):
                    kr_swap(d, s - 1, True).wait_recv()

        @pl.when(lax.rem(i, 4) == 1)
        def _():
            pass_on(s, 1)
            pass_on(s, 2)

        for part_of in (2, 3):
            @pl.when(lax.rem(i, 4) == part_of)
            def _():
                pass_on(s, part_of + 1)

        for step in range(2, q_ring.reach + 1):
            @pl.when(i == 2 * (step - 2))
            def _():
                q_ring.step(step)
                if step == q_ring.reach:
                    query_up()

        if tiles > 1:
            @pl.when(i == slots - 4)
            def _():
                context_tiles()

        @pl.when(lax.rem(i, 2) == 1)
        def _():
            j = i // 2

            @pl.loop(jnp.where(j > first, done_after(j - 1), 0), jnp.where(j >= first, done_after(j), 0))
            def _(n):
                attend_block(n)
        return carry

    lax.fori_loop(0, slots, kv_slot, 0)
    for d in range(2):
        kr_swap(d, reach - 1, True).wait_recv()

    @pl.loop(done_after(slots // 2 - 1), 2 * reach - 1)
    def _(n):
        attend_block(n)
    kv_ring.ring_arrival(0, reach, 0).wait_recv()
    for d, ch in ((0, 1), (0, 2), (1, 3), (1, 4)):
        kv_ring.ring_arrival(d, reach, ch).wait_recv()
    kr_swap(0, reach, False).start()
    unpack(tiles - 1)
    kr_swap(0, reach, True).wait_recv()
    attend_block(2 * reach - 1)
    attend(kvc[0:KROWS, 128 * (tiles - 1):], kvc[KROWS:KROWS + VROWS, 128 * (tiles - 1):], True)

    outT = jnp.concatenate([acc[0] / l_ref[0], acc[1] / l_ref[1]], axis=0)
    mine_at = lambda p, c: pl.ds(pl.multiple_of((2 * p + c) * VROWS, VROWS), VROWS)
    att[:, mine_at(chip, core)] = outT.T.astype(BF)
    rows_of = tok // 8
    att_ring = Gather(nx, chip, along_x,
                      [lambda p, c, i=i: att.at[pl.ds(i * rows_of, rows_of), mine_at(p, c)] for i in range(8)],
                      att_x, partner, core)
    att_ring.start()
    for s in range(1, att_ring.reach + 1):
        att_ring.step(s)

    def am(k, incoming):
        far = lax.rem(t + nt - k, nt) if incoming else lax.rem(t + k, nt)
        if incoming:
            return pltpu.make_async_remote_copy(pbuf.at[far], mbuf.at[far], a_s.at[k], a_r.at[k], device_id={"tp": far}, device_id_type=MESH)
        return pltpu.make_async_remote_copy(pbuf.at[far], mbuf.at[t], a_s.at[k], a_r.at[k], device_id={"tp": far}, device_id_type=MESH)

    for s in range(0, att_ring.reach + 1):
        att_ring.pair_step(s)
    proj = jnp.dot(att[...], wo[...], preferred_element_type=F32)
    for j in range(nt):
        pbuf[j] = proj[j * rows:(j + 1) * rows].astype(BF)
    for k in sorted(range(1, nt), key=lambda k: -min(k, nt - k)):
        am(k, False).start()
    mbuf[t] = pbuf[t]
    gate_ref[...] = mod[4:5, :]
    for k in range(1, nt):
        am(k, True).wait_recv()
    for j in range(nt):
        cut = slice(j * part, (j + 1) * part)
        proj_ref[:, cut] = mbuf[j]

    for k in range(1, nz):
        zm(k, False).wait_send()
    for k in range(1, nt):
        xm(k, False).wait_send()
        am(k, False).wait_send()
    lat_ring.finish()
    for k in by_distance:
        raw_copy(k, False).wait_send()
    for side in range(2):
        raw_last(side, False).wait_send()
    for k in range(nx):
        raw_pair(k, False).wait_send()
    for s in range(1, reach + 1):
        for d in range(2 if s < reach else 1):
            kr_swap(d, s, False).wait_send()
    q_ring.finish()
    kv_ring.finish()
    att_ring.finish()


def sems(count, chunks, paired):
    kinds = 4 if paired else 2
    return tuple(pltpu.SemaphoreType.DMA((2, count // 2 + 2, chunks)) for _ in range(kinds))


def on_device(latents, conditions, context, w_shift, w_scale, w_gate, w_qdown, w_kvdown, w_rope, q_gain,
              latent_norm_gain, query_up_weight, key_up_weight, value_up_weight, context_bias, w_out):
    nz, nt = lax.axis_size("sp"), lax.axis_size("tp")
    nx = nt // 2
    rows, width = latents.shape
    tok = rows * nt
    crows = context.shape[0]
    rank_q, rank_kv = w_qdown.shape[1], w_kvdown.shape[1]
    part = width // nt
    vm = pltpu.VMEM
    dma = pltpu.SemaphoreType.DMA
    scratch = [
        vm((nt, rows, width), BF), vm((crows, width), BF), vm((nx, 2 * rows, 1), F32), vm((nx, 2 * rows, 1), F32),
        vm(key_up_weight.shape, BF), vm(value_up_weight.shape, BF), vm(w_out.shape, BF),
        vm((rank_q + rank_kv + ROTARY, width), BF), vm(query_up_weight.shape[::-1], BF), vm((2 * PLAIN + VROWS, nt * rank_kv), BF),
        vm((nz, 8, part), F32), vm((nt, 8, part), F32), vm((8, width), F32),
        vm((tok + crows, width), BF),
        vm((nt * rank_q, tok), BF), vm((nt * rank_kv, tok + 128), BF),
        vm((nz, KROWS + VROWS, tok), BF), vm((nz, 80, 128), BF), vm((KROWS + VROWS, nz * crows), BF), vm((2, KROWS, tok), BF),
        vm((2, 1, tok), F32), vm((2, 1, tok), F32), vm((2, VALUE, tok), F32),
        vm((tok, nt * VROWS), BF), vm((nt, rows, part), BF), vm((nt, rows, part), BF),
        vm((nt * rank_q, 1), F32), vm((nt * rank_kv, 1), F32), vm((4, 8, tok), F32),
        dma((9,)), dma((nz,)), dma((nz,)), dma((nt,)), dma((nt,)), dma((nt,)), dma((nt,)),
        sems(nx, 4, True), dma((nx + 1,)), dma((nx + 1,)), dma((nx,)), dma((nx,)), sems(nx, 2, True), sems(nz, 5, False),
        dma((2, nz // 2 + 1)), dma((2, nz // 2 + 1)), sems(nx, 8, True),
    ]
    here = pl.BlockSpec(memory_space=vm)
    away = pl.BlockSpec(memory_space=pl.ANY)
    small = pl.BlockSpec(memory_space=pltpu.SMEM)
    proj, gate = pl.pallas_call(
        functools.partial(kernel, nz, nt),
        out_shape=(jax.ShapeDtypeStruct((rows, width), BF), jax.ShapeDtypeStruct((1, width), F32)),
        in_specs=[away, here, away, here, here, here, away, away, away, here, here, away, away, away, small, away],
        out_specs=(here, here),
        scratch_shapes=scratch,
        compiler_params=pltpu.CompilerParams(collective_id=0, has_side_effects=True, vmem_limit_bytes=60 * 1024 * 1024),
        name="block",
    )(latents, conditions, context, w_shift, w_scale, w_gate, w_qdown.T, w_kvdown.T, w_rope.T, q_gain.reshape(1, -1),
      latent_norm_gain.reshape(1, -1), query_up_weight.T, key_up_weight, value_up_weight, context_bias.reshape(1, -1), w_out)
    return (latents.astype(F32) + gate * proj.astype(F32)).astype(BF)


def solution(mesh):
    in_specs = (
        P(("grp", "sp", "tp"), None),
        P("grp", "sp"),
        P(("grp", "sp"), None),
        P("sp", "tp"),
        P("sp", "tp"),
        P("sp", "tp"),
        P(None, "tp"),
        P(None, "tp"),
        P(),
        P(),
        P(),
        P(None, "tp"),
        P(None, "tp"),
        P(None, "tp"),
        P("tp"),
        P(None, "tp"),
    )
    return jax.shard_map(on_device, mesh=mesh, in_specs=in_specs, out_specs=P(("grp", "sp", "tp"), None), check_vma=False)
```

```python
import functools
import math

import jax
import jax.numpy as jnp
from jax import lax
from jax.experimental import pallas as pl
from jax.experimental.pallas import tpu as pltpu
from jax.sharding import PartitionSpec as P

PLAIN = 64
ROTARY = 32
VALUE = 64
GRID_W = 64
EPSILON = 1e-6
NEGATIVE = -1e30
LOG2E = 1.4426950408889634
SCORE = (PLAIN + ROTARY) ** (-0.5)
MESH = pl.DeviceIdType.MESH
BF = jnp.bfloat16
F32 = jnp.float32
KROWS = 2 * PLAIN + ROTARY
VROWS = 2 * VALUE


class Gather:
    def __init__(self, count, place, towards, chunks, sems, partner=None, core=0):
        self.count, self.place, self.towards = count, place, towards
        self.chunks, self.partner, self.core = chunks, partner, core
        self.recv, self.send = sems[0], sems[1]
        self.pair_recv, self.pair_send = (sems[2], sems[3]) if partner is not None else (None, None)
        self.reach = count // 2
        self.cut = (len(chunks) + 1) // 2

    def active(self, d, s, ch):
        if s < self.reach:
            return True
        if s > self.reach:
            return False
        return (ch < self.cut) if d == 0 else (ch >= self.cut)

    def source(self, d, s):
        move = (self.count - s) if d == 0 else s
        return lax.rem(self.place + move, self.count)

    def ring_copy(self, d, s, ch):
        piece = self.chunks[ch](self.source(d, s), self.core)
        return pltpu.make_async_remote_copy(
            src_ref=piece, dst_ref=piece, send_sem=self.send.at[d, s, ch], recv_sem=self.recv.at[d, s + 1, ch],
            device_id=self.towards(1 if d == 0 else self.count - 1), device_id_type=MESH)

    def ring_arrival(self, d, s, ch):
        piece = self.chunks[ch](self.source(d, s), self.core)
        return pltpu.make_async_remote_copy(
            src_ref=piece, dst_ref=piece, send_sem=self.send.at[d, s, ch], recv_sem=self.recv.at[d, s, ch],
            device_id=self.towards(self.count - 1 if d == 0 else 1), device_id_type=MESH)

    def pair_copy(self, d, s, ch, core):
        piece = self.chunks[ch](self.source(d, s), core)
        return pltpu.make_async_remote_copy(
            src_ref=piece, dst_ref=piece, send_sem=self.pair_send.at[d, s, ch], recv_sem=self.pair_recv.at[d, s, ch],
            device_id=self.partner, device_id_type=MESH)

    def start(self, only=None):
        for ch in range(len(self.chunks)) if only is None else only:
            for d in range(2):
                if self.active(d, 1, ch):
                    self.ring_copy(d, 0, ch).start()
            if self.partner is not None:
                self.pair_copy(0, 0, ch, self.core).start()

    def step(self, s):
        for ch in range(len(self.chunks)):
            for d in range(2):
                if self.active(d, s, ch):
                    self.ring_arrival(d, s, ch).wait_recv()
                    if self.active(d, s + 1, ch):
                        self.ring_copy(d, s, ch).start()
                    if self.partner is not None:
                        self.pair_copy(d, s, ch, self.core).start()

    def pair_step(self, s, only=None):
        for ch in range(len(self.chunks)) if only is None else only:
            for d in range(2):
                if (s == 0 and d == 0) or (s > 0 and self.active(d, s, ch)):
                    self.pair_copy(d, s, ch, 1 - self.core).wait_recv()

    def finish(self):
        for s in range(self.reach + 1):
            for ch in range(len(self.chunks)):
                for d in range(2):
                    if self.active(d, s + 1, ch):
                        self.ring_copy(d, s, ch).wait_send()
                    if self.partner is not None and ((s == 0 and d == 0) or (s > 0 and self.active(d, s, ch))):
                        self.pair_copy(d, s, ch, self.core).wait_send()


def axial_turn(a, row_cos, row_sin, col_cos, col_sin):
    a0, a1, a2, a3 = a[0:8], a[8:16], a[16:24], a[24:32]
    return jnp.concatenate(
        [a0 * row_cos - a1 * row_sin, a0 * row_sin + a1 * row_cos,
         a2 * col_cos - a3 * col_sin, a2 * col_sin + a3 * col_cos], axis=0)


def modulated(block, shift, scale):
    values = block.astype(F32)
    center = values - jnp.mean(values, axis=-1, keepdims=True)
    spread = jnp.mean(center * center, axis=-1, keepdims=True)
    return (center * lax.rsqrt(spread + EPSILON) * (1.0 + scale) + shift).astype(BF)


def rms_columns(raw, gain):
    values = raw.astype(F32)
    factor = lax.rsqrt(jnp.mean(values * values, axis=0, keepdims=True) + EPSILON)
    return (values * factor * gain).astype(BF)


def kernel(nz, nt, *refs):
    (lat_hbm, cond_ref, ctx_hbm, wsh_ref, wsc_ref, wg_ref, wq_hbm, wkv_hbm, wr_hbm, qg_ref, kg_ref,
     uq_hbm, uk_hbm, uv_hbm, bias_ref, wo_hbm, proj_ref, gate_ref,
     lat, ctx, mean_ref, rstd_ref, uk, uv, wo,
     wcat, uqT, ukvT, zmod, xmod, mod, h, qraw, kvraw, kv, kvp, kvc, qb,
     m_ref, l_ref, acc, att, pbuf, mbuf, q_gain_ref, kv_gain_ref, turn_ref,
     load_sem, zm_s, zm_r, xm_s, xm_r, a_s, a_r, lat_x, raw_s, raw_r, rawp_s, rawp_r, q_x, kv_z, kr_s, kr_r, att_x) = refs
    z, t = lax.axis_index("sp"), lax.axis_index("tp")
    core = lax.rem(t, 2)
    chip = t // 2
    nx = nt // 2
    rows = lat.shape[1]
    tok = rows * nt
    crows = ctx.shape[0]
    width = lat.shape[2]
    part = width // nt
    rank_q, rank_kv = wq_hbm.shape[0], wkv_hbm.shape[0]
    along_z = lambda k: {"sp": lax.rem(z + k, nz)}
    along_x = lambda k: {"tp": lax.rem(t + 2 * k, nt)}
    partner = {"tp": t + 1 - 2 * core}
    fourth_of_width = width // 4

    loads = [
        pltpu.make_async_copy(lat_hbm, lat.at[t], load_sem.at[0]),
        pltpu.make_async_copy(ctx_hbm, ctx, load_sem.at[1]),
        pltpu.make_async_copy(wq_hbm, wcat.at[pl.ds(0, rank_q)], load_sem.at[2]),
        pltpu.make_async_copy(wkv_hbm, wcat.at[pl.ds(rank_q, rank_kv)], load_sem.at[3]),
        pltpu.make_async_copy(wr_hbm, wcat.at[pl.ds(rank_q + rank_kv, ROTARY)], load_sem.at[4]),
        pltpu.make_async_copy(uq_hbm, uqT, load_sem.at[5]),
        pltpu.make_async_copy(uk_hbm, uk, load_sem.at[6]),
        pltpu.make_async_copy(uv_hbm, uv, load_sem.at[7]),
        pltpu.make_async_copy(wo_hbm, wo, load_sem.at[8]),
    ]
    barrier = pltpu.get_barrier_semaphore()
    for k in range(1, nz):
        pl.semaphore_signal(barrier, inc=1, device_id=along_z(k), device_id_type=MESH)
    for k in range(1, nt):
        pl.semaphore_signal(barrier, inc=1, device_id={"tp": lax.rem(t + k, nt)}, device_id_type=MESH)
    for load in loads:
        load.start()

    cond = cond_ref[...]
    act = cond / (1.0 + jnp.exp(-cond))
    act = jnp.concatenate([act, jnp.zeros((14, act.shape[1]), F32)], axis=0).astype(BF)
    shift_part = jnp.dot(act, wsh_ref[...], preferred_element_type=F32)
    scale_part = jnp.dot(act, wsc_ref[...], preferred_element_type=F32)
    gate_part = jnp.dot(act, wg_ref[...], preferred_element_type=F32)
    zmod[z] = jnp.concatenate([shift_part[0:2], scale_part[0:2], gate_part[0:2], gate_part[2:4]], axis=0)
    pl.semaphore_wait(barrier, nz + nt - 2)

    def zm(k, incoming):
        if incoming:
            src = lax.rem(z + nz - k, nz)
            return pltpu.make_async_remote_copy(zmod.at[src], zmod.at[src], zm_s.at[k], zm_r.at[k], device_id=along_z(nz - k), device_id_type=MESH)
        return pltpu.make_async_remote_copy(zmod.at[z], zmod.at[z], zm_s.at[k], zm_r.at[k], device_id=along_z(k), device_id_type=MESH)

    def xm(k, incoming):
        if incoming:
            src = lax.rem(t + nt - k, nt)
            return pltpu.make_async_remote_copy(xmod.at[src], xmod.at[src], xm_s.at[k], xm_r.at[k], device_id={"tp": src}, device_id_type=MESH)
        return pltpu.make_async_remote_copy(xmod.at[t], xmod.at[t], xm_s.at[k], xm_r.at[k], device_id={"tp": lax.rem(t + k, nt)}, device_id_type=MESH)

    order = sorted(range(1, nz), key=lambda k: -min(k, nz - k))
    for k in order:
        zm(k, False).start()
    loads[0].wait()
    lat_ring = Gather(nx, chip, along_x,
                      [lambda p, c, i=i: lat.at[2 * p + c, :, pl.ds(i * fourth_of_width, fourth_of_width)] for i in range(4)],
                      lat_x, partner, core)
    lat_ring.start()
    for load in loads[1:]:
        load.wait()
    ukvT[0:2 * PLAIN, :] = uk[...].astype(F32).T.astype(BF)
    ukvT[2 * PLAIN:2 * PLAIN + VROWS, :] = uv[...].astype(F32).T.astype(BF)
    q_gain_ref[...] = jnp.broadcast_to(qg_ref[...], (8, qg_ref.shape[1])).T[:, 0:1]
    kv_gain_ref[...] = jnp.broadcast_to(kg_ref[...], (8, kg_ref.shape[1])).T[:, 0:1]
    pos = lax.broadcasted_iota(jnp.int32, (8, tok), 1) + z * tok
    freq = jnp.exp(lax.broadcasted_iota(jnp.int32, (8, tok), 0).astype(F32) * (-math.log(10000.0) / 8))
    row_angle = (pos >> 6).astype(F32) * freq
    col_angle = (pos & (GRID_W - 1)).astype(F32) * freq
    turn = (jnp.cos(row_angle), jnp.sin(row_angle), jnp.cos(col_angle), jnp.sin(col_angle))

    def chip_rows(p):
        return jnp.concatenate([lat[2 * p].astype(F32), lat[2 * p + 1].astype(F32)], axis=0)

    def note_statistics(p):
        values = chip_rows(p)
        center = values - jnp.mean(values, axis=-1, keepdims=True)
        mean_ref[p] = jnp.mean(values, axis=-1, keepdims=True)
        rstd_ref[p] = lax.rsqrt(jnp.mean(center * center, axis=-1, keepdims=True) + EPSILON)

    lat_ring.step(1)
    far = lat_ring.reach
    for s in range(2, far + 1):
        lat_ring.pair_step(s - 2)

        @pl.loop(0, 1 if s == 2 else 2)
        def _(i):
            note_statistics(lax.rem(chip + jnp.where(i == 0, nx - (s - 2), s - 2), nx))

        lat_ring.step(s)
        if s == min(2, far):
            for k in reversed(order):
                zm(k, True).wait_recv()
            total = zmod[0]
            for k in range(1, nz):
                total = total + zmod[k]
            xmod[t] = total
            for k in range(1, nt):
                xm(k, False).start()
    lat_ring.pair_step(far - 1)

    @pl.loop(0, 2 if far > 1 else 1)
    def _(i):
        note_statistics(lax.rem(chip + jnp.where(i == 0, nx - (far - 1), far - 1), nx))

    lat_ring.pair_step(far)
    note_statistics(lax.rem(chip + far, nx))
    for k in range(1, nt):
        xm(k, True).wait_recv()
    for j in range(nt):
        mod[:, j * part:(j + 1) * part] = xmod[j]

    @pl.loop(0, nx)
    def _(p):
        at = pl.ds(pl.multiple_of(p * 2 * rows, 2 * rows), 2 * rows)
        normed = (chip_rows(p) - mean_ref[p]) * rstd_ref[p]
        h[at, :] = (normed * (1.0 + mod[2:3, :]) + mod[0:1, :]).astype(BF)

    h[tok:, :] = modulated(ctx[...], mod[1:2, :], mod[3:4, :])
    product = lax.dot_general(h[...], wcat[...], (((1,), (1,)), ((), ())), preferred_element_type=F32)
    raw = product[0:tok].T
    rawc = jnp.concatenate([product[tok:], jnp.zeros((128 - crows, product.shape[1]), F32)], axis=0).T
    q_at = lambda p, c, i: pl.ds(pl.multiple_of((2 * p + c) * rank_q + i * (rank_q // 2), rank_q // 2), rank_q // 2)
    kv_at = lambda p, c: pl.ds(pl.multiple_of((2 * p + c) * rank_kv, rank_kv), rank_kv)
    kvraw[kv_at(chip, core), 0:tok] = raw[rank_q:rank_q + rank_kv].astype(BF)
    kvraw[kv_at(chip, core), tok:] = rawc[rank_q:rank_q + rank_kv].astype(BF)
    lane_half = kvraw.shape[1] // 2
    opposite = nx // 2

    def raw_piece(k, side, c):
        piece = kvraw.at[kv_at(lax.rem(chip + nx - k, nx), c)]
        return piece if side is None else kvraw.at[kv_at(lax.rem(chip + nx - k, nx), c), pl.ds(side * lane_half, lane_half)]

    def raw_copy(k, incoming):
        piece = raw_piece(k if incoming else 0, None, core)
        return pltpu.make_async_remote_copy(piece, piece, raw_s.at[k], raw_r.at[k], device_id=along_x(k), device_id_type=MESH)

    def raw_last(side, incoming):
        near = 1 if side == 0 else nx - 1
        piece = raw_piece(opposite if incoming else near, side, core)
        at = opposite if side == 0 else nx
        return pltpu.make_async_remote_copy(piece, piece, raw_s.at[at], raw_r.at[at],
                                            device_id=along_x(opposite - 1 if side == 0 else nx - opposite + 1), device_id_type=MESH)

    def raw_pair(k, incoming):
        piece = raw_piece(k, None, 1 - core if incoming else core)
        return pltpu.make_async_remote_copy(piece, piece, rawp_s.at[k], rawp_r.at[k], device_id=partner, device_id_type=MESH)

    by_distance = [k for m in range(1, opposite) for k in (m, nx - m)]
    for k in by_distance:
        raw_copy(k, False).start()
    raw_pair(0, False).start()
    qraw[pl.ds(pl.multiple_of(t * rank_q, rank_q), rank_q), :] = raw[0:rank_q].astype(BF)
    q_ring = Gather(nx, chip, along_x,
                    [lambda p, c: qraw.at[q_at(p, c, 0), :], lambda p, c: qraw.at[q_at(p, c, 1), :]],
                    q_x, partner, core)
    q_ring.start()
    own_last = lambda a: jnp.where(core == 0, jnp.concatenate([a[ROTARY // 2:], a[:ROTARY // 2]], axis=0), a)
    kv[z, 2 * PLAIN:KROWS, :] = own_last(axial_turn(raw[rank_q + rank_kv:], *turn)).astype(BF)
    for i in range(4):
        turn_ref[i] = turn[i]
    for k in by_distance:
        raw_copy(k, True).wait_recv()
        if k in (1, nx - 1):
            raw_last(0 if k == 1 else 1, False).start()
        raw_pair(k, False).start()
    q_ring.step(1)
    for side in range(2):
        raw_last(side, True).wait_recv()
    raw_pair(opposite, False).start()
    for k in range(nx):
        raw_pair(k, True).wait_recv()

    ckv = rms_columns(kvraw[...], kv_gain_ref[...])
    own = jnp.dot(ukvT[...], ckv, preferred_element_type=F32).astype(BF)
    kv[z, 0:2 * PLAIN, :] = own[0:2 * PLAIN, 0:tok]
    kv[z, KROWS:KROWS + VROWS, :] = own[2 * PLAIN:, 0:tok]
    loose = jnp.concatenate([own[0:2 * PLAIN, tok:].astype(F32), own_last(rawc[rank_q + rank_kv:]).astype(BF).astype(F32), own[2 * PLAIN:, tok:].astype(F32)], axis=0)
    group = (KROWS + VROWS) // 4
    packed = loose[0:group]
    for g in range(1, 4):
        packed = packed + pltpu.roll(loose[g * group:(g + 1) * group], g * crows, 1)
    kvp[z] = jnp.concatenate([packed, jnp.zeros((kvp.shape[1] - group, 128), F32)], axis=0).astype(BF)
    kr_half = ROTARY // 2
    top = 2 * PLAIN + kr_half
    kv_chunks = [lambda p, c: kv.at[p, pl.ds(0, PLAIN)], lambda p, c: kv.at[p, pl.ds(PLAIN, PLAIN)], lambda p, c: kvp.at[p],
                 lambda p, c: kv.at[p, pl.ds(top, kr_half + VALUE)], lambda p, c: kv.at[p, pl.ds(top + kr_half + VALUE, VALUE)]]
    kv_ring = Gather(nz, z, along_z, kv_chunks, kv_z)
    kv_ring.start()

    def query_up():
        for s in range(0, q_ring.reach + 1):
            q_ring.pair_step(s)
        cq = rms_columns(qraw[...], q_gain_ref[...])
        q = jnp.dot(uqT[...], cq, preferred_element_type=F32)
        per = PLAIN + ROTARY
        for head in range(2):
            mine = q[head * per:(head + 1) * per]
            plain = mine[0:PLAIN].astype(BF)
            blank = jnp.zeros_like(plain)
            qb[head, head * PLAIN:(head + 1) * PLAIN, :] = plain
            qb[head, (1 - head) * PLAIN:(2 - head) * PLAIN, :] = blank
            qb[head, 2 * PLAIN:KROWS, :] = own_last(axial_turn(mine[PLAIN:], *[turn_ref[i] for i in range(4)])).astype(BF)

    m_ref[...] = jnp.full_like(m_ref, NEGATIVE)
    l_ref[...] = jnp.zeros_like(l_ref)
    acc[...] = jnp.zeros_like(acc)

    def attend(keysT, valuesT, biased):
        keys = keysT.astype(F32).T.astype(BF)
        for head in range(2):
            s = jnp.dot(keys, qb[head], preferred_element_type=F32) * (SCORE * LOG2E)
            if biased:
                s = s + bias_ref[0, head] * LOG2E
            old = m_ref[head]
            new = jnp.maximum(old, jnp.max(s, axis=0, keepdims=True))
            alpha = jnp.exp2(old - new)
            e = jnp.exp2(s - new)
            m_ref[head] = new
            l_ref[head] = l_ref[head] * alpha + jnp.sum(e, axis=0, keepdims=True)
            acc[head] = acc[head] * alpha + jnp.dot(valuesT[head * VALUE:(head + 1) * VALUE], e.astype(BF), preferred_element_type=F32)

    reach = kv_ring.reach

    def ring_source(d, s):
        return lax.rem(z + jnp.where(d == 0, nz - s, s), nz)

    def nth_source(n):
        return ring_source(1 - lax.rem(n, 2), (n + 1) // 2)

    def hop(d, s, ch, into):
        piece = kv_chunks[ch](ring_source(d, s), 0)
        return pltpu.make_async_remote_copy(piece, piece, kv_z[1].at[d, s, ch], kv_z[0].at[d, into, ch],
                                            device_id=along_z(1 if d == 0 else nz - 1), device_id_type=MESH)

    def kr_swap(d, s, incoming):
        b = ring_source(d, s)
        mine, theirs = kv.at[b, pl.ds(2 * PLAIN + kr_half, kr_half)], kv.at[b, pl.ds(2 * PLAIN, kr_half)]
        return pltpu.make_async_remote_copy(theirs if incoming else mine, theirs, kr_s.at[d, s], kr_r.at[d, s],
                                            device_id=partner, device_id_type=MESH)

    def pass_on(s, ch):
        for d in range(2):
            hop(d, s, ch, s).wait_recv()
            if d == ch // 3:
                hop(d, s, ch, s + 1).start()
            else:
                @pl.when(s + 1 < reach)
                def _():
                    hop(d, s, ch, s + 1).start()
            if ch == 3:
                kr_swap(d, s, False).start()

    def attend_block(n):
        b = nth_source(n)
        attend(kv[b, 0:KROWS, :], kv[b, KROWS:KROWS + VROWS, :], False)

    def unpack(tile):
        lanes = lax.broadcasted_iota(jnp.int32, (group, 128), 1) // crows
        parts = [None] * 4
        for j in range(4):
            held = kvp[nth_source(4 * tile + j)][0:group].astype(F32)
            for g in range(4):
                moved = jnp.where(lanes == g, held, 0.0)
                if g != j:
                    moved = pltpu.roll(moved, ((j - g) % 4) * crows, 1)
                parts[g] = moved if parts[g] is None else parts[g] + moved
        kvc[:, tile * 128:(tile + 1) * 128] = jnp.concatenate(parts, axis=0).astype(BF)

    slots = 4 * (reach - 1)
    first = min(2, q_ring.reach - 1)
    tiles = nz // 4

    def done_after(j):
        return jnp.clip(2 * (j - first + 1), 0, j)

    def context_tiles():
        for tile in range(tiles - 1):
            unpack(tile)
        attend(kvc[0:KROWS, 0:128 * (tiles - 1)], kvc[KROWS:KROWS + VROWS, 0:128 * (tiles - 1)], True)

    def kv_slot(i, carry):
        s = i // 4 + 1

        @pl.when(lax.rem(i, 4) == 0)
        def _():
            pass_on(s, 0)

            @pl.when(s > 1)
            def _():
                for d in range(2):
                    kr_swap(d, s - 1, True).wait_recv()

        @pl.when(lax.rem(i, 4) == 1)
        def _():
            pass_on(s, 1)
            pass_on(s, 2)

        for part_of in (2, 3):
            @pl.when(lax.rem(i, 4) == part_of)
            def _():
                pass_on(s, part_of + 1)

        for step in range(2, q_ring.reach + 1):
            @pl.when(i == 2 * (step - 2))
            def _():
                q_ring.step(step)
                if step == q_ring.reach:
                    query_up()

        if tiles > 1:
            @pl.when(i == slots - 4)
            def _():
                context_tiles()

        @pl.when(lax.rem(i, 2) == 1)
        def _():
            j = i // 2

            @pl.loop(jnp.where(j > first, done_after(j - 1), 0), jnp.where(j >= first, done_after(j), 0))
            def _(n):
                attend_block(n)
        return carry

    lax.fori_loop(0, slots, kv_slot, 0)
    for d in range(2):
        kr_swap(d, reach - 1, True).wait_recv()

    @pl.loop(done_after(slots // 2 - 1), 2 * reach - 1)
    def _(n):
        attend_block(n)
    kv_ring.ring_arrival(0, reach, 0).wait_recv()
    for d, ch in ((0, 1), (0, 2), (1, 3), (1, 4)):
        kv_ring.ring_arrival(d, reach, ch).wait_recv()
    kr_swap(0, reach, False).start()
    unpack(tiles - 1)
    kr_swap(0, reach, True).wait_recv()
    attend_block(2 * reach - 1)
    attend(kvc[0:KROWS, 128 * (tiles - 1):], kvc[KROWS:KROWS + VROWS, 128 * (tiles - 1):], True)

    outT = jnp.concatenate([acc[0] / l_ref[0], acc[1] / l_ref[1]], axis=0)
    mine_at = lambda p, c: pl.ds(pl.multiple_of((2 * p + c) * VROWS, VROWS), VROWS)
    att[:, mine_at(chip, core)] = outT.T.astype(BF)
    fourth = tok // 4
    att_ring = Gather(nx, chip, along_x,
                      [lambda p, c, i=i: att.at[pl.ds(i * fourth, fourth), mine_at(p, c)] for i in range(4)],
                      att_x, partner, core)
    att_ring.start()
    for s in range(1, att_ring.reach + 1):
        att_ring.step(s)

    def am(k, incoming):
        far = lax.rem(t + nt - k, nt) if incoming else lax.rem(t + k, nt)
        if incoming:
            return pltpu.make_async_remote_copy(pbuf.at[far], mbuf.at[far], a_s.at[k], a_r.at[k], device_id={"tp": far}, device_id_type=MESH)
        return pltpu.make_async_remote_copy(pbuf.at[far], mbuf.at[t], a_s.at[k], a_r.at[k], device_id={"tp": far}, device_id_type=MESH)

    for s in range(0, att_ring.reach + 1):
        att_ring.pair_step(s)
    peers = nt // 2
    for part_of in range(2):
        at = part_of * peers
        proj = jnp.dot(att[at * rows:(at + peers) * rows, :], wo[...], preferred_element_type=F32)
        for j in range(peers):
            pbuf[at + j] = proj[j * rows:(j + 1) * rows].astype(BF)
        for j in range(peers):
            far_one = at + lax.rem(t + j, peers)

            @pl.when(far_one != t)
            def _():
                am(lax.rem(far_one - t + nt, nt), False).start()
    mbuf[t] = pbuf[t]
    gate_ref[...] = mod[4:5, :]
    for k in range(1, nt):
        am(k, True).wait_recv()
    for j in range(nt):
        cut = slice(j * part, (j + 1) * part)
        proj_ref[:, cut] = mbuf[j]

    for k in range(1, nz):
        zm(k, False).wait_send()
    for k in range(1, nt):
        xm(k, False).wait_send()
        am(k, False).wait_send()
    lat_ring.finish()
    for k in by_distance:
        raw_copy(k, False).wait_send()
    for side in range(2):
        raw_last(side, False).wait_send()
    for k in range(nx):
        raw_pair(k, False).wait_send()
    for s in range(1, reach + 1):
        for d in range(2 if s < reach else 1):
            kr_swap(d, s, False).wait_send()
    q_ring.finish()
    kv_ring.finish()
    att_ring.finish()


def sems(count, chunks, paired):
    kinds = 4 if paired else 2
    return tuple(pltpu.SemaphoreType.DMA((2, count // 2 + 2, chunks)) for _ in range(kinds))


def on_device(latents, conditions, context, w_shift, w_scale, w_gate, w_qdown, w_kvdown, w_rope, q_gain,
              latent_norm_gain, query_up_weight, key_up_weight, value_up_weight, context_bias, w_out):
    nz, nt = lax.axis_size("sp"), lax.axis_size("tp")
    nx = nt // 2
    rows, width = latents.shape
    tok = rows * nt
    crows = context.shape[0]
    rank_q, rank_kv = w_qdown.shape[1], w_kvdown.shape[1]
    part = width // nt
    vm = pltpu.VMEM
    dma = pltpu.SemaphoreType.DMA
    scratch = [
        vm((nt, rows, width), BF), vm((crows, width), BF), vm((nx, 2 * rows, 1), F32), vm((nx, 2 * rows, 1), F32),
        vm(key_up_weight.shape, BF), vm(value_up_weight.shape, BF), vm(w_out.shape, BF),
        vm((rank_q + rank_kv + ROTARY, width), BF), vm(query_up_weight.shape[::-1], BF), vm((2 * PLAIN + VROWS, nt * rank_kv), BF),
        vm((nz, 8, part), F32), vm((nt, 8, part), F32), vm((8, width), F32),
        vm((tok + crows, width), BF),
        vm((nt * rank_q, tok), BF), vm((nt * rank_kv, tok + 128), BF),
        vm((nz, KROWS + VROWS, tok), BF), vm((nz, 80, 128), BF), vm((KROWS + VROWS, nz * crows), BF), vm((2, KROWS, tok), BF),
        vm((2, 1, tok), F32), vm((2, 1, tok), F32), vm((2, VALUE, tok), F32),
        vm((tok, nt * VROWS), BF), vm((nt, rows, part), BF), vm((nt, rows, part), BF),
        vm((nt * rank_q, 1), F32), vm((nt * rank_kv, 1), F32), vm((4, 8, tok), F32),
        dma((9,)), dma((nz,)), dma((nz,)), dma((nt,)), dma((nt,)), dma((nt,)), dma((nt,)),
        sems(nx, 4, True), dma((nx + 1,)), dma((nx + 1,)), dma((nx,)), dma((nx,)), sems(nx, 2, True), sems(nz, 5, False),
        dma((2, nz // 2 + 1)), dma((2, nz // 2 + 1)), sems(nx, 4, True),
    ]
    here = pl.BlockSpec(memory_space=vm)
    away = pl.BlockSpec(memory_space=pl.ANY)
    small = pl.BlockSpec(memory_space=pltpu.SMEM)
    proj, gate = pl.pallas_call(
        functools.partial(kernel, nz, nt),
        out_shape=(jax.ShapeDtypeStruct((rows, width), BF), jax.ShapeDtypeStruct((1, width), F32)),
        in_specs=[away, here, away, here, here, here, away, away, away, here, here, away, away, away, small, away],
        out_specs=(here, here),
        scratch_shapes=scratch,
        compiler_params=pltpu.CompilerParams(collective_id=0, has_side_effects=True, vmem_limit_bytes=60 * 1024 * 1024),
        name="block",
    )(latents, conditions, context, w_shift, w_scale, w_gate, w_qdown.T, w_kvdown.T, w_rope.T, q_gain.reshape(1, -1),
      latent_norm_gain.reshape(1, -1), query_up_weight.T, key_up_weight, value_up_weight, context_bias.reshape(1, -1), w_out)
    return (latents.astype(F32) + gate * proj.astype(F32)).astype(BF)


def solution(mesh):
    in_specs = (
        P(("grp", "sp", "tp"), None),
        P("grp", "sp"),
        P(("grp", "sp"), None),
        P("sp", "tp"),
        P("sp", "tp"),
        P("sp", "tp"),
        P(None, "tp"),
        P(None, "tp"),
        P(),
        P(),
        P(),
        P(None, "tp"),
        P(None, "tp"),
        P(None, "tp"),
        P("tp"),
        P(None, "tp"),
    )
    return jax.shard_map(on_device, mesh=mesh, in_specs=in_specs, out_specs=P(("grp", "sp", "tp"), None), check_vma=False)
```
